128 devices in a mesh: sp: 16 (over z, x), tp: 8 (over y, core).
Axes of the slice: x: 4, y: 4, z: 4, core: 2. Of those that a mesh axis runs over, the one named last changes fastest.
Arguments:
- inputs: bfloat16 [8192, 4096], P('sp', 'tp'), may hold values from -6 to 6
- w_value: bfloat16 [4096, 4096], P(None, 'tp'), may hold values from -0.09375 to 0.09375
- w_gate: bfloat16 [4096, 4096], P(None, 'tp'), may hold values from -0.09375 to 0.09375
- taps: bfloat16 [31, 4096], P(None, 'tp'), may hold values from -1 to 1
- ln_gain: float32 [4096], P('tp'), may hold values from 0.1 to 1.9
- w_out: bfloat16 [4096, 4096], P(None, 'tp'), may hold values from -0.09375 to 0.09375
- grad_out: bfloat16 [8192, 4096], P('sp', 'tp'), may hold values from -6 to 6
Outputs:
- grad_input: bfloat16 [8192, 4096], P('sp', 'tp')
- grad_value_w: float32 [4096, 4096], P('sp', 'tp')
- grad_gate_w: float32 [4096, 4096], P('sp', 'tp')
- grad_out_w: float32 [4096, 4096], P('sp', 'tp')
- grad_taps: float32 [31, 4096], P(None, 'tp')
- grad_gain: float32 [4096], P('tp')
The draws below stay inside these ranges and needn't reach their ends.
All inputs are finite; a program needn't handle non-finite values.
Results may differ from the reference program's by a relative error of at most 0.017.
Values may be sent and summed in bfloat16 or wider, within the bound.
A program may use at most 128 MiB of HBM per device.

```python
import jax
import jax.numpy as jnp
from jax import lax

D = 4096
CONV = 31
SEQ = 8192
N_TP = 8


def with_spikes(result, key, source, target, shards_of, factor):
    def block_of(position):
        return (jnp.arange(result.shape[position]) // (result.shape[position] // shards_of)).reshape((-1,) + (1,) * (result.ndim - 1 - position))

    first = jax.random.permutation(key, shards_of)[block_of(target)]
    second = (block_of(target) + shards_of // 2) % shards_of
    return jnp.where((block_of(source) == first) | (block_of(source) == second), factor * result, result)


def block_scale(key, dims, cuts, low, high):
    def one(axis_at, shards_of):
        draws = jax.random.uniform(jax.random.fold_in(jax.random.fold_in(key, 6), axis_at), (shards_of,), jnp.float32, low / len(cuts), high / len(cuts))
        return jnp.repeat(jnp.exp(draws), dims[axis_at] // shards_of).reshape((-1,) + (1,) * (len(dims) - axis_at - 1))

    gain = one(*cuts[0])
    for cut in cuts[1:]:
        gain = gain * one(*cut)
    return gain


def noise(rng, shape, spread, limit, split=(), held_as=jnp.bfloat16):
    array = spread * jax.random.normal(rng, shape, jnp.float32)
    if split:
        array = array * block_scale(rng, shape, split, -0.22, 0.18)
    return jnp.clip(array, -limit, limit).astype(held_as)


def heavy_noise(own_key, extent, spread, bound, split, heavy, kind=jnp.bfloat16):
    drawn = spread * jax.random.normal(own_key, extent, jnp.float32)
    if split:
        drawn = drawn * block_scale(own_key, extent, split, -0.22, 0.18)
    return jnp.clip(with_spikes(drawn, jax.random.fold_in(own_key, 3), *heavy), -bound, bound).astype(kind)


def setup_inputs(seed: int = 0) -> dict:
    arg_keys = jax.random.split(jax.random.key(seed), 8)
    return {
        "inputs": heavy_noise(arg_keys[0], (SEQ, D), 1.0, 6.0, ((0, 16), (1, 8)), (0, 1, 16, 2.0)),
        "w_value": noise(arg_keys[1], (D, D), D ** -0.5, 0.09375, ((1, 8),)),
        "w_gate": noise(arg_keys[2], (D, D), D ** -0.5, 0.09375, ((1, 8),)),
        "taps": noise(arg_keys[3], (CONV, D), CONV ** -0.5, 1.0, ((1, 8),)),
        "ln_gain": jnp.clip(1.0 + 0.18 * jax.random.normal(arg_keys[4], (D,), jnp.float32), 0.1, 1.9),
        "w_out": noise(arg_keys[5], (D, D), D ** -0.5, 0.09375, ((1, 8),)),
        "grad_out": heavy_noise(arg_keys[6], (SEQ, D), 1.0, 6.0, ((0, 16), (1, 8)), (0, 1, 16, 2.0)),
    }


def contract_tokens(left, right):
    return lax.dot_general(left, right, (((0,), (0,)), ((), ())), preferred_element_type=jnp.float32)

def contract_channels(left, right):
    return lax.dot_general(left, right, (((1,), (1,)), ((), ())), preferred_element_type=jnp.float32)

def reference(inputs, w_value, w_gate, taps, ln_gain, w_out, grad_out):
    seq_len = inputs.shape[0]
    full_width = inputs.shape[1]
    radius = taps.shape[0] // 2
    pre_value = jnp.dot(inputs, w_value, preferred_element_type=jnp.float32)
    pre_gate = jnp.dot(inputs, w_gate, preferred_element_type=jnp.float32)
    gate_sigmoid = jax.nn.sigmoid(pre_gate)
    hidden = (pre_value * gate_sigmoid).astype(jnp.bfloat16)
    padded = jnp.pad(hidden.astype(jnp.float32), ((radius, radius), (0, 0)))
    tap_values = taps.astype(jnp.float32)
    convolved = jnp.zeros((seq_len, full_width), jnp.float32)
    for offset in range(taps.shape[0]):
        convolved = convolved + tap_values[offset] * padded[offset:offset + seq_len]
    mean = lax.optimization_barrier(jnp.sum(convolved, axis=1, keepdims=True)) / full_width
    variance = lax.optimization_barrier(jnp.sum(convolved * convolved, axis=1, keepdims=True)) / full_width - mean * mean
    inverse = lax.rsqrt(variance + 1e-06)
    normed = (convolved - mean) * inverse
    scaled = normed * ln_gain
    activated = jax.nn.silu(scaled).astype(jnp.bfloat16)
    grad_act = jnp.dot(grad_out, w_out, preferred_element_type=jnp.float32)
    sig_scaled = jax.nn.sigmoid(scaled)
    grad_scaled = grad_act * sig_scaled * (1.0 + scaled * (1.0 - sig_scaled))
    grad_gain = lax.optimization_barrier(jnp.sum(grad_scaled * normed, axis=0))
    grad_normed = grad_scaled * ln_gain
    first_sum = lax.optimization_barrier(jnp.sum(grad_normed, axis=1, keepdims=True)) / full_width
    second_sum = lax.optimization_barrier(jnp.sum(grad_normed * normed, axis=1, keepdims=True)) / full_width
    grad_conv = inverse * (grad_normed - first_sum - normed * second_sum)
    tap_rows = []
    for offset in range(taps.shape[0]):
        tap_rows.append(lax.optimization_barrier(jnp.sum(padded[offset:offset + seq_len] * grad_conv, axis=0)))
    grad_taps = jnp.stack(tap_rows, axis=0)
    grad_padded = jnp.pad(grad_conv, ((radius, radius), (0, 0)))
    grad_hidden = jnp.zeros((seq_len, full_width), jnp.float32)
    for offset in range(taps.shape[0]):
        begin = 2 * radius - offset
        grad_hidden = grad_hidden + tap_values[offset] * grad_padded[begin:begin + seq_len]
    grad_value = (grad_hidden * gate_sigmoid).astype(jnp.bfloat16)
    grad_gate = (grad_hidden * pre_value * gate_sigmoid * (1.0 - gate_sigmoid)).astype(jnp.bfloat16)
    grad_value_w = contract_tokens(inputs, grad_value)
    grad_gate_w = contract_tokens(inputs, grad_gate)
    grad_out_w = contract_tokens(grad_out, activated)
    block = full_width // N_TP
    total = jnp.zeros((seq_len, full_width), jnp.float32)
    for index in range(N_TP):
        lower = index * block
        partial_value = contract_channels(grad_value[:, lower:lower + block], w_value[:, lower:lower + block])
        partial_value = partial_value + contract_channels(grad_gate[:, lower:lower + block], w_gate[:, lower:lower + block])
        rounded = lax.optimization_barrier(partial_value.astype(jnp.bfloat16))
        total = total + rounded.astype(jnp.float32)
    grad_input = total.astype(jnp.bfloat16)
    return (grad_input, grad_value_w, grad_gate_w, grad_out_w, grad_taps, grad_gain)
```

```python
import jax
import jax.numpy as jnp
from jax import lax
from jax.experimental import pallas as pl
from jax.experimental.pallas import tpu as pltpu
from jax.sharding import PartitionSpec as P

MESH = pl.DeviceIdType.MESH
F32 = jnp.float32
BF16 = jnp.bfloat16
HI = lax.Precision.HIGHEST
T = 512
C = 512
NB = 8
RAD = 15
TAPS = 31
PAD = 16
COLS = (0, 128, 256, 384)
N_COPIES = 160


def sig(v):
    return 1.0 / (1.0 + jnp.exp(-v))


def dot_nn(a, b):
    return lax.dot_general(a, b, (((1,), (0,)), ((), ())), preferred_element_type=F32)


def dot_nt(a, b):
    return lax.dot_general(a, b, (((1,), (1,)), ((), ())), preferred_element_type=F32)


def dot_tn(a, b):
    return lax.dot_general(a, b, (((0,), (0,)), ((), ())), preferred_element_type=F32)


def kernel(
    x_hbm, g_hbm, wv_hbm, wg_hbm, wo_hbm, taps_ref, gain_ref,
    gi_out, gvw_out, ggw_out, gow_out, taps_out, gain_out,
    X, G, WV, WG, WO, PV, PG, GA, NRM, HID, GC, ACT, GV, GG,
    SA, SQ, MEAN, INV, TF, ST, STR, TP, GP, TG, TGR,
    part, r1, r2, r3, r4, PR, y1, y2, ss, rs, ls,
):
    sp = lax.axis_index("sp")
    tp = lax.axis_index("tp")
    z, x = sp // 4, sp % 4
    y, c = tp // 2, tp % 2

    def at_tp(t):
        return (sp, t)

    def at_y(yy):
        return (sp, (yy % 4) * 2 + c)

    def at_x(xx):
        return (z * 4 + xx % 4, tp)

    def at_z(zz):
        return ((zz % 4) * 4 + x, tp)

    partner = at_tp(y * 2 + (1 - c))

    counter = [0]
    sent = []
    done = []

    def rcopy(src, dst, dev):
        i = counter[0]
        counter[0] += 1
        cp = pltpu.make_async_remote_copy(
            src_ref=src, dst_ref=dst, send_sem=ss.at[i], recv_sem=rs.at[i],
            device_id=dev, device_id_type=MESH,
        )
        cp.start()
        sent.append(cp)
        return cp

    loads = []
    for i, (src, dst) in enumerate(
        ((x_hbm, X.at[tp]), (wv_hbm, WV), (wg_hbm, WG), (g_hbm, G.at[tp]), (wo_hbm, WO))
    ):
        cp = pltpu.make_async_copy(src, dst, ls.at[i])
        cp.start()
        loads.append(cp)

    barrier = pltpu.get_barrier_semaphore()
    peers = [at_tp((tp + d) % 8) for d in range(1, 8)]
    peers += [at_x(x + d) for d in range(1, 4)] + [at_z(z + d) for d in range(1, 4)]
    peers += [((sp + 1) % 16, tp), ((sp + 15) % 16, tp)]
    for dev in peers:
        pl.semaphore_signal(barrier, inc=1, device_id=dev, device_id_type=MESH)
    PV[...] = jnp.zeros((T, C), F32)
    PG[...] = jnp.zeros((T, C), F32)
    GA[...] = jnp.zeros((T, C), F32)
    TF[...] = jnp.zeros((32, C), F32)
    TF[0:TAPS, :] = taps_ref[...].astype(F32)
    pl.semaphore_wait(barrier, len(peers))

    jm = ((y + 3) % 4) * 2 + c
    jp = ((y + 1) % 4) * 2 + c
    jo = ((y + 2) % 4) * 2 + c
    LO, HIH = pl.ds(0, 256), pl.ds(256, 256)

    class Gather:
        def __init__(self, buf):
            self.b = buf

        def start(self):
            b = self.b
            self.h1p = rcopy(b.at[tp, LO], b.at[tp, LO], at_y(y + 1))
            self.h1m = rcopy(b.at[tp, HIH], b.at[tp, HIH], at_y(y + 3))
            self.d0 = rcopy(b.at[tp], b.at[tp], partner)
            self.h2p = rcopy(b.at[tp, HIH], b.at[tp, HIH], at_y(y + 1))
            self.h2m = rcopy(b.at[tp, LO], b.at[tp, LO], at_y(y + 3))

        def first(self):
            b = self.b
            self.h1p.wait_recv()
            self.fp = rcopy(b.at[jm, LO], b.at[jm, LO], at_y(y + 1))
            self.d1p = rcopy(b.at[jm, LO], b.at[jm, LO], partner)
            self.h1m.wait_recv()
            self.fm = rcopy(b.at[jp, HIH], b.at[jp, HIH], at_y(y + 3))
            self.d1m = rcopy(b.at[jp, HIH], b.at[jp, HIH], partner)

        def second(self):
            b = self.b
            self.h2p.wait_recv()
            self.d2p = rcopy(b.at[jm, HIH], b.at[jm, HIH], partner)
            self.h2m.wait_recv()
            self.d2m = rcopy(b.at[jp, LO], b.at[jp, LO], partner)

        def third(self):
            b = self.b
            self.fp.wait_recv()
            self.d3p = rcopy(b.at[jo, LO], b.at[jo, LO], partner)
            self.fm.wait_recv()
            self.d3m = rcopy(b.at[jo, HIH], b.at[jo, HIH], partner)

    def mm(buf, pairs, d_even, d_odd, row_even, row_odd, lo, hi):
        def body(i, _):
            e = i % 2
            par = i // 2
            cc = c + par - 2 * c * par
            j = ((y + d_even + e * (d_odd - d_even)) % 4) * 2 + cc
            row = pl.multiple_of(row_even + e * (row_odd - row_even), 256)
            rows = pl.ds(row, 256)
            a = buf[j, rows, :]
            for w, acc in pairs:
                for n in (0, 256):
                    acc[rows, n:n + 256] += dot_nn(a, w[j, :, n:n + 256])
            return 0

        lax.fori_loop(lo, hi, body, 0)

    gx, gg_ = Gather(X), Gather(G)
    vg = ((WV, PV), (WG, PG))
    wo = ((WO, GA),)
    loads[0].wait()
    gx.start()
    loads[1].wait()
    loads[2].wait()
    mm(X, vg, 0, 0, 0, 256, 0, 2)
    gx.d0.wait_recv()
    mm(X, vg, 0, 0, 0, 256, 2, 4)
    gx.first()
    loads[3].wait()
    gg_.start()
    mm(X, vg, 3, 1, 0, 256, 0, 2)
    gx.d1p.wait_recv()
    gx.d1m.wait_recv()
    mm(X, vg, 3, 1, 0, 256, 2, 4)
    gx.second()
    mm(X, vg, 3, 1, 256, 0, 0, 2)
    gx.d2p.wait_recv()
    gx.d2m.wait_recv()
    mm(X, vg, 3, 1, 256, 0, 2, 4)
    gx.third()
    mm(X, vg, 2, 2, 0, 256, 0, 2)
    gx.d3p.wait_recv()
    gx.d3m.wait_recv()
    mm(X, vg, 2, 2, 0, 256, 2, 4)

    def hidden_body(i, _):
        rows = pl.ds(pl.multiple_of(i * 32, 32), 32)
        out_rows = pl.ds(pl.multiple_of(i * 32 + PAD, 16), 32)
        s = sig(PG[rows, :])
        PG[rows, :] = s
        HID[out_rows, :] = (PV[rows, :] * s).astype(BF16).astype(F32)
        return 0

    lax.fori_loop(0, T // 32, hidden_body, 0)

    following, previous = ((sp + 1) % 16, tp), ((sp + 15) % 16, tp)

    def halo_start(buf):
        up = rcopy(buf.at[pl.ds(T, PAD)], buf.at[pl.ds(0, PAD)], following)
        down = rcopy(buf.at[pl.ds(PAD, PAD)], buf.at[pl.ds(T + PAD, PAD)], previous)
        return up, down

    def halo_finish(buf, pair):
        pair[0].wait_recv()
        pair[1].wait_recv()

        @pl.when(sp == 0)
        def _():
            buf[0:PAD, :] = jnp.zeros((PAD, C), F32)

        @pl.when(sp == 15)
        def _():
            buf[T + PAD:T + 2 * PAD, :] = jnp.zeros((PAD, C), F32)

    halo = halo_start(HID)
    loads[4].wait()
    mm(G, wo, 0, 0, 0, 256, 0, 2)
    gg_.d0.wait_recv()
    mm(G, wo, 0, 0, 0, 256, 2, 4)
    halo_finish(HID, halo)
    gg_.first()

    R = 64

    def conv_tile(src, r0, cs, flip):
        acc = jnp.zeros((R, 128), F32)
        window = src.at[pl.ds(r0, R + 2 * PAD)]
        for o in range(1, TAPS + 1):
            k = TAPS - o if flip else o - 1
            acc = acc + TF[k:k + 1, cs:cs + 128] * window[o:o + R, cs:cs + 128]
        return acc

    def conv_body(i, _):
        r0 = pl.multiple_of(i * R, R)
        rows = pl.ds(r0, R)
        s = jnp.zeros((R, 128), F32)
        q = jnp.zeros((R, 128), F32)
        for cs in COLS:
            v = conv_tile(HID, r0, cs, False)
            NRM[rows, cs:cs + 128] = v
            s = s + v
            q = q + v * v
        SA[rows, :] = s
        SQ[rows, :] = q
        return 0

    lax.fori_loop(0, T // R, conv_body, 0)

    def stats_start(e):
        row = lax.broadcasted_iota(jnp.int32, (8, 128), 0)
        dims = (((1,), (1,)), ((), ()))
        tile = lax.dot_general(
            jnp.where(row == 0, 1.0, 0.0).astype(F32), SA[...], dims, precision=HI, preferred_element_type=F32
        ) + lax.dot_general(
            jnp.where(row == 1, 1.0, 0.0).astype(F32), SQ[...], dims, precision=HI, preferred_element_type=F32
        )
        ST[e] = tile
        STR[e, tp] = tile
        return [rcopy(ST.at[e], STR.at[e, tp], at_tp((tp + d) % 8)) for d in range(1, 8)]

    def stats_finish(e, copies):
        for cp in copies:
            cp.wait_recv()
        row = lax.broadcasted_iota(jnp.int32, (64, 256), 0) & 7
        lane = lax.broadcasted_iota(jnp.int32, (64, 256), 1)
        want = jnp.where(lane < 128, 0, 1)
        pick = jnp.where(row == want, 1.0, 0.0).astype(F32)
        for t in range(0, T, 128):
            block = STR[e, :, :, t:t + 128].reshape(64, 128)
            both = lax.dot_general(
                block, pick, (((0,), (0,)), ((), ())), precision=HI, preferred_element_type=F32
            ) * (1.0 / (NB * C))
            if e == 0:
                mean = both[:, :128]
                MEAN[t:t + 128, :] = mean
                INV[t:t + 128, :] = lax.rsqrt(both[:, 128:] - mean * mean + 1e-06)
            else:
                SA[t:t + 128, :] = both[:, :128]
                SQ[t:t + 128, :] = both[:, 128:]

    stats = stats_start(0)
    mm(G, wo, 3, 1, 0, 256, 0, 2)
    gg_.d1p.wait_recv()
    gg_.d1m.wait_recv()
    mm(G, wo, 3, 1, 0, 256, 2, 4)
    stats_finish(0, stats)

    def norm_body(i, _):
        rows = pl.ds(pl.multiple_of(i * 32, 32), 32)
        m, iv = MEAN[rows, :], INV[rows, :]
        for cs in COLS:
            n = (NRM[rows, cs:cs + 128] - m) * iv
            NRM[rows, cs:cs + 128] = n
            sc = n * gain_ref[0:1, cs:cs + 128]
            ACT[rows, cs:cs + 128] = (sc * sig(sc)).astype(BF16)
        return 0

    lax.fori_loop(0, T // 32, norm_body, 0)

    gg_.second()
    mm(G, wo, 3, 1, 256, 0, 0, 2)
    gg_.d2p.wait_recv()
    gg_.d2m.wait_recv()
    mm(G, wo, 3, 1, 256, 0, 2, 4)
    gg_.third()
    mm(G, wo, 2, 2, 0, 256, 0, 2)
    gg_.d3p.wait_recv()
    gg_.d3m.wait_recv()
    mm(G, wo, 2, 2, 0, 256, 2, 4)

    GP[...] = jnp.zeros((8, C), F32)

    def scaled_body(i, _):
        rows = pl.ds(pl.multiple_of(i * 32, 32), 32)
        s1 = jnp.zeros((32, 128), F32)
        s2 = jnp.zeros((32, 128), F32)
        for cs in COLS:
            n = NRM[rows, cs:cs + 128]
            gain = gain_ref[0:1, cs:cs + 128]
            sc = n * gain
            s = sig(sc)
            gs = GA[rows, cs:cs + 128] * s * (1.0 + sc * (1.0 - s))
            GP[:, cs:cs + 128] += (gs * n).reshape(4, 8, 128).sum(axis=0)
            gn = gs * gain
            GA[rows, cs:cs + 128] = gn
            s1 = s1 + gn
            s2 = s2 + gn * n
        SA[rows, :] = s1
        SQ[rows, :] = s2
        return 0

    lax.fori_loop(0, T // 32, scaled_body, 0)
    stats = stats_start(1)

    at_p = (at_x, at_z)
    at_q = (at_z, at_x)
    me_p = (x, z)
    me_q = (z, x)

    def dw(lhs, units, h, dp):
        p = (me_p[h] + dp) % 4

        def body(q, _):
            zz, xx = (q, p) if h == 0 else (p, q)
            s = zz * 4 + xx
            cols = pl.ds(pl.multiple_of((s % 2) * 256, 256), 256)
            a = lhs[s // 2, :, cols]
            for u, rhs in units:
                part[u, h, p, q] = dot_tn(a, rhs[:, h * 256:h * 256 + 256]).astype(BF16)
            return 0

        lax.fori_loop(0, 4, body, 0)

    class Scatter:
        def __init__(self, u, h):
            self.u, self.h = u, h
            self.p, self.q = me_p[h], me_q[h]

        def blk(self, dp, q0, n=2):
            return part.at[self.u, self.h, (self.p + dp) % 4, pl.ds(q0, n)]

        def s1(self):
            u, h, p = self.u, self.h, self.p
            self.a = rcopy(self.blk(2, 0), r1.at[u, h, 0], at_p[h](p + 1))
            self.b = rcopy(self.blk(2, 2), r1.at[u, h, 1], at_p[h](p + 3))

        def s2i(self):
            u, h, p = self.u, self.h, self.p
            self.c = rcopy(self.blk(1, 2), r2.at[u, h, 0, pl.ds(2, 2)], at_p[h](p + 1))
            self.d = rcopy(self.blk(3, 0), r2.at[u, h, 1, pl.ds(0, 2)], at_p[h](p + 3))

        def add(self, dst_index, rows, sources):
            u, h = self.u, self.h

            def body(i, _):
                rr = pl.ds(pl.multiple_of(rows + i * 32, 32), 32)
                v = part[(u, h) + dst_index + (rr,)].astype(F32)
                for ref, index, off in sources:
                    v = v + ref[index + (pl.ds(pl.multiple_of(off + i * 32, 32), 32),)].astype(F32)
                part[(u, h) + dst_index + (rr,)] = v.astype(BF16)
                return 0

            return body

        def s2d(self):
            u, h, p = self.u, self.h, self.p
            self.a.wait_recv()
            for q in (0, 1):
                lax.fori_loop(0, 8, self.add(((p + 1) % 4, q), 0, [(r1, (u, h, 0, q), 0)]), 0)
            self.e = rcopy(self.blk(1, 0), r2.at[u, h, 0, pl.ds(0, 2)], at_p[h](p + 1))
            self.b.wait_recv()
            for q in (2, 3):
                lax.fori_loop(0, 8, self.add(((p + 3) % 4, q), 0, [(r1, (u, h, 1, q - 2), 0)]), 0)
            self.f = rcopy(self.blk(3, 2), r2.at[u, h, 1, pl.ds(2, 2)], at_p[h](p + 3))

        def p1(self):
            u, h, p, q = self.u, self.h, self.p, self.q
            for cp in (self.c, self.d, self.e, self.f):
                cp.wait_recv()
            for dq in (2, 1, 3, 0):
                qq = (q + dq) % 4
                lax.fori_loop(
                    0, 8, self.add((p, qq), 0, [(r2, (u, h, 0, qq), 0), (r2, (u, h, 1, qq), 0)]), 0
                )
                if dq == 2:
                    src = part.at[u, h, p, qq]
                    self.i = rcopy(src.at[pl.ds(0, 128)], r3.at[u, h, 0], at_q[h](q + 1))
                    self.j = rcopy(src.at[pl.ds(128, 128)], r3.at[u, h, 1], at_q[h](q + 3))

        def p2(self):
            u, h, p, q = self.u, self.h, self.p, self.q
            up, down = (q + 1) % 4, (q + 3) % 4
            self.i.wait_recv()
            lax.fori_loop(0, 4, self.add((p, up), 0, [(r3, (u, h, 0), 0)]), 0)
            self.k = rcopy(part.at[u, h, p, up], r4.at[u, h, 0], at_q[h](q + 1))
            self.j.wait_recv()
            lax.fori_loop(0, 4, self.add((p, down), 128, [(r3, (u, h, 1), 0)]), 0)
            self.l = rcopy(part.at[u, h, p, down], r4.at[u, h, 1], at_q[h](q + 3))

        def finish(self, out):
            u, h, p, q = self.u, self.h, self.p, self.q
            self.k.wait_recv()
            self.l.wait_recv()

            def body(i, _):
                rr = pl.ds(pl.multiple_of(i * 32, 32), 32)
                out[rr, h * 256:h * 256 + 256] = (
                    part[u, h, p, q, rr].astype(F32)
                    + r4[u, h, 0, rr].astype(F32)
                    + r4[u, h, 1, rr].astype(F32)
                )
                return 0

            lax.fori_loop(0, 8, body, 0)

    sc = [[Scatter(u, h) for h in (0, 1)] for u in range(3)]

    def produce(lhs, units):
        for h in (0, 1):
            dw(lhs, units, h, 2)
            for u, _ in units:
                sc[u][h].s1()
        for h in (0, 1):
            dw(lhs, units, h, 1)
            dw(lhs, units, h, 3)
            for u, _ in units:
                sc[u][h].s2i()
        for h in (0, 1):
            dw(lhs, units, h, 0)

    produce(G, [(0, ACT)])
    stats_finish(1, stats)

    def gc_body(i, _):
        rows = pl.ds(pl.multiple_of(i * 32, 32), 32)
        out_rows = pl.ds(pl.multiple_of(i * 32 + PAD, 16), 32)
        f, s, iv = SA[rows, :], SQ[rows, :], INV[rows, :]
        for cs in COLS:
            col = slice(cs, cs + 128)
            GC[out_rows, col] = iv * (GA[rows, col] - f - NRM[rows, col] * s)
        return 0

    lax.fori_loop(0, T // 32, gc_body, 0)
    halo = halo_start(GC)

    for cs in COLS:
        def tap_body(i, accs, cs=cs):
            r0 = pl.multiple_of(i * 8, 8)
            window = HID.at[pl.ds(r0, 8 + 2 * PAD)]
            g = GC[pl.ds(pl.multiple_of(r0 + PAD, 8), 8), cs:cs + 128]
            return tuple(
                a + window[1 + k:9 + k, cs:cs + 128] * g for k, a in enumerate(accs)
            )

        accs = lax.fori_loop(
            0, T // 8, tap_body, tuple(jnp.zeros((8, 128), F32) for _ in range(TAPS))
        )
        for k, a in enumerate(accs):
            TP[k:k + 1, cs:cs + 128] = jnp.sum(a, axis=0, keepdims=True)
    TP[TAPS:TAPS + 1, :] = jnp.sum(GP[...], axis=0, keepdims=True)

    def small_start(e, me, at):
        TGR[e, me] = TG[e]
        return [rcopy(TG.at[e], TGR.at[e, me], at(me + d)) for d in range(1, 4)]

    def small_finish(e, copies):
        for cp in copies:
            cp.wait_recv()
        v = TGR[e, 0].astype(F32)
        for i in range(1, 4):
            v = v + TGR[e, i].astype(F32)
        return v

    TG[0] = TP[...].astype(BF16)
    small = small_start(0, x, at_x)

    for h in (0, 1):
        sc[0][h].s2d()
    halo_finish(GC, halo)

    def back_body(i, _):
        r0 = pl.multiple_of(i * R, R)
        rows = pl.ds(r0, R)
        for cs in COLS:
            col = slice(cs, cs + 128)
            gh = conv_tile(GC, r0, cs, True)
            s = PG[rows, col]
            gv = gh * s
            GV[rows, col] = gv.astype(BF16)
            GG[rows, col] = (gv * PV[rows, col] * (1.0 - s)).astype(BF16)
        return 0

    lax.fori_loop(0, T // R, back_body, 0)

    produce(X, [(1, GV), (2, GG)])

    for h in (0, 1):
        sc[0][h].p1()
    TG[1] = small_finish(0, small).astype(BF16)
    small = small_start(1, z, at_z)

    for cp in (gg_.h1p, gg_.h1m, gg_.d0, gg_.h2p, gg_.h2m, gg_.fp, gg_.fm, gg_.d1p, gg_.d1m,
               gg_.d2p, gg_.d2m, gg_.d3p, gg_.d3m):
        cp.wait_send()
        done.append(id(cp))

    def partial(parity):
        def body(i, _):
            yy = i // 2
            rows = pl.ds(pl.multiple_of((i % 2) * 256, 256), 256)
            j = yy * 2 + parity
            gv, gt = GV[rows, :], GG[rows, :]
            for n in (0, 256):
                G[parity * 4 + yy, rows, n:n + 256] = (
                    dot_nt(gv, WV[j, n:n + 256, :]) + dot_nt(gt, WG[j, n:n + 256, :])
                ).astype(BF16)
            return 0

        lax.fori_loop(0, 8, body, 0)

    partial(1 - c)
    swap = rcopy(G.at[pl.ds((1 - c) * 4, 4)], PR, partner)
    for u in (1, 2):
        for h in (0, 1):
            sc[u][h].s2d()
    partial(c)
    swap.wait_recv()

    def y_add(block, row0, n, sources):
        def body(i, _):
            rr = pl.ds(pl.multiple_of(row0 + i * 32, 32), 32)
            v = G[block, rr].astype(F32)
            for ref, index, off in sources:
                v = v + ref[index + (pl.ds(pl.multiple_of(off + i * 32, 32), 32),)].astype(F32)
            G[block, rr] = v.astype(BF16)
            return 0

        lax.fori_loop(0, n // 32, body, 0)

    base = c * 4
    y2_, yp_, ym_ = (y + 2) % 4, (y + 1) % 4, (y + 3) % 4
    y_add(base + y2_, 0, T, [(PR, (y2_,), 0)])
    ya = rcopy(G.at[base + y2_, LO], y1.at[0], at_y(y + 1))
    yb = rcopy(G.at[base + y2_, HIH], y1.at[1], at_y(y + 3))
    y_add(base + yp_, 0, T, [(PR, (yp_,), 0)])
    yc = rcopy(G.at[base + yp_, HIH], y2.at[0, HIH], at_y(y + 1))
    y_add(base + ym_, 0, T, [(PR, (ym_,), 0)])
    yd = rcopy(G.at[base + ym_, LO], y2.at[1, LO], at_y(y + 3))
    y_add(base + y, 0, T, [(PR, (y,), 0)])

    for h in (0, 1):
        sc[0][h].p2()
    ya.wait_recv()
    y_add(base + yp_, 0, 256, [(y1, (0,), 0)])
    ye = rcopy(G.at[base + yp_, LO], y2.at[0, LO], at_y(y + 1))
    yb.wait_recv()
    y_add(base + ym_, 256, 256, [(y1, (1,), 0)])
    yf = rcopy(G.at[base + ym_, HIH], y2.at[1, HIH], at_y(y + 3))

    for h in (0, 1):
        sc[1][h].p1()
    for h in (0, 1):
        sc[0][h].finish(gow_out)
    total = small_finish(1, small)
    taps_out[...] = total[0:TAPS]
    gain_out[...] = total[TAPS:TAPS + 1]
    for h in (0, 1):
        sc[2][h].p1()
    for h in (0, 1):
        sc[1][h].p2()
    for h in (0, 1):
        sc[2][h].p2()
    for cp in (yc, yd, ye, yf):
        cp.wait_recv()

    def gi_body(i, _):
        rr = pl.ds(pl.multiple_of(i * 32, 32), 32)
        gi_out[rr, :] = (
            G[base + y, rr].astype(F32) + y2[0, rr].astype(F32) + y2[1, rr].astype(F32)
        ).astype(BF16)
        return 0

    lax.fori_loop(0, T // 32, gi_body, 0)
    for h in (0, 1):
        sc[1][h].finish(gvw_out)
    for h in (0, 1):
        sc[2][h].finish(ggw_out)
    for cp in sent:
        if id(cp) not in done:
            cp.wait_send()
    assert counter[0] <= N_COPIES, counter[0]


def local(inputs, w_value, w_gate, taps, ln_gain, w_out, grad_out):
    vm = pltpu.VMEM
    anyspace = pl.BlockSpec(memory_space=pl.ANY)
    in_vmem = pl.BlockSpec(memory_space=pltpu.VMEM)
    shape3 = (NB, C, C)
    gi, gvw, ggw, gow, gt, gg = pl.pallas_call(
        kernel,
        out_shape=(
            jax.ShapeDtypeStruct((T, C), BF16),
            jax.ShapeDtypeStruct((256, C), F32),
            jax.ShapeDtypeStruct((256, C), F32),
            jax.ShapeDtypeStruct((256, C), F32),
            jax.ShapeDtypeStruct((TAPS, C), F32),
            jax.ShapeDtypeStruct((1, C), F32),
        ),
        in_specs=[anyspace] * 5 + [in_vmem] * 2,
        out_specs=(in_vmem,) * 6,
        scratch_shapes=[
            vm((NB, T, C), BF16), vm((NB, T, C), BF16),
            vm(shape3, BF16), vm(shape3, BF16), vm(shape3, BF16),
            vm((T, C), F32), vm((T, C), F32), vm((T, C), F32), vm((T, C), F32),
            vm((T + 2 * PAD, C), F32), vm((T + 2 * PAD, C), F32),
            vm((T, C), BF16), vm((T, C), BF16), vm((T, C), BF16),
            vm((T, 128), F32), vm((T, 128), F32), vm((T, 128), F32), vm((T, 128), F32),
            vm((32, C), F32),
            vm((2, 8, T), F32), vm((2, NB, 8, T), F32),
            vm((32, C), F32), vm((8, C), F32),
            vm((2, 32, C), BF16), vm((2, 4, 32, C), BF16),
            vm((3, 2, 4, 4, 256, 256), BF16),
            vm((3, 2, 2, 2, 256, 256), BF16),
            vm((3, 2, 2, 4, 256, 256), BF16),
            vm((3, 2, 2, 128, 256), BF16),
            vm((3, 2, 2, 256, 256), BF16),
            vm((4, T, C), BF16),
            vm((2, 256, C), BF16), vm((2, T, C), BF16),
            pltpu.SemaphoreType.DMA((N_COPIES,)),
            pltpu.SemaphoreType.DMA((N_COPIES,)),
            pltpu.SemaphoreType.DMA((5,)),
        ],
        compiler_params=pltpu.CompilerParams(
            collective_id=0, has_side_effects=True, vmem_limit_bytes=67043328
        ),
    )(
        inputs, grad_out, w_value.reshape(shape3), w_gate.reshape(shape3), w_out.reshape(shape3),
        taps, ln_gain.reshape(1, C),
    )
    return gi, gvw, ggw, gow, gt, gg.reshape(C)


def solution(mesh):
    in_specs = (
        P("sp", "tp"), P(None, "tp"), P(None, "tp"), P(None, "tp"), P("tp"), P(None, "tp"), P("sp", "tp"),
    )
    out_specs = (P("sp", "tp"), P("sp", "tp"), P("sp", "tp"), P("sp", "tp"), P(None, "tp"), P("tp"))
    return jax.shard_map(local, mesh=mesh, in_specs=in_specs, out_specs=out_specs, check_vma=False)
```

```python
import jax
import jax.numpy as jnp
from jax import lax
from jax.experimental import pallas as pl
from jax.experimental.pallas import tpu as pltpu
from jax.sharding import PartitionSpec as P

MESH = pl.DeviceIdType.MESH
F32 = jnp.float32
BF16 = jnp.bfloat16
HI = lax.Precision.HIGHEST
T = 512
C = 512
NB = 8
RAD = 15
TAPS = 31
PAD = 16
COLS = (0, 128, 256, 384)
N_COPIES = 160


def sig(v):
    return 1.0 / (1.0 + jnp.exp(-v))


def dot_nn(a, b):
    return lax.dot_general(a, b, (((1,), (0,)), ((), ())), preferred_element_type=F32)


def dot_nt(a, b):
    return lax.dot_general(a, b, (((1,), (1,)), ((), ())), preferred_element_type=F32)


def dot_tn(a, b):
    return lax.dot_general(a, b, (((0,), (0,)), ((), ())), preferred_element_type=F32)


def kernel(
    x_hbm, g_hbm, wv_hbm, wg_hbm, wo_hbm, taps_ref, gain_ref,
    gi_out, w_out, taps_out,
    X, G, WV, WG, WO, PV, PG, GA, NRM, HID, GC, ACT, GV, GG, AT, BT,
    SA, SQ, MEAN, INV, TF, ST, STR, TP, GP, TG, TGR,
    part, r1, r2, r3, r4, PR, y1, y2, ss, rs, ls,
):
    sp = lax.axis_index("sp")
    tp = lax.axis_index("tp")
    z, x = sp // 4, sp % 4
    y, c = tp // 2, tp % 2

    def at_tp(t):
        return (sp, t)

    def at_y(yy):
        return (sp, (yy % 4) * 2 + c)

    def at_x(xx):
        return (z * 4 + xx % 4, tp)

    def at_z(zz):
        return ((zz % 4) * 4 + x, tp)

    partner = at_tp(y * 2 + (1 - c))

    scope = [None]

    def mark(name):
        if scope[0] is not None:
            scope[0].__exit__(None, None, None)
        scope[0] = jax.named_scope(name) if name else None
        if name:
            scope[0].__enter__()

    counter = [0]
    sent = []
    done = []

    def rcopy(src, dst, dev):
        i = counter[0]
        counter[0] += 1
        cp = pltpu.make_async_remote_copy(
            src_ref=src, dst_ref=dst, send_sem=ss.at[i], recv_sem=rs.at[i],
            device_id=dev, device_id_type=MESH,
        )
        cp.start()
        sent.append(cp)
        return cp

    mark("entry")
    loads = []
    for i, (src, dst) in enumerate(
        ((x_hbm, X.at[tp]), (wv_hbm, WV), (wg_hbm, WG), (g_hbm, G.at[tp]), (wo_hbm, WO))
    ):
        cp = pltpu.make_async_copy(src, dst, ls.at[i])
        cp.start()
        loads.append(cp)

    barrier = pltpu.get_barrier_semaphore()
    peers = [at_tp((tp + d) % 8) for d in range(1, 8)]
    peers += [at_x(x + d) for d in range(1, 4)] + [at_z(z + d) for d in range(1, 4)]
    peers += [((sp + 1) % 16, tp), ((sp + 15) % 16, tp)]
    for dev in peers:
        pl.semaphore_signal(barrier, inc=1, device_id=dev, device_id_type=MESH)
    PV[...] = jnp.zeros((T, C), F32)
    PG[...] = jnp.zeros((T, C), F32)
    GA[...] = jnp.zeros((T, C), F32)
    TF[...] = jnp.zeros((32, C), F32)
    TF[0:TAPS, :] = taps_ref[...].astype(F32)
    pl.semaphore_wait(barrier, len(peers))

    jm = ((y + 3) % 4) * 2 + c
    jp = ((y + 1) % 4) * 2 + c
    jo = ((y + 2) % 4) * 2 + c
    LO, HIH = pl.ds(0, 256), pl.ds(256, 256)

    class Gather:
        def __init__(self, buf):
            self.b = buf

        def start(self):
            b = self.b
            self.h1p = rcopy(b.at[tp, LO], b.at[tp, LO], at_y(y + 1))
            self.h1m = rcopy(b.at[tp, HIH], b.at[tp, HIH], at_y(y + 3))
            self.d0 = rcopy(b.at[tp], b.at[tp], partner)
            self.h2p = rcopy(b.at[tp, HIH], b.at[tp, HIH], at_y(y + 1))
            self.h2m = rcopy(b.at[tp, LO], b.at[tp, LO], at_y(y + 3))

        def first(self):
            b = self.b
            self.h1p.wait_recv()
            self.fp = rcopy(b.at[jm, LO], b.at[jm, LO], at_y(y + 1))
            self.d1p = rcopy(b.at[jm, LO], b.at[jm, LO], partner)
            self.h1m.wait_recv()
            self.fm = rcopy(b.at[jp, HIH], b.at[jp, HIH], at_y(y + 3))
            self.d1m = rcopy(b.at[jp, HIH], b.at[jp, HIH], partner)

        def second(self):
            b = self.b
            self.h2p.wait_recv()
            self.d2p = rcopy(b.at[jm, HIH], b.at[jm, HIH], partner)
            self.h2m.wait_recv()
            self.d2m = rcopy(b.at[jp, LO], b.at[jp, LO], partner)

        def third(self):
            b = self.b
            self.fp.wait_recv()
            self.d3p = rcopy(b.at[jo, LO], b.at[jo, LO], partner)
            self.fm.wait_recv()
            self.d3m = rcopy(b.at[jo, HIH], b.at[jo, HIH], partner)

    def mm(buf, pairs, d_even, d_odd, row_even, row_odd, lo, hi):
        def body(i, _):
            e = i % 2
            par = i // 2
            cc = c + par - 2 * c * par
            j = ((y + d_even + e * (d_odd - d_even)) % 4) * 2 + cc
            row = pl.multiple_of(row_even + e * (row_odd - row_even), 256)
            rows = pl.ds(row, 256)
            a = buf[j, rows, :]
            for w, acc in pairs:
                for n in (0, 256):
                    acc[rows, n:n + 256] += dot_nn(a, w[j, :, n:n + 256])
            return 0

        lax.fori_loop(lo, hi, body, 0)

    gx, gg_ = Gather(X), Gather(G)
    vg = ((WV, PV), (WG, PG))
    wo = ((WO, GA),)
    mark("xload")
    loads[0].wait()
    gx.start()
    mark("wload")
    loads[1].wait()
    loads[2].wait()
    mark("x0")
    mm(X, vg, 0, 0, 0, 256, 0, 2)
    gx.d0.wait_recv()
    mm(X, vg, 0, 0, 0, 256, 2, 4)
    mark("x1w")
    gx.first()
    loads[3].wait()
    gg_.start()
    mark("x1")
    mm(X, vg, 3, 1, 0, 256, 0, 2)
    gx.d1p.wait_recv()
    gx.d1m.wait_recv()
    mm(X, vg, 3, 1, 0, 256, 2, 4)
    mark("x2w")
    gx.second()
    mark("x2")
    mm(X, vg, 3, 1, 256, 0, 0, 2)
    gx.d2p.wait_recv()
    gx.d2m.wait_recv()
    mm(X, vg, 3, 1, 256, 0, 2, 4)
    mark("x3w")
    gx.third()
    mark("x3")
    mm(X, vg, 2, 2, 0, 256, 0, 2)
    gx.d3p.wait_recv()
    gx.d3m.wait_recv()
    mm(X, vg, 2, 2, 0, 256, 2, 4)

    mark("hidden")
    def hidden_body(i, _):
        rows = pl.ds(pl.multiple_of(i * 32, 32), 32)
        out_rows = pl.ds(pl.multiple_of(i * 32 + PAD, 16), 32)
        s = sig(PG[rows, :])
        PG[rows, :] = s
        HID[out_rows, :] = (PV[rows, :] * s).astype(BF16).astype(F32)
        return 0

    lax.fori_loop(0, T // 32, hidden_body, 0)

    following, previous = ((sp + 1) % 16, tp), ((sp + 15) % 16, tp)

    def halo_start(buf):
        up = rcopy(buf.at[pl.ds(T, PAD)], buf.at[pl.ds(0, PAD)], following)
        down = rcopy(buf.at[pl.ds(PAD, PAD)], buf.at[pl.ds(T + PAD, PAD)], previous)
        return up, down

    def halo_finish(buf, pair):
        pair[0].wait_recv()
        pair[1].wait_recv()

        @pl.when(sp == 0)
        def _():
            buf[0:PAD, :] = jnp.zeros((PAD, C), F32)

        @pl.when(sp == 15)
        def _():
            buf[T + PAD:T + 2 * PAD, :] = jnp.zeros((PAD, C), F32)

    mark("g0")
    halo = halo_start(HID)
    loads[4].wait()
    mm(G, wo, 0, 0, 0, 256, 0, 2)
    gg_.d0.wait_recv()
    mm(G, wo, 0, 0, 0, 256, 2, 4)
    mark("halo1w")
    halo_finish(HID, halo)
    mark("g1w")
    gg_.first()

    mark("conv")
    R = 64

    def conv_tile(src, r0, cs, flip):
        acc = jnp.zeros((R, 128), F32)
        window = src.at[pl.ds(r0, R + 2 * PAD)]
        for b in range(8):
            v = window[b:b + R + 24, cs:cs + 128]
            for a in range(4):
                o = 8 * a + b
                if o:
                    k = TAPS - o if flip else o - 1
                    acc = acc + TF[k:k + 1, cs:cs + 128] * v[8 * a:8 * a + R]
        return acc

    def conv_body(i, _):
        r0 = pl.multiple_of(i * R, R)
        rows = pl.ds(r0, R)
        s = jnp.zeros((R, 128), F32)
        q = jnp.zeros((R, 128), F32)
        for cs in COLS:
            v = conv_tile(HID, r0, cs, False)
            NRM[rows, cs:cs + 128] = v
            s = s + v
            q = q + v * v
        SA[rows, :] = s
        SQ[rows, :] = q
        return 0

    lax.fori_loop(0, T // R, conv_body, 0)

    def stats_start(e):
        row = lax.broadcasted_iota(jnp.int32, (8, 128), 0)
        dims = (((1,), (1,)), ((), ()))
        tile = lax.dot_general(
            jnp.where(row == 0, 1.0, 0.0).astype(F32), SA[...], dims, precision=HI, preferred_element_type=F32
        ) + lax.dot_general(
            jnp.where(row == 1, 1.0, 0.0).astype(F32), SQ[...], dims, precision=HI, preferred_element_type=F32
        )
        ST[e] = tile
        STR[e, tp] = tile
        return [rcopy(ST.at[e], STR.at[e, tp], at_tp((tp + d) % 8)) for d in range(1, 8)]

    def stats_finish(e, copies):
        for cp in copies:
            cp.wait_recv()
        row = lax.broadcasted_iota(jnp.int32, (64, 256), 0) & 7
        lane = lax.broadcasted_iota(jnp.int32, (64, 256), 1)
        want = jnp.where(lane < 128, 0, 1)
        pick = jnp.where(row == want, 1.0, 0.0).astype(F32)
        for t in range(0, T, 128):
            block = STR[e, :, :, t:t + 128].reshape(64, 128)
            both = lax.dot_general(
                block, pick, (((0,), (0,)), ((), ())), precision=HI, preferred_element_type=F32
            ) * (1.0 / (NB * C))
            if e == 0:
                mean = both[:, :128]
                MEAN[t:t + 128, :] = mean
                INV[t:t + 128, :] = lax.rsqrt(both[:, 128:] - mean * mean + 1e-06)
            else:
                SA[t:t + 128, :] = both[:, :128]
                SQ[t:t + 128, :] = both[:, 128:]

    mark("stats1")
    stats = stats_start(0)
    mark("g1")
    mm(G, wo, 3, 1, 0, 256, 0, 2)
    gg_.d1p.wait_recv()
    gg_.d1m.wait_recv()
    mm(G, wo, 3, 1, 0, 256, 2, 4)
    mark("g2w")
    gg_.second()
    mark("g2")
    mm(G, wo, 3, 1, 256, 0, 0, 2)
    gg_.d2p.wait_recv()
    gg_.d2m.wait_recv()
    mm(G, wo, 3, 1, 256, 0, 2, 4)
    mark("g3w")
    gg_.third()
    mark("g3")
    mm(G, wo, 2, 2, 0, 256, 0, 2)
    gg_.d3p.wait_recv()
    gg_.d3m.wait_recv()
    mm(G, wo, 2, 2, 0, 256, 2, 4)

    mark("stats1w")
    stats_finish(0, stats)
    mark("scaled")
    GP[...] = jnp.zeros((8, C), F32)

    def scaled_body(i, _):
        rows = pl.ds(pl.multiple_of(i * 32, 32), 32)
        m, iv = MEAN[rows, :], INV[rows, :]
        s1 = jnp.zeros((32, 128), F32)
        s2 = jnp.zeros((32, 128), F32)
        for cs in COLS:
            col = slice(cs, cs + 128)
            n = (NRM[rows, col] - m) * iv
            NRM[rows, col] = n
            gain = gain_ref[0:1, col]
            sc = n * gain
            s = sig(sc)
            ACT[rows, col] = (sc * s).astype(BF16)
            gs = GA[rows, col] * s * (1.0 + sc * (1.0 - s))
            GP[:, col] += (gs * n).reshape(4, 8, 128).sum(axis=0)
            gn = gs * gain
            GA[rows, col] = gn
            s1 = s1 + gn
            s2 = s2 + gn * n
        SA[rows, :] = s1
        SQ[rows, :] = s2
        return 0

    lax.fori_loop(0, T // 32, scaled_body, 0)
    mark("stats2")
    stats = stats_start(1)

    at_p = (at_x, at_z)
    at_q = (at_z, at_x)
    me_p = (x, z)
    me_q = (z, x)

    def dw(lhs, units, left, h, dp):
        p = (me_p[h] + dp) % 4

        def body(q, _):
            zz, xx = (q, p) if h == 0 else (p, q)
            s = zz * 4 + xx
            cols = pl.ds(pl.multiple_of((s % 2) * 256, 256), 256)
            r = dot_nn(left(h), lhs[s // 2, :, cols]).astype(BF16)
            for n, u in enumerate(units):
                part[u, h, p, q] = r[n * 256:n * 256 + 256]
            return 0

        lax.fori_loop(0, 4, body, 0)

    class Scatter:
        def __init__(self, u, h):
            self.u, self.h = u, h
            self.p, self.q = me_p[h], me_q[h]

        def blk(self, dp, q0, n=2):
            return part.at[self.u, self.h, (self.p + dp) % 4, pl.ds(q0, n)]

        def s1(self):
            u, h, p = self.u, self.h, self.p
            self.a = rcopy(self.blk(2, 0), r1.at[u, h, 0], at_p[h](p + 1))
            self.b = rcopy(self.blk(2, 2), r1.at[u, h, 1], at_p[h](p + 3))

        def s2i(self):
            u, h, p = self.u, self.h, self.p
            self.c = rcopy(self.blk(1, 2), r2.at[u, h, 0, pl.ds(2, 2)], at_p[h](p + 1))
            self.d = rcopy(self.blk(3, 0), r2.at[u, h, 1, pl.ds(0, 2)], at_p[h](p + 3))

        def add(self, dst_index, rows, sources):
            u, h = self.u, self.h

            def body(i, _):
                rr = pl.ds(pl.multiple_of(rows + i * 32, 32), 32)
                v = part[(u, h) + dst_index + (rr,)].astype(F32)
                for ref, index, off in sources:
                    v = v + ref[index + (pl.ds(pl.multiple_of(off + i * 32, 32), 32),)].astype(F32)
                part[(u, h) + dst_index + (rr,)] = v.astype(BF16)
                return 0

            return body

        def s2d(self):
            u, h, p = self.u, self.h, self.p
            self.a.wait_recv()
            for q in (0, 1):
                lax.fori_loop(0, 8, self.add(((p + 1) % 4, q), 0, [(r1, (u, h, 0, q), 0)]), 0)
            self.e = rcopy(self.blk(1, 0), r2.at[u, h, 0, pl.ds(0, 2)], at_p[h](p + 1))
            self.b.wait_recv()
            for q in (2, 3):
                lax.fori_loop(0, 8, self.add(((p + 3) % 4, q), 0, [(r1, (u, h, 1, q - 2), 0)]), 0)
            self.f = rcopy(self.blk(3, 2), r2.at[u, h, 1, pl.ds(2, 2)], at_p[h](p + 3))

        def p1(self):
            u, h, p, q = self.u, self.h, self.p, self.q
            for cp in (self.c, self.d, self.e, self.f):
                cp.wait_recv()
            for dq in (2, 1, 3, 0):
                qq = (q + dq) % 4
                lax.fori_loop(
                    0, 8, self.add((p, qq), 0, [(r2, (u, h, 0, qq), 0), (r2, (u, h, 1, qq), 0)]), 0
                )
                if dq == 2:
                    src = part.at[u, h, p, qq]
                    self.i = rcopy(src.at[pl.ds(0, 128)], r3.at[u, h, 0], at_q[h](q + 1))
                    self.j = rcopy(src.at[pl.ds(128, 128)], r3.at[u, h, 1], at_q[h](q + 3))

        def p2(self):
            u, h, p, q = self.u, self.h, self.p, self.q
            up, down = (q + 1) % 4, (q + 3) % 4
            self.i.wait_recv()
            lax.fori_loop(0, 4, self.add((p, up), 0, [(r3, (u, h, 0), 0)]), 0)
            self.k = rcopy(part.at[u, h, p, up], r4.at[u, h, 0], at_q[h](q + 1))
            self.j.wait_recv()
            lax.fori_loop(0, 4, self.add((p, down), 128, [(r3, (u, h, 1), 0)]), 0)
            self.l = rcopy(part.at[u, h, p, down], r4.at[u, h, 1], at_q[h](q + 3))

        def finish(self):
            u, h, p, q = self.u, self.h, self.p, self.q
            self.k.wait_recv()
            self.l.wait_recv()
            for i in (0, 128):
                rr = slice(i, i + 128)
                v = (
                    part[u, h, p, q, rr].astype(F32)
                    + r4[u, h, 0, rr].astype(F32)
                    + r4[u, h, 1, rr].astype(F32)
                )
                w_out[u, :, h * 256 + i:h * 256 + i + 128] = v.T.astype(BF16)

    sc = [[Scatter(u, h) for h in (0, 1)] for u in range(3)]

    def produce(lhs, units, left):
        for h in (0, 1):
            dw(lhs, units, left, h, 2)
            for u in units:
                sc[u][h].s1()
        for h in (0, 1):
            dw(lhs, units, left, h, 1)
            dw(lhs, units, left, h, 3)
            for u in units:
                sc[u][h].s2i()
        for h in (0, 1):
            dw(lhs, units, left, h, 0)

    def flip(src, dst, k):
        for cs in COLS:
            dst[cs // 256, k + cs % 256:k + cs % 256 + 128, :] = src[:, cs:cs + 128].T

    flip(ACT, AT, 0)
    produce(G, [0], lambda h: AT[h])
    mark("stats2w")
    stats_finish(1, stats)

    mark("gc")
    def gc_body(i, _):
        rows = pl.ds(pl.multiple_of(i * 32, 32), 32)
        out_rows = pl.ds(pl.multiple_of(i * 32 + PAD, 16), 32)
        f, s, iv = SA[rows, :], SQ[rows, :], INV[rows, :]
        for cs in COLS:
            col = slice(cs, cs + 128)
            GC[out_rows, col] = iv * (GA[rows, col] - f - NRM[rows, col] * s)
        return 0

    lax.fori_loop(0, T // 32, gc_body, 0)
    halo = halo_start(GC)

    mark("taps")
    for cs in COLS:
        def tap_body(i, accs, cs=cs):
            r0 = pl.multiple_of(i * 32, 32)
            window = HID.at[pl.ds(r0, 32 + 2 * PAD)]
            g = GC[pl.ds(pl.multiple_of(r0 + PAD, 16), 32), cs:cs + 128]
            accs = list(accs)
            for b in range(8):
                v = window[b:b + 56, cs:cs + 128]
                for a in range(4):
                    o = 8 * a + b
                    if o:
                        prod = v[8 * a:8 * a + 32] * g
                        accs[o - 1] = accs[o - 1] + prod.reshape(4, 8, 128).sum(axis=0)
            return tuple(accs)

        accs = lax.fori_loop(
            0, T // 32, tap_body, tuple(jnp.zeros((8, 128), F32) for _ in range(TAPS))
        )
        for k, a in enumerate(accs):
            TP[k:k + 1, cs:cs + 128] = jnp.sum(a, axis=0, keepdims=True)
    TP[TAPS:TAPS + 1, :] = jnp.sum(GP[...], axis=0, keepdims=True)

    def small_start(e, me, at):
        TGR[e, me] = TG[e]
        return [rcopy(TG.at[e], TGR.at[e, me], at(me + d)) for d in range(1, 4)]

    def small_finish(e, copies):
        for cp in copies:
            cp.wait_recv()
        v = TGR[e, 0].astype(F32)
        for i in range(1, 4):
            v = v + TGR[e, i].astype(F32)
        return v

    mark("ow_s2d")
    TG[0] = TP[...].astype(BF16)
    small = small_start(0, x, at_x)

    for h in (0, 1):
        sc[0][h].s2d()
    mark("halo2w")
    halo_finish(GC, halo)

    mark("back")
    def back_body(i, _):
        r0 = pl.multiple_of(i * R, R)
        rows = pl.ds(r0, R)
        for cs in COLS:
            col = slice(cs, cs + 128)
            gh = conv_tile(GC, r0, cs, True)
            s = PG[rows, col]
            gv = gh * s
            GV[rows, col] = gv.astype(BF16)
            GG[rows, col] = (gv * PV[rows, col] * (1.0 - s)).astype(BF16)
        return 0

    lax.fori_loop(0, T // R, back_body, 0)

    mark("vg_dw")
    flip(GV, BT, 0)
    flip(GG, BT, 256)
    produce(X, [1, 2], lambda h: BT[h])

    mark("ow_p1")
    for h in (0, 1):
        sc[0][h].p1()
    TG[1] = small_finish(0, small).astype(BF16)
    small = small_start(1, z, at_z)

    mark("partial1")
    for cp in (gg_.h1p, gg_.h1m, gg_.d0, gg_.h2p, gg_.h2m, gg_.fp, gg_.fm, gg_.d1p, gg_.d1m,
               gg_.d2p, gg_.d2m, gg_.d3p, gg_.d3m):
        cp.wait_send()
        done.append(id(cp))

    def partial(parity):
        def body(i, _):
            yy = i // 2
            rows = pl.ds(pl.multiple_of((i % 2) * 256, 256), 256)
            j = yy * 2 + parity
            gv, gt = GV[rows, :], GG[rows, :]
            for n in (0, 256):
                G[parity * 4 + yy, rows, n:n + 256] = (
                    dot_nt(gv, WV[j, n:n + 256, :]) + dot_nt(gt, WG[j, n:n + 256, :])
                ).astype(BF16)
            return 0

        lax.fori_loop(0, 8, body, 0)

    partial(1 - c)
    swap = rcopy(G.at[pl.ds((1 - c) * 4, 4)], PR, partner)
    mark("vg_s2d")
    for u in (1, 2):
        for h in (0, 1):
            sc[u][h].s2d()
    mark("partial2")
    partial(c)
    mark("yadd")
    swap.wait_recv()

    def y_add(block, row0, n, sources):
        def body(i, _):
            rr = pl.ds(pl.multiple_of(row0 + i * 32, 32), 32)
            v = G[block, rr].astype(F32)
            for ref, index, off in sources:
                v = v + ref[index + (pl.ds(pl.multiple_of(off + i * 32, 32), 32),)].astype(F32)
            G[block, rr] = v.astype(BF16)
            return 0

        lax.fori_loop(0, n // 32, body, 0)

    base = c * 4
    y2_, yp_, ym_ = (y + 2) % 4, (y + 1) % 4, (y + 3) % 4
    y_add(base + y2_, 0, T, [(PR, (y2_,), 0)])
    ya = rcopy(G.at[base + y2_, LO], y1.at[0], at_y(y + 1))
    yb = rcopy(G.at[base + y2_, HIH], y1.at[1], at_y(y + 3))
    y_add(base + yp_, 0, T, [(PR, (yp_,), 0)])
    yc = rcopy(G.at[base + yp_, HIH], y2.at[0, HIH], at_y(y + 1))
    y_add(base + ym_, 0, T, [(PR, (ym_,), 0)])
    yd = rcopy(G.at[base + ym_, LO], y2.at[1, LO], at_y(y + 3))
    y_add(base + y, 0, T, [(PR, (y,), 0)])

    mark("ow_p2")
    for h in (0, 1):
        sc[0][h].p2()
    mark("y_s2")
    ya.wait_recv()
    y_add(base + yp_, 0, 256, [(y1, (0,), 0)])
    ye = rcopy(G.at[base + yp_, LO], y2.at[0, LO], at_y(y + 1))
    yb.wait_recv()
    y_add(base + ym_, 256, 256, [(y1, (1,), 0)])
    yf = rcopy(G.at[base + ym_, HIH], y2.at[1, HIH], at_y(y + 3))

    mark("v_p1")
    for h in (0, 1):
        sc[1][h].p1()
    mark("ow_fin")
    for h in (0, 1):
        sc[0][h].finish()
    total = small_finish(1, small)
    taps_out[...] = total
    mark("g_p1")
    for h in (0, 1):
        sc[2][h].p1()
    mark("v_p2")
    for h in (0, 1):
        sc[1][h].p2()
    mark("g_p2")
    for h in (0, 1):
        sc[2][h].p2()
    mark("y_fin")
    for cp in (yc, yd, ye, yf):
        cp.wait_recv()

    def gi_body(i, _):
        rr = pl.ds(pl.multiple_of(i * 32, 32), 32)
        gi_out[rr, :] = (
            G[base + y, rr].astype(F32) + y2[0, rr].astype(F32) + y2[1, rr].astype(F32)
        ).astype(BF16)
        return 0

    lax.fori_loop(0, T // 32, gi_body, 0)
    mark("fin")
    for h in (0, 1):
        sc[1][h].finish()
    for h in (0, 1):
        sc[2][h].finish()
    mark("sends")
    for cp in sent:
        if id(cp) not in done:
            cp.wait_send()
    mark(None)
    assert counter[0] <= N_COPIES, counter[0]


def unpack(gi_in, w_in, small_in, gi, gvw, ggw, gow, gt, gg, b_gi, b_in, b_out, b_small, si, so):
    reads = [
        pltpu.make_async_copy(w_in.at[u], b_in.at[u], si.at[u]) for u in range(3)
    ] + [
        pltpu.make_async_copy(gi_in, b_gi, si.at[3]),
        pltpu.make_async_copy(small_in, b_small, si.at[4]),
    ]
    for cp in reads:
        cp.start()
    writes = []
    for u, dst in enumerate((gow, gvw, ggw)):
        reads[u].wait()
        b_out[u] = b_in[u].astype(F32)
        writes.append(pltpu.make_async_copy(b_out.at[u], dst, so.at[u]))
        writes[-1].start()
    reads[3].wait()
    writes.append(pltpu.make_async_copy(b_gi, gi, so.at[3]))
    writes[-1].start()
    reads[4].wait()
    gt[...] = b_small[0:TAPS]
    gg[...] = b_small[TAPS:TAPS + 1]
    for cp in writes:
        cp.wait()


def local(inputs, w_value, w_gate, taps, ln_gain, w_out, grad_out):
    vm = pltpu.VMEM
    anyspace = pl.BlockSpec(memory_space=pl.ANY)
    in_vmem = pl.BlockSpec(memory_space=pltpu.VMEM)
    shape3 = (NB, C, C)
    gi, w3, small = pl.pallas_call(
        kernel,
        out_shape=(
            jax.ShapeDtypeStruct((T, C), BF16),
            jax.ShapeDtypeStruct((3, 256, C), BF16),
            jax.ShapeDtypeStruct((32, C), F32),
        ),
        in_specs=[anyspace] * 5 + [in_vmem] * 2,
        out_specs=(in_vmem,) * 3,
        scratch_shapes=[
            vm((NB, T, C), BF16), vm((NB, T, C), BF16),
            vm(shape3, BF16), vm(shape3, BF16), vm(shape3, BF16),
            vm((T, C), F32), vm((T, C), F32), vm((T, C), F32), vm((T, C), F32),
            vm((T + 2 * PAD, C), F32), vm((T + 2 * PAD, C), F32),
            vm((T, C), BF16), vm((T, C), BF16), vm((T, C), BF16),
            vm((2, 256, T), BF16), vm((2, 512, T), BF16),
            vm((T, 128), F32), vm((T, 128), F32), vm((T, 128), F32), vm((T, 128), F32),
            vm((32, C), F32),
            vm((2, 8, T), F32), vm((2, NB, 8, T), F32),
            vm((32, C), F32), vm((8, C), F32),
            vm((2, 32, C), BF16), vm((2, 4, 32, C), BF16),
            vm((3, 2, 4, 4, 256, 256), BF16),
            vm((3, 2, 2, 2, 256, 256), BF16),
            vm((3, 2, 2, 4, 256, 256), BF16),
            vm((3, 2, 2, 128, 256), BF16),
            vm((3, 2, 2, 256, 256), BF16),
            vm((4, T, C), BF16),
            vm((2, 256, C), BF16), vm((2, T, C), BF16),
            pltpu.SemaphoreType.DMA((N_COPIES,)),
            pltpu.SemaphoreType.DMA((N_COPIES,)),
            pltpu.SemaphoreType.DMA((5,)),
        ],
        compiler_params=pltpu.CompilerParams(
            collective_id=0, has_side_effects=True, vmem_limit_bytes=67043328
        ),
    )(
        inputs, grad_out, w_value.reshape(shape3), w_gate.reshape(shape3), w_out.reshape(shape3),
        taps, ln_gain.reshape(1, C),
    )
    gi, gvw, ggw, gow, gt, gg = pl.pallas_call(
        unpack,
        out_shape=(
            jax.ShapeDtypeStruct((T, C), BF16),
            jax.ShapeDtypeStruct((256, C), F32),
            jax.ShapeDtypeStruct((256, C), F32),
            jax.ShapeDtypeStruct((256, C), F32),
            jax.ShapeDtypeStruct((TAPS, C), F32),
            jax.ShapeDtypeStruct((1, C), F32),
        ),
        in_specs=[anyspace] * 3,
        out_specs=(anyspace,) * 4 + (in_vmem,) * 2,
        scratch_shapes=[
            vm((T, C), BF16), vm((3, 256, C), BF16), vm((3, 256, C), F32), vm((32, C), F32),
            pltpu.SemaphoreType.DMA((5,)), pltpu.SemaphoreType.DMA((4,)),
        ],
    )(gi, w3, small)
    return gi, gvw, ggw, gow, gt, gg.reshape(C)


def solution(mesh):
    in_specs = (
        P("sp", "tp"), P(None, "tp"), P(None, "tp"), P(None, "tp"), P("tp"), P(None, "tp"), P("sp", "tp"),
    )
    out_specs = (P("sp", "tp"), P("sp", "tp"), P("sp", "tp"), P("sp", "tp"), P(None, "tp"), P("tp"))
    return jax.shard_map(local, mesh=mesh, in_specs=in_specs, out_specs=out_specs, check_vma=False)
```

```python
import jax
import jax.numpy as jnp
from jax import lax
from jax.experimental import pallas as pl
from jax.experimental.pallas import tpu as pltpu
from jax.sharding import PartitionSpec as P

MESH = pl.DeviceIdType.MESH
F32 = jnp.float32
BF16 = jnp.bfloat16
HI = lax.Precision.HIGHEST
T = 512
C = 512
NB = 8
RAD = 15
TAPS = 31
PAD = 16
COLS = (0, 128, 256, 384)
N_COPIES = 160


def sig(v):
    return 1.0 / (1.0 + jnp.exp(-v))


def dot_nn(a, b):
    return lax.dot_general(a, b, (((1,), (0,)), ((), ())), preferred_element_type=F32)


def dot_nt(a, b):
    return lax.dot_general(a, b, (((1,), (1,)), ((), ())), preferred_element_type=F32)


def dot_tn(a, b):
    return lax.dot_general(a, b, (((0,), (0,)), ((), ())), preferred_element_type=F32)


def kernel(
    x_hbm, g_hbm, wv_hbm, wg_hbm, wo_hbm, taps_ref, gain_ref,
    gi_out, w_out, small_out,
    X, G, WV, WG, WO, PV, PG, GA, NRM, HID, GC, ACT, GV, GG, AT, BT,
    SA, SQ, MEAN, INV, TF, ST, STR, TP, GP, TG, TGR,
    part, r1, r2, r3, r4, XA, XB, BTR, VACC, VP, r3v, r4v, PR, y1, y2, ss, rs, ls,
):
    sp = lax.axis_index("sp")
    tp = lax.axis_index("tp")
    z, x = sp // 4, sp % 4
    y, c = tp // 2, tp % 2

    def at_tp(t):
        return (sp, t)

    def at_y(yy):
        return (sp, (yy % 4) * 2 + c)

    def at_x(xx):
        return (z * 4 + xx % 4, tp)

    def at_z(zz):
        return ((zz % 4) * 4 + x, tp)

    partner = at_tp(y * 2 + (1 - c))

    scope = [None]

    def mark(name):
        if scope[0] is not None:
            scope[0].__exit__(None, None, None)
        scope[0] = jax.named_scope(name) if name else None
        if name:
            scope[0].__enter__()

    counter = [0]
    sent = []
    done = []

    def rcopy(src, dst, dev):
        i = counter[0]
        counter[0] += 1
        cp = pltpu.make_async_remote_copy(
            src_ref=src, dst_ref=dst, send_sem=ss.at[i], recv_sem=rs.at[i],
            device_id=dev, device_id_type=MESH,
        )
        cp.start()
        sent.append(cp)
        return cp

    mark("entry")
    loads = []
    for i, (src, dst) in enumerate(
        ((x_hbm, X.at[tp]), (wv_hbm, WV), (wg_hbm, WG), (g_hbm, G.at[tp]), (wo_hbm, WO))
    ):
        cp = pltpu.make_async_copy(src, dst, ls.at[i])
        cp.start()
        loads.append(cp)

    barrier = pltpu.get_barrier_semaphore()
    peers = [at_tp((tp + d) % 8) for d in range(1, 8)]
    peers += [at_x(x + d) for d in range(1, 4)] + [at_z(z + d) for d in range(1, 4)]
    peers += [((sp + 1) % 16, tp), ((sp + 15) % 16, tp)]
    for dev in peers:
        pl.semaphore_signal(barrier, inc=1, device_id=dev, device_id_type=MESH)
    PV[...] = jnp.zeros((T, C), F32)
    PG[...] = jnp.zeros((T, C), F32)
    GA[...] = jnp.zeros((T, C), F32)
    TF[...] = jnp.zeros((32, C), F32)
    TF[0:TAPS, :] = taps_ref[...].astype(F32)
    pl.semaphore_wait(barrier, len(peers))

    jm = ((y + 3) % 4) * 2 + c
    jp = ((y + 1) % 4) * 2 + c
    jo = ((y + 2) % 4) * 2 + c
    LO, HIH = pl.ds(0, 256), pl.ds(256, 256)

    class Gather:
        def __init__(self, buf):
            self.b = buf

        def start(self):
            b = self.b
            self.h1p = rcopy(b.at[tp, LO], b.at[tp, LO], at_y(y + 1))
            self.h1m = rcopy(b.at[tp, HIH], b.at[tp, HIH], at_y(y + 3))
            self.d0 = rcopy(b.at[tp], b.at[tp], partner)
            self.h2p = rcopy(b.at[tp, HIH], b.at[tp, HIH], at_y(y + 1))
            self.h2m = rcopy(b.at[tp, LO], b.at[tp, LO], at_y(y + 3))

        def first(self):
            b = self.b
            self.h1p.wait_recv()
            self.fp = rcopy(b.at[jm, LO], b.at[jm, LO], at_y(y + 1))
            self.d1p = rcopy(b.at[jm, LO], b.at[jm, LO], partner)
            self.h1m.wait_recv()
            self.fm = rcopy(b.at[jp, HIH], b.at[jp, HIH], at_y(y + 3))
            self.d1m = rcopy(b.at[jp, HIH], b.at[jp, HIH], partner)

        def second(self):
            b = self.b
            self.h2p.wait_recv()
            self.d2p = rcopy(b.at[jm, HIH], b.at[jm, HIH], partner)
            self.h2m.wait_recv()
            self.d2m = rcopy(b.at[jp, LO], b.at[jp, LO], partner)

        def third(self):
            b = self.b
            self.fp.wait_recv()
            self.d3p = rcopy(b.at[jo, LO], b.at[jo, LO], partner)
            self.fm.wait_recv()
            self.d3m = rcopy(b.at[jo, HIH], b.at[jo, HIH], partner)

    def mm(buf, pairs, d_even, d_odd, row_even, row_odd, lo, hi):
        def body(i, _):
            e = i % 2
            par = i // 2
            cc = c + par - 2 * c * par
            j = ((y + d_even + e * (d_odd - d_even)) % 4) * 2 + cc
            row = pl.multiple_of(row_even + e * (row_odd - row_even), 256)
            rows = pl.ds(row, 256)
            a = buf[j, rows, :]
            for w, acc in pairs:
                for n in (0, 256):
                    acc[rows, n:n + 256] += dot_nn(a, w[j, :, n:n + 256])
            return 0

        lax.fori_loop(lo, hi, body, 0)

    toks = pl.ds(pl.multiple_of(c * 256, 256), 256)
    ex_a = []
    b0 = counter[0]
    counter[0] += 3

    def ex_b(d, yy):
        return pltpu.make_async_remote_copy(
            src_ref=X.at[pl.ds(2 * yy, 2), toks], dst_ref=XB.at[d - 1, :, toks],
            send_sem=ss.at[b0 + d - 1], recv_sem=rs.at[b0 + d - 1],
            device_id=at_z(z + d), device_id_type=MESH,
        )

    def exchange(yy):
        yy = yy % 4
        for d in (1, 3, 2):
            t = (x + d) % 4
            cols = pl.ds(pl.multiple_of((t % 2) * 256, 256), 256)
            ex_a.append((d, rcopy(X.at[yy * 2 + t // 2, toks, cols], XA.at[d - 1, yy, toks], at_x(t))))

        @pl.when(yy != z)
        def _():
            ex_b((yy + 4 - z) % 4, yy).start()

    def exchange_relay():
        out = []
        for d in (1, 3, 2):
            for dd, cp in ex_a:
                if dd == d:
                    cp.wait_recv()
            out.append(rcopy(XA.at[d - 1, :, toks], XA.at[d - 1, :, toks], partner))
        for d in (1, 3, 2):
            ex_b(d, y).wait_recv()
            out.append(rcopy(XB.at[d - 1, :, toks], XB.at[d - 1, :, toks], partner))
        return out

    gx, gg_ = Gather(X), Gather(G)
    vg = ((WV, PV), (WG, PG))
    wo = ((WO, GA),)
    mark("xload")
    loads[0].wait()
    gx.start()
    mark("wload")
    loads[1].wait()
    loads[2].wait()
    mark("x0")
    mm(X, vg, 0, 0, 0, 256, 0, 2)
    gx.d0.wait_recv()
    exchange(y)
    mm(X, vg, 0, 0, 0, 256, 2, 4)
    mark("x1w")
    gx.first()
    loads[3].wait()
    gg_.start()
    mark("x1")
    mm(X, vg, 3, 1, 0, 256, 0, 2)
    gx.d1p.wait_recv()
    gx.d1m.wait_recv()
    exchange(y + 3 + 2 * c)
    mm(X, vg, 3, 1, 0, 256, 2, 4)
    mark("x2w")
    gx.second()
    mark("x2")
    mm(X, vg, 3, 1, 256, 0, 0, 2)
    gx.d2p.wait_recv()
    gx.d2m.wait_recv()
    mm(X, vg, 3, 1, 256, 0, 2, 4)
    mark("x3w")
    gx.third()
    mark("x3")
    mm(X, vg, 2, 2, 0, 256, 0, 2)
    gx.d3p.wait_recv()
    gx.d3m.wait_recv()
    mm(X, vg, 2, 2, 0, 256, 2, 4)

    mark("hidden")
    def hidden_body(i, _):
        rows = pl.ds(pl.multiple_of(i * 32, 32), 32)
        out_rows = pl.ds(pl.multiple_of(i * 32 + PAD, 16), 32)
        for n, cs in enumerate(COLS):
            col = slice(cs, cs + 128)
            s = sig(PG[rows, col])
            PG[rows, col] = s
            HID[n, out_rows, :] = (PV[rows, col] * s).astype(BF16).astype(F32)
        return 0

    lax.fori_loop(0, T // 32, hidden_body, 0)

    following, previous = ((sp + 1) % 16, tp), ((sp + 15) % 16, tp)

    def halo_start(buf):
        up = rcopy(buf.at[:, pl.ds(T, PAD)], buf.at[:, pl.ds(0, PAD)], following)
        down = rcopy(buf.at[:, pl.ds(PAD, PAD)], buf.at[:, pl.ds(T + PAD, PAD)], previous)
        return up, down

    def halo_finish(buf, pair):
        pair[0].wait_recv()
        pair[1].wait_recv()

        @pl.when(sp == 0)
        def _():
            buf[:, 0:PAD, :] = jnp.zeros((4, PAD, 128), F32)

        @pl.when(sp == 15)
        def _():
            buf[:, T + PAD:T + 2 * PAD, :] = jnp.zeros((4, PAD, 128), F32)

    mark("g0")
    halo = halo_start(HID)
    exchange(y + 1 + 2 * c)
    exchange(y + 2)
    loads[4].wait()
    mm(G, wo, 0, 0, 0, 256, 0, 2)
    gg_.d0.wait_recv()
    mm(G, wo, 0, 0, 0, 256, 2, 4)
    mark("halo1w")
    halo_finish(HID, halo)
    mark("g1w")
    gg_.first()

    mark("conv")
    R = 64

    def conv_tile(src, r0, cs, flip):
        acc = jnp.zeros((R, 128), F32)
        for o in range(1, TAPS + 1):
            k = TAPS - o if flip else o - 1
            acc = acc + TF[k:k + 1, cs:cs + 128] * src[cs // 128, pl.ds(r0 + o, R), :]
        return acc

    def conv_body(i, _):
        r0 = pl.multiple_of(i * R, R)
        rows = pl.ds(r0, R)
        s = jnp.zeros((R, 128), F32)
        q = jnp.zeros((R, 128), F32)
        for cs in COLS:
            v = conv_tile(HID, r0, cs, False)
            NRM[rows, cs:cs + 128] = v
            s = s + v
            q = q + v * v
        SA[rows, :] = s
        SQ[rows, :] = q
        return 0

    lax.fori_loop(0, T // R, conv_body, 0)

    def stats_start(e):
        row = lax.broadcasted_iota(jnp.int32, (8, 128), 0)
        dims = (((1,), (1,)), ((), ()))
        tile = lax.dot_general(
            jnp.where(row == 0, 1.0, 0.0).astype(F32), SA[...], dims, precision=HI, preferred_element_type=F32
        ) + lax.dot_general(
            jnp.where(row == 1, 1.0, 0.0).astype(F32), SQ[...], dims, precision=HI, preferred_element_type=F32
        )
        ST[e] = tile
        STR[e, tp] = tile
        return [rcopy(ST.at[e], STR.at[e, tp], at_tp((tp + d) % 8)) for d in range(1, 8)]

    def stats_finish(e, copies):
        for cp in copies:
            cp.wait_recv()
        row = lax.broadcasted_iota(jnp.int32, (64, 256), 0) & 7
        lane = lax.broadcasted_iota(jnp.int32, (64, 256), 1)
        want = jnp.where(lane < 128, 0, 1)
        pick = jnp.where(row == want, 1.0, 0.0).astype(F32)
        for t in range(0, T, 128):
            block = STR[e, :, :, t:t + 128].reshape(64, 128)
            both = lax.dot_general(
                block, pick, (((0,), (0,)), ((), ())), precision=HI, preferred_element_type=F32
            ) * (1.0 / (NB * C))
            if e == 0:
                mean = both[:, :128]
                MEAN[t:t + 128, :] = mean
                INV[t:t + 128, :] = lax.rsqrt(both[:, 128:] - mean * mean + 1e-06)
            else:
                SA[t:t + 128, :] = both[:, :128]
                SQ[t:t + 128, :] = both[:, 128:]

    mark("stats1")
    stats = stats_start(0)
    mark("g1")
    mm(G, wo, 3, 1, 0, 256, 0, 2)
    gg_.d1p.wait_recv()
    gg_.d1m.wait_recv()
    mm(G, wo, 3, 1, 0, 256, 2, 4)
    mark("g2w")
    gg_.second()
    mark("g2")
    mm(G, wo, 3, 1, 256, 0, 0, 2)
    gg_.d2p.wait_recv()
    gg_.d2m.wait_recv()
    mm(G, wo, 3, 1, 256, 0, 2, 4)
    mark("g3w")
    gg_.third()
    mark("g3")
    mm(G, wo, 2, 2, 0, 256, 0, 2)
    gg_.d3p.wait_recv()
    gg_.d3m.wait_recv()
    mm(G, wo, 2, 2, 0, 256, 2, 4)

    mark("stats1w")
    stats_finish(0, stats)
    mark("scaled")
    GP[...] = jnp.zeros((8, C), F32)

    def scaled_body(i, _):
        rows = pl.ds(pl.multiple_of(i * 32, 32), 32)
        m, iv = MEAN[rows, :], INV[rows, :]
        s1 = jnp.zeros((32, 128), F32)
        s2 = jnp.zeros((32, 128), F32)
        for cs in COLS:
            col = slice(cs, cs + 128)
            n = (NRM[rows, col] - m) * iv
            NRM[rows, col] = n
            gain = gain_ref[0:1, col]
            sc = n * gain
            s = sig(sc)
            ACT[rows, col] = (sc * s).astype(BF16)
            gs = GA[rows, col] * s * (1.0 + sc * (1.0 - s))
            GP[:, col] += (gs * n).reshape(4, 8, 128).sum(axis=0)
            gn = gs * gain
            GA[rows, col] = gn
            s1 = s1 + gn
            s2 = s2 + gn * n
        SA[rows, :] = s1
        SQ[rows, :] = s2
        return 0

    lax.fori_loop(0, T // 32, scaled_body, 0)
    mark("stats2")
    stats = stats_start(1)

    at_p = (at_x, at_z)
    at_q = (at_z, at_x)
    me_p = (x, z)
    me_q = (z, x)

    def dw(lhs, units, left, pair):
        def body(zz, _):
            for e in (0, 1):
                r = dot_nn(left, lhs[zz * 2 + pair, :, e * 256:e * 256 + 256]).astype(BF16)
                for n, u in enumerate(units):
                    a = r[n * 512:n * 512 + 256]
                    b = r[n * 512 + 256:n * 512 + 512]
                    part[u, 0, 2 * pair + e, zz] = a
                    part[u, 1, zz, 2 * pair + e] = b
            return 0

        lax.fori_loop(0, 4, body, 0)

    class Scatter:
        def __init__(self, u, h):
            self.u, self.h = u, h
            self.p, self.q = me_p[h], me_q[h]

        def blk(self, dp, q0, n=2):
            return part.at[self.u, self.h, (self.p + dp) % 4, pl.ds(q0, n)]

        def s1(self):
            u, h, p = self.u, self.h, self.p
            self.a = rcopy(self.blk(2, 0), r1.at[u, h, 0], at_p[h](p + 1))
            self.b = rcopy(self.blk(2, 2), r1.at[u, h, 1], at_p[h](p + 3))

        def s2i(self):
            u, h, p = self.u, self.h, self.p
            self.c = rcopy(self.blk(1, 2), r2.at[u, h, 0, pl.ds(2, 2)], at_p[h](p + 1))
            self.d = rcopy(self.blk(3, 0), r2.at[u, h, 1, pl.ds(0, 2)], at_p[h](p + 3))

        def add(self, dst_index, rows, sources):
            u, h = self.u, self.h

            def body(i, _):
                rr = pl.ds(pl.multiple_of(rows + i * 32, 32), 32)
                v = part[(u, h) + dst_index + (rr,)].astype(F32)
                for ref, index, off in sources:
                    v = v + ref[index + (pl.ds(pl.multiple_of(off + i * 32, 32), 32),)].astype(F32)
                part[(u, h) + dst_index + (rr,)] = v.astype(BF16)
                return 0

            return body

        def s2d(self):
            u, h, p = self.u, self.h, self.p
            self.a.wait_recv()
            for q in (0, 1):
                lax.fori_loop(0, 8, self.add(((p + 1) % 4, q), 0, [(r1, (u, h, 0, q), 0)]), 0)
            self.e = rcopy(self.blk(1, 0), r2.at[u, h, 0, pl.ds(0, 2)], at_p[h](p + 1))
            self.b.wait_recv()
            for q in (2, 3):
                lax.fori_loop(0, 8, self.add(((p + 3) % 4, q), 0, [(r1, (u, h, 1, q - 2), 0)]), 0)
            self.f = rcopy(self.blk(3, 2), r2.at[u, h, 1, pl.ds(2, 2)], at_p[h](p + 3))

        def p1(self):
            u, h, p, q = self.u, self.h, self.p, self.q
            for cp in (self.c, self.d, self.e, self.f):
                cp.wait_recv()
            for dq in (2, 1, 3, 0):
                qq = (q + dq) % 4
                lax.fori_loop(
                    0, 8, self.add((p, qq), 0, [(r2, (u, h, 0, qq), 0), (r2, (u, h, 1, qq), 0)]), 0
                )
                if dq == 2:
                    src = part.at[u, h, p, qq]
                    self.i = rcopy(src.at[pl.ds(0, 128)], r3.at[u, h, 0], at_q[h](q + 1))
                    self.j = rcopy(src.at[pl.ds(128, 128)], r3.at[u, h, 1], at_q[h](q + 3))

        def p2(self):
            u, h, p, q = self.u, self.h, self.p, self.q
            up, down = (q + 1) % 4, (q + 3) % 4
            self.i.wait_recv()
            lax.fori_loop(0, 4, self.add((p, up), 0, [(r3, (u, h, 0), 0)]), 0)
            self.k = rcopy(part.at[u, h, p, up], r4.at[u, h, 0], at_q[h](q + 1))
            self.j.wait_recv()
            lax.fori_loop(0, 4, self.add((p, down), 128, [(r3, (u, h, 1), 0)]), 0)
            self.l = rcopy(part.at[u, h, p, down], r4.at[u, h, 1], at_q[h](q + 3))

        def finish(self):
            u, h, p, q = self.u, self.h, self.p, self.q
            self.k.wait_recv()
            self.l.wait_recv()
            for i in (0, 128):
                rr = slice(i, i + 128)
                v = (
                    part[u, h, p, q, rr].astype(F32)
                    + r4[u, h, 0, rr].astype(F32)
                    + r4[u, h, 1, rr].astype(F32)
                )
                w_out[u, :, h * 256 + i:h * 256 + i + 128] = v.T.astype(BF16)

    sc = [[Scatter(0, h) for h in (0, 1)]]

    def produce(lhs, units, left):
        pair = x // 2
        dw(lhs, units, left[...], 1 - pair)
        for u in units:
            sc[u][0].s1()
        dw(lhs, units, left[...], pair)
        for u in units:
            sc[u][1].s1()

    def flip(src, dst, k):
        for cs in COLS:
            dst[k + cs:k + cs + 128, :] = src[:, cs:cs + 128].T

    flip(ACT, AT, 0)
    produce(G, [0], AT)
    mark("stats2w")
    stats_finish(1, stats)

    mark("gc")
    def gc_body(i, _):
        rows = pl.ds(pl.multiple_of(i * 32, 32), 32)
        out_rows = pl.ds(pl.multiple_of(i * 32 + PAD, 16), 32)
        f, s, iv = SA[rows, :], SQ[rows, :], INV[rows, :]
        for cs in COLS:
            col = slice(cs, cs + 128)
            GC[cs // 128, out_rows, :] = iv * (GA[rows, col] - f - NRM[rows, col] * s)
        return 0

    lax.fori_loop(0, T // 32, gc_body, 0)
    halo = halo_start(GC)
    for h in (0, 1):
        sc[0][h].s2i()

    mark("taps")
    for cs in COLS:
        def tap_body(i, accs, cs=cs):
            r0 = pl.multiple_of(i * 32, 32)
            g = GC[cs // 128, pl.ds(r0 + PAD, 32), :]
            accs = list(accs)
            for o in range(1, TAPS + 1):
                prod = HID[cs // 128, pl.ds(r0 + o, 32), :] * g
                accs[o - 1] = accs[o - 1] + prod.reshape(4, 8, 128).sum(axis=0)
            return tuple(accs)

        accs = lax.fori_loop(
            0, T // 32, tap_body, tuple(jnp.zeros((8, 128), F32) for _ in range(TAPS))
        )
        for k, a in enumerate(accs):
            TP[k:k + 1, cs:cs + 128] = jnp.sum(a, axis=0, keepdims=True)
    TP[TAPS:TAPS + 1, :] = jnp.sum(GP[...], axis=0, keepdims=True)

    def small_start(e, me, at):
        TGR[e, me] = TG[e]
        return [rcopy(TG.at[e], TGR.at[e, me], at(me + d)) for d in range(1, 4)]

    def small_finish(e, copies):
        for cp in copies:
            cp.wait_recv()
        v = TGR[e, 0].astype(F32)
        for i in range(1, 4):
            v = v + TGR[e, i].astype(F32)
        return v

    mark("ow_s2d")
    TG[0] = TP[...].astype(BF16)
    small = small_start(0, x, at_x)

    for h in (0, 1):
        sc[0][h].s2d()
    mark("relay")
    relays = exchange_relay()
    mark("halo2w")
    halo_finish(GC, halo)

    mark("back")
    def back_body(i, _):
        r0 = pl.multiple_of(i * R, R)
        rows = pl.ds(r0, R)
        for cs in COLS:
            col = slice(cs, cs + 128)
            gh = conv_tile(GC, r0, cs, True)
            s = PG[rows, col]
            gv = gh * s
            GV[rows, col] = gv.astype(BF16)
            GG[rows, col] = (gv * PV[rows, col] * (1.0 - s)).astype(BF16)
        return 0

    lax.fori_loop(0, T // R, back_body, 0)

    mark("vg_t")
    for src, k in ((GV, 0), (GG, 256)):
        for cs in COLS:
            r = k + cs % 256
            BT[cs // 256, r:r + 128, :] = src[:, cs:cs + 128].T

    class Spread:
        def __init__(self, h):
            self.h, self.p = h, me_p[h]

        def start(self):
            h, p = self.h, self.p
            own, got = BT.at[h], BTR.at[h]
            nxt, prv = at_p[h](p + 1), at_p[h](p + 3)
            self.h1p = rcopy(own.at[LO], got.at[0, LO], nxt)
            self.h1m = rcopy(own.at[HIH], got.at[2, HIH], prv)
            self.h2p = rcopy(own.at[HIH], got.at[0, HIH], nxt)
            self.h2m = rcopy(own.at[LO], got.at[2, LO], prv)

        def first(self):
            h, p = self.h, self.p
            got = BTR.at[h]
            self.h1p.wait_recv()
            self.fp = rcopy(got.at[0, LO], got.at[1, LO], at_p[h](p + 1))
            self.h1m.wait_recv()
            self.fm = rcopy(got.at[2, HIH], got.at[1, HIH], at_p[h](p + 3))

        def second(self):
            self.h2p.wait_recv()
            self.h2m.wait_recv()

        def third(self):
            self.fp.wait_recv()
            self.fm.wait_recv()

    def own_in(h, q):
        zz, xx = (q, x) if h == 0 else (z, q)
        cols = pl.ds(pl.multiple_of((xx % 2) * 256, 256), 256)
        return X[zz * 2 + xx // 2, :, cols]

    def got_in(h, k, q):
        if h == 0:
            return XA[k, q]
        return XB[k, q // 2, :, pl.ds(pl.multiple_of((q % 2) * 256, 256), 256)]

    def vg_own(h):
        def body(q, _):
            VACC[h, q] = dot_nn(BT[h], own_in(h, q))
            return 0

        lax.fori_loop(0, 4, body, 0)

    def vg_near(h):
        def body(q, _):
            VACC[h, q] += dot_nn(BTR[h, 0], got_in(h, 0, q)) + dot_nn(BTR[h, 2], got_in(h, 2, q))
            return 0

        lax.fori_loop(0, 4, body, 0)

    class Last:
        def __init__(self, h):
            self.h, self.q = h, me_q[h]

        def make(self, dq):
            h = self.h
            qq = (self.q + dq) % 4
            VP[h, qq] = (VACC[h, qq] + dot_nn(BTR[h, 1], got_in(h, 1, qq))).astype(BF16)

        def s1(self):
            h, q = self.h, self.q
            src = VP.at[h, (q + 2) % 4]
            self.i = rcopy(src.at[LO], r3v.at[h, 0], at_q[h](q + 1))
            self.j = rcopy(src.at[HIH], r3v.at[h, 1], at_q[h](q + 3))

        def s2(self):
            h, q = self.h, self.q

            def add(qq, row0, k):
                def body(i, _):
                    rr = pl.ds(pl.multiple_of(row0 + i * 64, 64), 64)
                    fr = pl.ds(pl.multiple_of(i * 64, 64), 64)
                    VP[h, qq, rr] = (VP[h, qq, rr].astype(F32) + r3v[h, k, fr].astype(F32)).astype(BF16)
                    return 0

                lax.fori_loop(0, 4, body, 0)

            up, down = (q + 1) % 4, (q + 3) % 4
            self.i.wait_recv()
            add(up, 0, 0)
            self.k = rcopy(VP.at[h, up], r4v.at[h, 0], at_q[h](q + 1))
            self.j.wait_recv()
            add(down, 256, 1)
            self.l = rcopy(VP.at[h, down], r4v.at[h, 1], at_q[h](q + 3))

        def finish(self):
            h, q = self.h, self.q
            self.k.wait_recv()
            self.l.wait_recv()
            for u in (1, 2):
                for i in (0, 128):
                    r = (u - 1) * 256 + i
                    rr = slice(r, r + 128)
                    v = VP[h, q, rr].astype(F32) + r4v[h, 0, rr].astype(F32) + r4v[h, 1, rr].astype(F32)
                    w_out[u, :, h * 256 + i:h * 256 + i + 128] = v.T.astype(BF16)

    spread = [Spread(0), Spread(1)]
    last = [Last(0), Last(1)]
    for h in (0, 1):
        spread[h].start()
    TG[1] = small_finish(0, small).astype(BF16)
    small = small_start(1, z, at_z)

    mark("partial1")
    for cp in (gg_.h1p, gg_.h1m, gg_.d0, gg_.h2p, gg_.h2m, gg_.fp, gg_.fm, gg_.d1p, gg_.d1m,
               gg_.d2p, gg_.d2m, gg_.d3p, gg_.d3m):
        cp.wait_send()
        done.append(id(cp))

    def partial(parity):
        def body(i, _):
            yy = i // 2
            rows = pl.ds(pl.multiple_of((i % 2) * 256, 256), 256)
            j = yy * 2 + parity
            gv, gt = GV[rows, :], GG[rows, :]
            for n in (0, 256):
                G[parity * 4 + yy, rows, n:n + 256] = (
                    dot_nt(gv, WV[j, n:n + 256, :]) + dot_nt(gt, WG[j, n:n + 256, :])
                ).astype(BF16)
            return 0

        lax.fori_loop(0, 8, body, 0)

    partial(1 - c)
    swap = rcopy(G.at[pl.ds((1 - c) * 4, 4)], PR, partner)
    mark("partial2")
    partial(c)
    mark("yadd")
    swap.wait_recv()

    def y_add(block, row0, n, sources):
        def body(i, _):
            rr = pl.ds(pl.multiple_of(row0 + i * 32, 32), 32)
            v = G[block, rr].astype(F32)
            for ref, index, off in sources:
                v = v + ref[index + (pl.ds(pl.multiple_of(off + i * 32, 32), 32),)].astype(F32)
            G[block, rr] = v.astype(BF16)
            return 0

        lax.fori_loop(0, n // 32, body, 0)

    base = c * 4
    y2_, yp_, ym_ = (y + 2) % 4, (y + 1) % 4, (y + 3) % 4
    y_add(base + y2_, 0, T, [(PR, (y2_,), 0)])
    ya = rcopy(G.at[base + y2_, LO], y1.at[0], at_y(y + 1))
    yb = rcopy(G.at[base + y2_, HIH], y1.at[1], at_y(y + 3))
    y_add(base + yp_, 0, T, [(PR, (yp_,), 0)])
    yc = rcopy(G.at[base + yp_, HIH], y2.at[0, HIH], at_y(y + 1))
    y_add(base + ym_, 0, T, [(PR, (ym_,), 0)])
    yd = rcopy(G.at[base + ym_, LO], y2.at[1, LO], at_y(y + 3))
    y_add(base + y, 0, T, [(PR, (y,), 0)])

    mark("vg_first")
    for h in (0, 1):
        spread[h].first()
    mark("vg_own")
    for h in (0, 1):
        vg_own(h)
    mark("ow_p1")
    for h in (0, 1):
        sc[0][h].p1()
    for cp in relays:
        cp.wait_recv()
    mark("vg_second")
    for h in (0, 1):
        spread[h].second()
    mark("vg_near")
    for h in (0, 1):
        vg_near(h)
    mark("y_s2")
    ya.wait_recv()
    y_add(base + yp_, 0, 256, [(y1, (0,), 0)])
    ye = rcopy(G.at[base + yp_, LO], y2.at[0, LO], at_y(y + 1))
    yb.wait_recv()
    y_add(base + ym_, 256, 256, [(y1, (1,), 0)])
    yf = rcopy(G.at[base + ym_, HIH], y2.at[1, HIH], at_y(y + 3))
    mark("vg_third")
    for h in (0, 1):
        spread[h].third()
    mark("vg_far")
    for h in (0, 1):
        last[h].make(2)
        last[h].s1()
    for dq in (1, 3):
        for h in (0, 1):
            last[h].make(dq)
    mark("ow_p2")
    for h in (0, 1):
        sc[0][h].p2()
    mark("vg_s2")
    for h in (0, 1):
        last[h].s2()
    mark("vg_mine")
    for h in (0, 1):
        last[h].make(0)
    mark("ow_fin")
    for h in (0, 1):
        sc[0][h].finish()
    small_out[...] = small_finish(1, small)
    mark("y_fin")
    for cp in (yc, yd, ye, yf):
        cp.wait_recv()

    def gi_body(i, _):
        rr = pl.ds(pl.multiple_of(i * 32, 32), 32)
        gi_out[rr, :] = (
            G[base + y, rr].astype(F32) + y2[0, rr].astype(F32) + y2[1, rr].astype(F32)
        ).astype(BF16)
        return 0

    lax.fori_loop(0, T // 32, gi_body, 0)
    mark("fin")
    for h in (0, 1):
        last[h].finish()
    mark("sends")
    for cp in sent:
        if id(cp) not in done:
            cp.wait_send()
    for d in (1, 2, 3):
        ex_b(d, (z + d) % 4).wait_send()
    mark(None)
    assert counter[0] <= N_COPIES, counter[0]


def unpack(gi_in, w_in, small_in, gi, gvw, ggw, gow, gt, gg, b_gi, b_in, b_out, b_small, si, so):
    reads = [
        pltpu.make_async_copy(w_in.at[u], b_in.at[u], si.at[u]) for u in range(3)
    ] + [
        pltpu.make_async_copy(gi_in, b_gi, si.at[3]),
        pltpu.make_async_copy(small_in, b_small, si.at[4]),
    ]
    for cp in reads:
        cp.start()
    writes = []
    for u, dst in enumerate((gow, gvw, ggw)):
        reads[u].wait()
        b_out[u] = b_in[u].astype(F32)
        writes.append(pltpu.make_async_copy(b_out.at[u], dst, so.at[u]))
        writes[-1].start()
    reads[3].wait()
    writes.append(pltpu.make_async_copy(b_gi, gi, so.at[3]))
    writes[-1].start()
    reads[4].wait()
    gt[...] = b_small[0:TAPS]
    gg[...] = b_small[TAPS:TAPS + 1]
    for cp in writes:
        cp.wait()


def local(inputs, w_value, w_gate, taps, ln_gain, w_out, grad_out):
    vm = pltpu.VMEM
    anyspace = pl.BlockSpec(memory_space=pl.ANY)
    in_vmem = pl.BlockSpec(memory_space=pltpu.VMEM)
    shape3 = (NB, C, C)
    gi, w3, small = pl.pallas_call(
        kernel,
        out_shape=(
            jax.ShapeDtypeStruct((T, C), BF16),
            jax.ShapeDtypeStruct((3, 256, C), BF16),
            jax.ShapeDtypeStruct((32, C), F32),
        ),
        in_specs=[anyspace] * 5 + [in_vmem] * 2,
        out_specs=(in_vmem,) * 3,
        scratch_shapes=[
            vm((NB, T, C), BF16), vm((NB, T, C), BF16),
            vm(shape3, BF16), vm(shape3, BF16), vm(shape3, BF16),
            vm((T, C), F32), vm((T, C), F32), vm((T, C), F32), vm((T, C), F32),
            vm((4, T + 2 * PAD, 128), F32), vm((4, T + 2 * PAD, 128), F32),
            vm((T, C), BF16), vm((T, C), BF16), vm((T, C), BF16),
            vm((512, T), BF16), vm((2, 512, T), BF16),
            vm((T, 128), F32), vm((T, 128), F32), vm((T, 128), F32), vm((T, 128), F32),
            vm((32, C), F32),
            vm((2, 8, T), F32), vm((2, NB, 8, T), F32),
            vm((32, C), F32), vm((8, C), F32),
            vm((2, 32, C), BF16), vm((2, 4, 32, C), BF16),
            vm((1, 2, 4, 4, 256, 256), BF16),
            vm((1, 2, 2, 2, 256, 256), BF16),
            vm((1, 2, 2, 4, 256, 256), BF16),
            vm((1, 2, 2, 128, 256), BF16),
            vm((1, 2, 2, 256, 256), BF16),
            vm((3, 4, T, 256), BF16), vm((3, 2, T, C), BF16),
            vm((2, 3, 512, T), BF16),
            vm((2, 4, 512, 256), F32), vm((2, 4, 512, 256), BF16),
            vm((2, 2, 256, 256), BF16), vm((2, 2, 512, 256), BF16),
            vm((4, T, C), BF16),
            vm((2, 256, C), BF16), vm((2, T, C), BF16),
            pltpu.SemaphoreType.DMA((N_COPIES,)),
            pltpu.SemaphoreType.DMA((N_COPIES,)),
            pltpu.SemaphoreType.DMA((5,)),
        ],
        compiler_params=pltpu.CompilerParams(
            collective_id=0, has_side_effects=True, vmem_limit_bytes=67043328
        ),
    )(
        inputs, grad_out, w_value.reshape(shape3), w_gate.reshape(shape3), w_out.reshape(shape3),
        taps, ln_gain.reshape(1, C),
    )
    gi, gvw, ggw, gow, gt, gg = pl.pallas_call(
        unpack,
        out_shape=(
            jax.ShapeDtypeStruct((T, C), BF16),
            jax.ShapeDtypeStruct((256, C), F32),
            jax.ShapeDtypeStruct((256, C), F32),
            jax.ShapeDtypeStruct((256, C), F32),
            jax.ShapeDtypeStruct((TAPS, C), F32),
            jax.ShapeDtypeStruct((1, C), F32),
        ),
        in_specs=[anyspace] * 3,
        out_specs=(anyspace,) * 4 + (in_vmem,) * 2,
        scratch_shapes=[
            vm((T, C), BF16), vm((3, 256, C), BF16), vm((3, 256, C), F32), vm((32, C), F32),
            pltpu.SemaphoreType.DMA((5,)), pltpu.SemaphoreType.DMA((4,)),
        ],
    )(gi, w3, small)
    return gi, gvw, ggw, gow, gt, gg.reshape(C)


def solution(mesh):
    in_specs = (
        P("sp", "tp"), P(None, "tp"), P(None, "tp"), P(None, "tp"), P("tp"), P(None, "tp"), P("sp", "tp"),
    )
    out_specs = (P("sp", "tp"), P("sp", "tp"), P("sp", "tp"), P("sp", "tp"), P(None, "tp"), P("tp"))
    return jax.shard_map(local, mesh=mesh, in_specs=in_specs, out_specs=out_specs, check_vma=False)
```

```python
import jax
import jax.numpy as jnp
from jax import lax
from jax.experimental import pallas as pl
from jax.experimental.pallas import tpu as pltpu
from jax.sharding import PartitionSpec as P

MESH = pl.DeviceIdType.MESH
F32 = jnp.float32
BF16 = jnp.bfloat16
HI = lax.Precision.HIGHEST
T = 512
C = 512
NB = 8
RAD = 15
TAPS = 31
PAD = 16
COLS = (0, 128, 256, 384)
N_COPIES = 160


def sig(v):
    return 1.0 / (1.0 + jnp.exp(-v))


def dot_nn(a, b):
    return lax.dot_general(a, b, (((1,), (0,)), ((), ())), preferred_element_type=F32)


def dot_nt(a, b):
    return lax.dot_general(a, b, (((1,), (1,)), ((), ())), preferred_element_type=F32)


def dot_tn(a, b):
    return lax.dot_general(a, b, (((0,), (0,)), ((), ())), preferred_element_type=F32)


def kernel(
    x_hbm, g_hbm, wv_hbm, wg_hbm, wo_hbm, taps_ref, gain_ref,
    gi_out, w_out, small_out,
    X, G, WV, WG, WO, PV, PG, GA, NRM, HID, GC, ACT, GV, GG, AT, BT,
    SA, SQ, MEAN, INV, TF, ST, STR, TP, GP, TG, TG1, TGR,
    part, r1, r2, r3, r4, XA, XB, BTR, VACC, VP, r3v, r4v, PR, y1, y2, ss, rs, ls,
):
    sp = lax.axis_index("sp")
    tp = lax.axis_index("tp")
    z, x = sp // 4, sp % 4
    y, c = tp // 2, tp % 2

    def at_tp(t):
        return (sp, t)

    def at_y(yy):
        return (sp, (yy % 4) * 2 + c)

    def at_x(xx):
        return (z * 4 + xx % 4, tp)

    def at_z(zz):
        return ((zz % 4) * 4 + x, tp)

    partner = at_tp(y * 2 + (1 - c))

    scope = [None]

    def mark(name):
        if scope[0] is not None:
            scope[0].__exit__(None, None, None)
        scope[0] = jax.named_scope(name) if name else None
        if name:
            scope[0].__enter__()

    counter = [0]
    sent = []
    done = []

    def rcopy(src, dst, dev):
        i = counter[0]
        counter[0] += 1
        cp = pltpu.make_async_remote_copy(
            src_ref=src, dst_ref=dst, send_sem=ss.at[i], recv_sem=rs.at[i],
            device_id=dev, device_id_type=MESH,
        )
        cp.start()
        sent.append(cp)
        return cp

    mark("entry")
    loads = []
    for i, (src, dst) in enumerate(
        ((x_hbm, X.at[tp]), (wv_hbm, WV), (wg_hbm, WG), (g_hbm, G.at[tp]), (wo_hbm, WO))
    ):
        cp = pltpu.make_async_copy(src, dst, ls.at[i])
        cp.start()
        loads.append(cp)

    barrier = pltpu.get_barrier_semaphore()
    peers = [at_tp((tp + d) % 8) for d in range(1, 8)]
    peers += [at_x(x + d) for d in range(1, 4)] + [at_z(z + d) for d in range(1, 4)]
    peers += [((sp + 1) % 16, tp), ((sp + 15) % 16, tp)]
    for dev in peers:
        pl.semaphore_signal(barrier, inc=1, device_id=dev, device_id_type=MESH)
    PV[...] = jnp.zeros((T, C), F32)
    PG[...] = jnp.zeros((T, C), F32)
    GA[...] = jnp.zeros((T, C), F32)
    TF[...] = jnp.zeros((32, C), F32)
    TF[0:TAPS, :] = taps_ref[...].astype(F32)
    pl.semaphore_wait(barrier, len(peers))

    jm = ((y + 3) % 4) * 2 + c
    jp = ((y + 1) % 4) * 2 + c
    jo = ((y + 2) % 4) * 2 + c
    LO, HIH = pl.ds(0, 256), pl.ds(256, 256)

    class Gather:
        def __init__(self, buf):
            self.b = buf

        def start(self):
            b = self.b
            self.h1p = rcopy(b.at[tp, LO], b.at[tp, LO], at_y(y + 1))
            self.h1m = rcopy(b.at[tp, HIH], b.at[tp, HIH], at_y(y + 3))
            self.d0 = rcopy(b.at[tp], b.at[tp], partner)
            self.h2p = rcopy(b.at[tp, HIH], b.at[tp, HIH], at_y(y + 1))
            self.h2m = rcopy(b.at[tp, LO], b.at[tp, LO], at_y(y + 3))

        def first(self):
            b = self.b
            self.h1p.wait_recv()
            self.fp = rcopy(b.at[jm, LO], b.at[jm, LO], at_y(y + 1))
            self.d1p = rcopy(b.at[jm, LO], b.at[jm, LO], partner)
            self.h1m.wait_recv()
            self.fm = rcopy(b.at[jp, HIH], b.at[jp, HIH], at_y(y + 3))
            self.d1m = rcopy(b.at[jp, HIH], b.at[jp, HIH], partner)

        def second(self):
            b = self.b
            self.h2p.wait_recv()
            self.d2p = rcopy(b.at[jm, HIH], b.at[jm, HIH], partner)
            self.h2m.wait_recv()
            self.d2m = rcopy(b.at[jp, LO], b.at[jp, LO], partner)

        def third(self):
            b = self.b
            self.fp.wait_recv()
            self.d3p = rcopy(b.at[jo, LO], b.at[jo, LO], partner)
            self.fm.wait_recv()
            self.d3m = rcopy(b.at[jo, HIH], b.at[jo, HIH], partner)

    def mm(buf, pairs, d_even, d_odd, row_even, row_odd, lo, hi):
        def body(i, _):
            e = i % 2
            par = i // 2
            cc = c + par - 2 * c * par
            j = ((y + d_even + e * (d_odd - d_even)) % 4) * 2 + cc
            row = pl.multiple_of(row_even + e * (row_odd - row_even), 256)
            rows = pl.ds(row, 256)
            a = buf[j, rows, :]
            for w, acc in pairs:
                for n in (0, 256):
                    acc[rows, n:n + 256] += dot_nn(a, w[j, :, n:n + 256])
            return 0

        lax.fori_loop(lo, hi, body, 0)

    toks = pl.ds(pl.multiple_of(c * 256, 256), 256)
    ex_a = []
    b0 = counter[0]
    counter[0] += 3

    def ex_b(d, yy):
        return pltpu.make_async_remote_copy(
            src_ref=X.at[pl.ds(2 * yy, 2), toks], dst_ref=XB.at[d - 1, :, toks],
            send_sem=ss.at[b0 + d - 1], recv_sem=rs.at[b0 + d - 1],
            device_id=at_z(z + d), device_id_type=MESH,
        )

    def exchange(yy):
        yy = yy % 4
        for d in (1, 3, 2):
            t = (x + d) % 4
            cols = pl.ds(pl.multiple_of((t % 2) * 256, 256), 256)
            ex_a.append((d, rcopy(X.at[yy * 2 + t // 2, toks, cols], XA.at[d - 1, yy, toks], at_x(t))))

        @pl.when(yy != z)
        def _():
            ex_b((yy + 4 - z) % 4, yy).start()

    def exchange_relay():
        out = []
        for d in (1, 3, 2):
            for dd, cp in ex_a:
                if dd == d:
                    cp.wait_recv()
            out.append(rcopy(XA.at[d - 1, :, toks], XA.at[d - 1, :, toks], partner))
        for d in (1, 3, 2):
            ex_b(d, y).wait_recv()
            out.append(rcopy(XB.at[d - 1, :, toks], XB.at[d - 1, :, toks], partner))
        return out

    gx, gg_ = Gather(X), Gather(G)
    vg = ((WV, PV), (WG, PG))
    wo = ((WO, GA),)
    mark("xload")
    loads[0].wait()
    gx.start()
    mark("wload")
    loads[1].wait()
    loads[2].wait()
    mark("x0")
    mm(X, vg, 0, 0, 0, 256, 0, 2)
    gx.d0.wait_recv()
    exchange(y)
    mm(X, vg, 0, 0, 0, 256, 2, 4)
    mark("x1w")
    gx.first()
    loads[3].wait()
    gg_.start()
    mark("x1")
    mm(X, vg, 3, 1, 0, 256, 0, 2)
    gx.d1p.wait_recv()
    gx.d1m.wait_recv()
    exchange(y + 3 + 2 * c)
    mm(X, vg, 3, 1, 0, 256, 2, 4)
    mark("x2w")
    gx.second()
    mark("x2")
    mm(X, vg, 3, 1, 256, 0, 0, 2)
    gx.d2p.wait_recv()
    gx.d2m.wait_recv()
    mm(X, vg, 3, 1, 256, 0, 2, 4)
    mark("x3w")
    gx.third()
    mark("x3")
    mm(X, vg, 2, 2, 0, 256, 0, 2)
    gx.d3p.wait_recv()
    gx.d3m.wait_recv()
    mm(X, vg, 2, 2, 0, 256, 2, 4)

    mark("hidden")
    def hidden_body(i, _):
        rows = pl.ds(pl.multiple_of(i * 32, 32), 32)
        out_rows = pl.ds(pl.multiple_of(i * 32 + PAD, 16), 32)
        for n, cs in enumerate(COLS):
            col = slice(cs, cs + 128)
            s = sig(PG[rows, col])
            PG[rows, col] = s
            HID[n, out_rows, :] = (PV[rows, col] * s).astype(BF16).astype(F32)
        return 0

    lax.fori_loop(0, T // 32, hidden_body, 0)

    following, previous = ((sp + 1) % 16, tp), ((sp + 15) % 16, tp)

    def halo_start(buf):
        up = rcopy(buf.at[:, pl.ds(T, PAD)], buf.at[:, pl.ds(0, PAD)], following)
        down = rcopy(buf.at[:, pl.ds(PAD, PAD)], buf.at[:, pl.ds(T + PAD, PAD)], previous)
        return up, down

    def halo_finish(buf, pair):
        pair[0].wait_recv()
        pair[1].wait_recv()

        @pl.when(sp == 0)
        def _():
            buf[:, 0:PAD, :] = jnp.zeros((4, PAD, 128), F32)

        @pl.when(sp == 15)
        def _():
            buf[:, T + PAD:T + 2 * PAD, :] = jnp.zeros((4, PAD, 128), F32)

    mark("g0")
    halo = halo_start(HID)
    exchange(y + 1 + 2 * c)
    exchange(y + 2)
    loads[4].wait()
    mm(G, wo, 0, 0, 0, 256, 0, 2)
    gg_.d0.wait_recv()
    mm(G, wo, 0, 0, 0, 256, 2, 4)
    mark("halo1w")
    halo_finish(HID, halo)
    mark("g1w")
    gg_.first()

    mark("conv")
    R = 64

    def conv_tile(src, r0, cs, flip):
        acc = jnp.zeros((R, 128), F32)
        for o in range(1, TAPS + 1):
            k = TAPS - o if flip else o - 1
            acc = acc + TF[k:k + 1, cs:cs + 128] * src[cs // 128, pl.ds(r0 + o, R), :]
        return acc

    def conv_body(i, _):
        r0 = pl.multiple_of(i * R, R)
        rows = pl.ds(r0, R)
        s = jnp.zeros((R, 128), F32)
        q = jnp.zeros((R, 128), F32)
        for cs in COLS:
            v = conv_tile(HID, r0, cs, False)
            NRM[rows, cs:cs + 128] = v
            s = s + v
            q = q + v * v
        SA[rows, :] = s
        SQ[rows, :] = q
        return 0

    lax.fori_loop(0, T // R, conv_body, 0)

    def stats_start(e):
        row = lax.broadcasted_iota(jnp.int32, (8, 128), 0)
        dims = (((1,), (1,)), ((), ()))
        tile = lax.dot_general(
            jnp.where(row == 0, 1.0, 0.0).astype(F32), SA[...], dims, precision=HI, preferred_element_type=F32
        ) + lax.dot_general(
            jnp.where(row == 1, 1.0, 0.0).astype(F32), SQ[...], dims, precision=HI, preferred_element_type=F32
        )
        ST[e] = tile
        STR[e, tp] = tile
        return [rcopy(ST.at[e], STR.at[e, tp], at_tp((tp + d) % 8)) for d in range(1, 8)]

    def stats_finish(e, copies):
        for cp in copies:
            cp.wait_recv()
        row = lax.broadcasted_iota(jnp.int32, (64, 256), 0) & 7
        lane = lax.broadcasted_iota(jnp.int32, (64, 256), 1)
        want = jnp.where(lane < 128, 0, 1)
        pick = jnp.where(row == want, 1.0, 0.0).astype(F32)
        for t in range(0, T, 128):
            block = STR[e, :, :, t:t + 128].reshape(64, 128)
            both = lax.dot_general(
                block, pick, (((0,), (0,)), ((), ())), precision=HI, preferred_element_type=F32
            ) * (1.0 / (NB * C))
            if e == 0:
                mean = both[:, :128]
                MEAN[t:t + 128, :] = mean
                INV[t:t + 128, :] = lax.rsqrt(both[:, 128:] - mean * mean + 1e-06)
            else:
                SA[t:t + 128, :] = both[:, :128]
                SQ[t:t + 128, :] = both[:, 128:]

    mark("stats1")
    stats = stats_start(0)
    mark("g1")
    mm(G, wo, 3, 1, 0, 256, 0, 2)
    gg_.d1p.wait_recv()
    gg_.d1m.wait_recv()
    mm(G, wo, 3, 1, 0, 256, 2, 4)
    mark("g2w")
    gg_.second()
    mark("g2")
    mm(G, wo, 3, 1, 256, 0, 0, 2)
    gg_.d2p.wait_recv()
    gg_.d2m.wait_recv()
    mm(G, wo, 3, 1, 256, 0, 2, 4)
    mark("g3w")
    gg_.third()
    mark("g3")
    mm(G, wo, 2, 2, 0, 256, 0, 2)
    gg_.d3p.wait_recv()
    gg_.d3m.wait_recv()
    mm(G, wo, 2, 2, 0, 256, 2, 4)

    mark("stats1w")
    stats_finish(0, stats)
    mark("scaled")
    GP[...] = jnp.zeros((8, C), F32)

    def scaled_body(i, _):
        rows = pl.ds(pl.multiple_of(i * 32, 32), 32)
        m, iv = MEAN[rows, :], INV[rows, :]
        s1 = jnp.zeros((32, 128), F32)
        s2 = jnp.zeros((32, 128), F32)
        for cs in COLS:
            col = slice(cs, cs + 128)
            n = (NRM[rows, col] - m) * iv
            NRM[rows, col] = n
            gain = gain_ref[0:1, col]
            sc = n * gain
            s = sig(sc)
            ACT[rows, col] = (sc * s).astype(BF16)
            gs = GA[rows, col] * s * (1.0 + sc * (1.0 - s))
            GP[:, col] += (gs * n).reshape(4, 8, 128).sum(axis=0)
            gn = gs * gain
            GA[rows, col] = gn
            s1 = s1 + gn
            s2 = s2 + gn * n
        SA[rows, :] = s1
        SQ[rows, :] = s2
        return 0

    lax.fori_loop(0, T // 32, scaled_body, 0)
    mark("stats2")
    stats = stats_start(1)

    at_p = (at_x, at_z)
    at_q = (at_z, at_x)
    me_p = (x, z)
    me_q = (z, x)

    def dw(lhs, units, left, pair):
        def body(zz, _):
            for e in (0, 1):
                r = dot_nn(left, lhs[zz * 2 + pair, :, e * 256:e * 256 + 256]).astype(BF16)
                for n, u in enumerate(units):
                    a = r[n * 512:n * 512 + 256]
                    b = r[n * 512 + 256:n * 512 + 512]
                    part[u, 0, 2 * pair + e, zz] = a
                    part[u, 1, zz, 2 * pair + e] = b
            return 0

        lax.fori_loop(0, 4, body, 0)

    class Scatter:
        def __init__(self, u, h):
            self.u, self.h = u, h
            self.p, self.q = me_p[h], me_q[h]

        def blk(self, dp, q0, n=2):
            return part.at[self.u, self.h, (self.p + dp) % 4, pl.ds(q0, n)]

        def s1(self):
            u, h, p = self.u, self.h, self.p
            self.a = rcopy(self.blk(2, 0), r1.at[u, h, 0], at_p[h](p + 1))
            self.b = rcopy(self.blk(2, 2), r1.at[u, h, 1], at_p[h](p + 3))

        def s2i(self):
            u, h, p = self.u, self.h, self.p
            self.c = rcopy(self.blk(1, 2), r2.at[u, h, 0, pl.ds(2, 2)], at_p[h](p + 1))
            self.d = rcopy(self.blk(3, 0), r2.at[u, h, 1, pl.ds(0, 2)], at_p[h](p + 3))

        def add(self, dst_index, rows, sources):
            u, h = self.u, self.h

            def body(i, _):
                rr = pl.ds(pl.multiple_of(rows + i * 32, 32), 32)
                v = part[(u, h) + dst_index + (rr,)].astype(F32)
                for ref, index, off in sources:
                    v = v + ref[index + (pl.ds(pl.multiple_of(off + i * 32, 32), 32),)].astype(F32)
                part[(u, h) + dst_index + (rr,)] = v.astype(BF16)
                return 0

            return body

        def s2d(self):
            u, h, p = self.u, self.h, self.p
            self.a.wait_recv()
            for q in (0, 1):
                lax.fori_loop(0, 8, self.add(((p + 1) % 4, q), 0, [(r1, (u, h, 0, q), 0)]), 0)
            self.e = rcopy(self.blk(1, 0), r2.at[u, h, 0, pl.ds(0, 2)], at_p[h](p + 1))
            self.b.wait_recv()
            for q in (2, 3):
                lax.fori_loop(0, 8, self.add(((p + 3) % 4, q), 0, [(r1, (u, h, 1, q - 2), 0)]), 0)
            self.f = rcopy(self.blk(3, 2), r2.at[u, h, 1, pl.ds(2, 2)], at_p[h](p + 3))

        def p1(self):
            u, h, p, q = self.u, self.h, self.p, self.q
            for cp in (self.c, self.d, self.e, self.f):
                cp.wait_recv()
            for dq in (2, 1, 3, 0):
                qq = (q + dq) % 4
                lax.fori_loop(
                    0, 8, self.add((p, qq), 0, [(r2, (u, h, 0, qq), 0), (r2, (u, h, 1, qq), 0)]), 0
                )
                if dq == 2:
                    src = part.at[u, h, p, qq]
                    self.i = rcopy(src.at[pl.ds(0, 128)], r3.at[u, h, 0], at_q[h](q + 1))
                    self.j = rcopy(src.at[pl.ds(128, 128)], r3.at[u, h, 1], at_q[h](q + 3))

        def p2(self):
            u, h, p, q = self.u, self.h, self.p, self.q
            up, down = (q + 1) % 4, (q + 3) % 4
            self.i.wait_recv()
            lax.fori_loop(0, 4, self.add((p, up), 0, [(r3, (u, h, 0), 0)]), 0)
            self.k = rcopy(part.at[u, h, p, up], r4.at[u, h, 0], at_q[h](q + 1))
            self.j.wait_recv()
            lax.fori_loop(0, 4, self.add((p, down), 128, [(r3, (u, h, 1), 0)]), 0)
            self.l = rcopy(part.at[u, h, p, down], r4.at[u, h, 1], at_q[h](q + 3))

        def finish(self):
            u, h, p, q = self.u, self.h, self.p, self.q
            self.k.wait_recv()
            self.l.wait_recv()
            for i in (0, 128):
                rr = slice(i, i + 128)
                v = (
                    part[u, h, p, q, rr].astype(F32)
                    + r4[u, h, 0, rr].astype(F32)
                    + r4[u, h, 1, rr].astype(F32)
                )
                w_out[u, :, h * 256 + i:h * 256 + i + 128] = v.T.astype(BF16)

    sc = [[Scatter(0, h) for h in (0, 1)]]

    def flipped(src, n):
        eye = (
            lax.broadcasted_iota(jnp.int32, (256, 256), 0) == lax.broadcasted_iota(jnp.int32, (256, 256), 1)
        ).astype(F32).astype(BF16)
        return dot_nt(eye, src[:, n:n + 256]).astype(BF16)

    for n in (0, 256):
        AT[n:n + 256, :] = flipped(ACT, n)
    dw(G, [0], AT[...], 1 - x // 2)
    sc[0][0].s1()
    mark("ow_dw2")
    dw(G, [0], AT[...], x // 2)
    mark("stats2w")
    stats_finish(1, stats)

    mark("gc")
    def gc_body(i, _):
        rows = pl.ds(pl.multiple_of(i * 32, 32), 32)
        out_rows = pl.ds(pl.multiple_of(i * 32 + PAD, 16), 32)
        f, s, iv = SA[rows, :], SQ[rows, :], INV[rows, :]
        for cs in COLS:
            col = slice(cs, cs + 128)
            GC[cs // 128, out_rows, :] = iv * (GA[rows, col] - f - NRM[rows, col] * s)
        return 0

    lax.fori_loop(0, T // 32, gc_body, 0)
    halo = halo_start(GC)
    sc[0][1].s1()
    for h in (0, 1):
        sc[0][h].s2i()

    mark("taps")
    for cs in COLS:
        def tap_body(i, accs, cs=cs):
            r0 = pl.multiple_of(i * 32, 32)
            g = GC[cs // 128, pl.ds(r0 + PAD, 32), :]
            accs = list(accs)
            for o in range(1, TAPS + 1):
                prod = HID[cs // 128, pl.ds(r0 + o, 32), :] * g
                accs[o - 1] = accs[o - 1] + prod.reshape(4, 8, 128).sum(axis=0)
            return tuple(accs)

        accs = lax.fori_loop(
            0, T // 32, tap_body, tuple(jnp.zeros((8, 128), F32) for _ in range(TAPS))
        )
        for k, a in enumerate(accs):
            TP[k:k + 1, cs:cs + 128] = jnp.sum(a, axis=0, keepdims=True)
    TP[TAPS:TAPS + 1, :] = jnp.sum(GP[...], axis=0, keepdims=True)

    def small_send(e, src, me, at):
        TGR[e, me] = src(me)[...]
        return [rcopy(src((me + d) % 4), TGR.at[e, me], at(me + d)) for d in (1, 3, 2)]

    def small_sum(e, copies):
        for cp in copies:
            cp.wait_recv()
        v = TGR[e, 0].astype(F32)
        for i in range(1, 4):
            v = v + TGR[e, i].astype(F32)
        return v.astype(BF16)

    for t in range(4):
        TG[t] = TP[:, t * 128:t * 128 + 128].astype(BF16)
    small = small_send(0, lambda t: TG.at[t], x, at_x)
    mark("relay")
    relays = exchange_relay()
    mark("halo2w")
    halo_finish(GC, halo)

    mark("back")
    def back_body(i, _):
        r0 = pl.multiple_of(i * R, R)
        rows = pl.ds(r0, R)
        for cs in COLS:
            col = slice(cs, cs + 128)
            gh = conv_tile(GC, r0, cs, True)
            s = PG[rows, col]
            gv = gh * s
            GV[rows, col] = gv.astype(BF16)
            GG[rows, col] = (gv * PV[rows, col] * (1.0 - s)).astype(BF16)
        return 0

    lax.fori_loop(0, T // R, back_body, 0)

    mark("vg_t")
    for n in (0, 256):
        BT[n // 256, 0:256, :] = flipped(GV, n)

    class Spread:
        def __init__(self, h, u):
            self.h, self.p = h, me_p[h]
            self.lo, self.hi = pl.ds(u * 256, 128), pl.ds(u * 256 + 128, 128)

        def start(self):
            h, p, lo, hi = self.h, self.p, self.lo, self.hi
            own, got = BT.at[h], BTR.at[h]
            nxt, prv = at_p[h](p + 1), at_p[h](p + 3)
            self.h1p = rcopy(own.at[lo], got.at[0, lo], nxt)
            self.h1m = rcopy(own.at[hi], got.at[2, hi], prv)
            self.h2p = rcopy(own.at[hi], got.at[0, hi], nxt)
            self.h2m = rcopy(own.at[lo], got.at[2, lo], prv)

        def first(self):
            h, p, lo, hi = self.h, self.p, self.lo, self.hi
            got = BTR.at[h]
            self.h1p.wait_recv()
            self.fp = rcopy(got.at[0, lo], got.at[1, lo], at_p[h](p + 1))
            self.h1m.wait_recv()
            self.fm = rcopy(got.at[2, hi], got.at[1, hi], at_p[h](p + 3))

        def second(self):
            self.h2p.wait_recv()
            self.h2m.wait_recv()

        def third(self):
            self.fp.wait_recv()
            self.fm.wait_recv()

    def own_in(h, q):
        zz, xx = (q, x) if h == 0 else (z, q)
        cols = pl.ds(pl.multiple_of((xx % 2) * 256, 256), 256)
        return X[zz * 2 + xx // 2, :, cols]

    def got_in(h, k, q):
        if h == 0:
            return XA[k, q]
        return XB[k, q // 2, :, pl.ds(pl.multiple_of((q % 2) * 256, 256), 256)]

    def vg_own(h):
        def body(q, _):
            VACC[h, q] = dot_nn(BT[h], own_in(h, q))
            return 0

        lax.fori_loop(0, 4, body, 0)

    def vg_near(h, u):
        rows = pl.ds(u * 256, 256)

        def body(q, _):
            VACC[h, q, rows] += dot_nn(BTR[h, 0, rows], got_in(h, 0, q)) + dot_nn(BTR[h, 2, rows], got_in(h, 2, q))
            return 0

        lax.fori_loop(0, 4, body, 0)

    class Last:
        def __init__(self, h, u):
            self.h, self.u, self.q = h, u, me_q[h]
            self.rows = pl.ds(u * 256, 256)

        def make(self, dq):
            h, rows = self.h, self.rows
            qq = (self.q + dq) % 4
            VP[h, qq, rows] = (VACC[h, qq, rows] + dot_nn(BTR[h, 1, rows], got_in(h, 1, qq))).astype(BF16)

        def s1(self):
            h, u, q = self.h, self.u, self.q
            src = VP.at[h, (q + 2) % 4]
            self.i = rcopy(src.at[pl.ds(u * 256, 128)], r3v.at[h, u, 0], at_q[h](q + 1))
            self.j = rcopy(src.at[pl.ds(u * 256 + 128, 128)], r3v.at[h, u, 1], at_q[h](q + 3))

        def s2(self):
            h, u, q, rows = self.h, self.u, self.q, self.rows

            def add(qq, row0, k):
                def body(i, _):
                    rr = pl.ds(pl.multiple_of(row0 + i * 64, 64), 64)
                    fr = pl.ds(pl.multiple_of(i * 64, 64), 64)
                    VP[h, qq, rr] = (VP[h, qq, rr].astype(F32) + r3v[h, u, k, fr].astype(F32)).astype(BF16)
                    return 0

                lax.fori_loop(0, 2, body, 0)

            up, down = (q + 1) % 4, (q + 3) % 4
            self.i.wait_recv()
            add(up, u * 256, 0)
            self.k = rcopy(VP.at[h, up, rows], r4v.at[h, 0, rows], at_q[h](q + 1))
            self.j.wait_recv()
            add(down, u * 256 + 128, 1)
            self.l = rcopy(VP.at[h, down, rows], r4v.at[h, 1, rows], at_q[h](q + 3))

        def finish(self):
            h, u, q = self.h, self.u, self.q
            self.k.wait_recv()
            self.l.wait_recv()
            for i in (0, 128):
                rr = slice(u * 256 + i, u * 256 + i + 128)
                v = VP[h, q, rr].astype(F32) + r4v[h, 0, rr].astype(F32) + r4v[h, 1, rr].astype(F32)
                w_out[u + 1, :, h * 256 + i:h * 256 + i + 128] = v.T.astype(BF16)

    spread = [[Spread(0, u), Spread(1, u)] for u in (0, 1)]
    last = [[Last(0, u), Last(1, u)] for u in (0, 1)]
    for h in (0, 1):
        spread[0][h].start()
    for n in (0, 256):
        BT[n // 256, 256:512, :] = flipped(GG, n)

    mark("partial1")
    for cp in (gg_.h1p, gg_.h1m, gg_.d0, gg_.h2p, gg_.h2m, gg_.fp, gg_.fm, gg_.d1p, gg_.d1m,
               gg_.d2p, gg_.d2m, gg_.d3p, gg_.d3m):
        cp.wait_send()
        done.append(id(cp))

    def partial(parity):
        def body(i, _):
            yy = i // 2
            rows = pl.ds(pl.multiple_of((i % 2) * 256, 256), 256)
            j = yy * 2 + parity
            gv, gt = GV[rows, :], GG[rows, :]
            for n in (0, 256):
                G[parity * 4 + yy, rows, n:n + 256] = (
                    dot_nt(gv, WV[j, n:n + 256, :]) + dot_nt(gt, WG[j, n:n + 256, :])
                ).astype(BF16)
            return 0

        lax.fori_loop(0, 8, body, 0)

    partial(1 - c)
    swap = rcopy(G.at[pl.ds((1 - c) * 4, 4)], PR, partner)
    mark("v_first")
    for h in (0, 1):
        spread[0][h].first()
    for h in (0, 1):
        spread[1][h].start()
    mark("partial2")
    partial(c)
    mark("yadd")
    swap.wait_recv()

    def y_add(block, row0, n, sources):
        def body(i, _):
            rr = pl.ds(pl.multiple_of(row0 + i * 32, 32), 32)
            v = G[block, rr].astype(F32)
            for ref, index, off in sources:
                v = v + ref[index + (pl.ds(pl.multiple_of(off + i * 32, 32), 32),)].astype(F32)
            G[block, rr] = v.astype(BF16)
            return 0

        lax.fori_loop(0, n // 32, body, 0)

    base = c * 4
    y2_, yp_, ym_ = (y + 2) % 4, (y + 1) % 4, (y + 3) % 4
    y_add(base + y2_, 0, T, [(PR, (y2_,), 0)])
    ya = rcopy(G.at[base + y2_, LO], y1.at[0], at_y(y + 1))
    yb = rcopy(G.at[base + y2_, HIH], y1.at[1], at_y(y + 3))
    y_add(base + yp_, 0, T, [(PR, (yp_,), 0)])
    yc = rcopy(G.at[base + yp_, HIH], y2.at[0, HIH], at_y(y + 1))
    y_add(base + ym_, 0, T, [(PR, (ym_,), 0)])
    yd = rcopy(G.at[base + ym_, LO], y2.at[1, LO], at_y(y + 3))
    y_add(base + y, 0, T, [(PR, (y,), 0)])

    mark("vg_own")
    for h in (0, 1):
        vg_own(h)
    mark("g_first")
    for h in (0, 1):
        spread[1][h].first()
    mark("ow_s2d")
    for h in (0, 1):
        sc[0][h].s2d()
    for cp in relays:
        cp.wait_recv()
    mark("v_near")
    for h in (0, 1):
        spread[0][h].second()
    for h in (0, 1):
        vg_near(h, 0)
    mark("v_third")
    for h in (0, 1):
        spread[0][h].third()
    mark("v_far")
    for h in (0, 1):
        last[0][h].make(2)
        last[0][h].s1()
    for dq in (1, 3, 0):
        for h in (0, 1):
            last[0][h].make(dq)
    mark("y_s2")
    ya.wait_recv()
    y_add(base + yp_, 0, 256, [(y1, (0,), 0)])
    ye = rcopy(G.at[base + yp_, LO], y2.at[0, LO], at_y(y + 1))
    yb.wait_recv()
    y_add(base + ym_, 256, 256, [(y1, (1,), 0)])
    yf = rcopy(G.at[base + ym_, HIH], y2.at[1, HIH], at_y(y + 3))
    mark("small")
    TG1[0] = small_sum(0, small)
    small = small_send(1, lambda t: TG1.at[0], z, at_z)
    mark("g_second")
    for h in (0, 1):
        spread[1][h].second()
    mark("g_near")
    for h in (0, 1):
        vg_near(h, 1)
    mark("g_third")
    for h in (0, 1):
        spread[1][h].third()
    mark("g_far")
    for h in (0, 1):
        last[1][h].make(2)
        last[1][h].s1()
    for dq in (1, 3, 0):
        for h in (0, 1):
            last[1][h].make(dq)
    mark("ow_p1")
    for h in (0, 1):
        sc[0][h].p1()
    TG1[1] = small_sum(1, small)
    small = small_send(2, lambda t: TG1.at[1], x, at_x)
    mark("v_s2")
    for h in (0, 1):
        last[0][h].s2()
    mark("g_s2")
    for h in (0, 1):
        last[1][h].s2()
    mark("ow_p2")
    for h in (0, 1):
        sc[0][h].p2()
    for cp in small:
        cp.wait_recv()
    for t in range(4):
        small_out[:, t * 128:t * 128 + 128] = TGR[2, t].astype(F32)
    mark("y_fin")
    for cp in (yc, yd, ye, yf):
        cp.wait_recv()

    def gi_body(i, _):
        rr = pl.ds(pl.multiple_of(i * 32, 32), 32)
        gi_out[rr, :] = (
            G[base + y, rr].astype(F32) + y2[0, rr].astype(F32) + y2[1, rr].astype(F32)
        ).astype(BF16)
        return 0

    lax.fori_loop(0, T // 32, gi_body, 0)
    mark("fin")
    for h in (0, 1):
        last[0][h].finish()
    mark("g_fin")
    for h in (0, 1):
        last[1][h].finish()
    mark("ow_fin")
    for h in (0, 1):
        sc[0][h].finish()
    mark("sends")
    for cp in sent:
        if id(cp) not in done:
            cp.wait_send()
    for d in (1, 2, 3):
        ex_b(d, (z + d) % 4).wait_send()
    mark(None)
    assert counter[0] <= N_COPIES, counter[0]


def unpack(gi_in, w_in, small_in, gi, gvw, ggw, gow, gt, gg, b_out, so):
    writes = [pltpu.make_async_copy(gi_in, gi, so.at[3])]
    writes[0].start()
    for u, dst in enumerate((gow, gvw, ggw)):
        b_out[u] = w_in[u].astype(F32)
        writes.append(pltpu.make_async_copy(b_out.at[u], dst, so.at[u]))
        writes[-1].start()
    gt[...] = small_in[0:TAPS]
    gg[...] = small_in[TAPS:TAPS + 1]
    for cp in writes:
        cp.wait()


def local(inputs, w_value, w_gate, taps, ln_gain, w_out, grad_out):
    vm = pltpu.VMEM
    anyspace = pl.BlockSpec(memory_space=pl.ANY)
    in_vmem = pl.BlockSpec(memory_space=pltpu.VMEM)
    shape3 = (NB, C, C)
    gi, w3, small = pl.pallas_call(
        kernel,
        out_shape=(
            vm((T, C), BF16),
            vm((3, 256, C), BF16),
            vm((32, C), F32),
        ),
        in_specs=[anyspace] * 5 + [in_vmem] * 2,
        out_specs=(in_vmem,) * 3,
        scratch_shapes=[
            vm((NB, T, C), BF16), vm((NB, T, C), BF16),
            vm(shape3, BF16), vm(shape3, BF16), vm(shape3, BF16),
            vm((T, C), F32), vm((T, C), F32), vm((T, C), F32), vm((T, C), F32),
            vm((4, T + 2 * PAD, 128), F32), vm((4, T + 2 * PAD, 128), F32),
            vm((T, C), BF16), vm((T, C), BF16), vm((T, C), BF16),
            vm((512, T), BF16), vm((2, 512, T), BF16),
            vm((T, 128), F32), vm((T, 128), F32), vm((T, 128), F32), vm((T, 128), F32),
            vm((32, C), F32),
            vm((2, 8, T), F32), vm((2, NB, 8, T), F32),
            vm((32, C), F32), vm((8, C), F32),
            vm((4, 32, 128), BF16), vm((2, 32, 128), BF16), vm((3, 4, 32, 128), BF16),
            vm((1, 2, 4, 4, 256, 256), BF16),
            vm((1, 2, 2, 2, 256, 256), BF16),
            vm((1, 2, 2, 4, 256, 256), BF16),
            vm((1, 2, 2, 128, 256), BF16),
            vm((1, 2, 2, 256, 256), BF16),
            vm((3, 4, T, 256), BF16), vm((3, 2, T, C), BF16),
            vm((2, 3, 512, T), BF16),
            vm((2, 4, 512, 256), F32), vm((2, 4, 512, 256), BF16),
            vm((2, 2, 2, 128, 256), BF16), vm((2, 2, 512, 256), BF16),
            vm((4, T, C), BF16),
            vm((2, 256, C), BF16), vm((2, T, C), BF16),
            pltpu.SemaphoreType.DMA((N_COPIES,)),
            pltpu.SemaphoreType.DMA((N_COPIES,)),
            pltpu.SemaphoreType.DMA((5,)),
        ],
        compiler_params=pltpu.CompilerParams(
            collective_id=0, has_side_effects=True, vmem_limit_bytes=64 * 1024 * 1024 - 3 * 1024 * 1024
        ),
    )(
        inputs, grad_out, w_value.reshape(shape3), w_gate.reshape(shape3), w_out.reshape(shape3),
        taps, ln_gain.reshape(1, C),
    )
    gi, gvw, ggw, gow, gt, gg = pl.pallas_call(
        unpack,
        out_shape=(
            jax.ShapeDtypeStruct((T, C), BF16),
            jax.ShapeDtypeStruct((256, C), F32),
            jax.ShapeDtypeStruct((256, C), F32),
            jax.ShapeDtypeStruct((256, C), F32),
            jax.ShapeDtypeStruct((TAPS, C), F32),
            jax.ShapeDtypeStruct((1, C), F32),
        ),
        in_specs=[in_vmem] * 3,
        out_specs=(anyspace,) * 4 + (in_vmem,) * 2,
        scratch_shapes=[vm((3, 256, C), F32), pltpu.SemaphoreType.DMA((4,))],
        compiler_params=pltpu.CompilerParams(vmem_limit_bytes=8 * 1024 * 1024),
    )(gi, w3, small)
    return gi, gvw, ggw, gow, gt, gg.reshape(C)


def solution(mesh):
    in_specs = (
        P("sp", "tp"), P(None, "tp"), P(None, "tp"), P(None, "tp"), P("tp"), P(None, "tp"), P("sp", "tp"),
    )
    out_specs = (P("sp", "tp"), P("sp", "tp"), P("sp", "tp"), P("sp", "tp"), P(None, "tp"), P("tp"))
    return jax.shard_map(local, mesh=mesh, in_specs=in_specs, out_specs=out_specs, check_vma=False)
```

```python
import jax
import jax.numpy as jnp
from jax import lax
from jax.experimental import pallas as pl
from jax.experimental.pallas import tpu as pltpu
from jax.sharding import PartitionSpec as P

MESH = pl.DeviceIdType.MESH
F32 = jnp.float32
BF16 = jnp.bfloat16
HI = lax.Precision.HIGHEST
T = 512
C = 512
NB = 8
RAD = 15
TAPS = 31
PAD = 16
COLS = (0, 128, 256, 384)
N_COPIES = 141
N_SENDS = 76


def sig(v):
    return 1.0 / (1.0 + jnp.exp(-v))


def dot_nn(a, b):
    return lax.dot_general(a, b, (((1,), (0,)), ((), ())), preferred_element_type=F32)


def dot_nt(a, b):
    return lax.dot_general(a, b, (((1,), (1,)), ((), ())), preferred_element_type=F32)


def dot_tn(a, b):
    return lax.dot_general(a, b, (((0,), (0,)), ((), ())), preferred_element_type=F32)


def kernel(
    x_hbm, g_hbm, wv_hbm, wg_hbm, wo_hbm, taps_hbm, gain_hbm,
    gi_out, w_out, small_out,
    X, G, WV, WG, WO, PV, PG, GA, NRM, HID, GC, ACT, GV, GG, AT, BT,
    SA, SQ, MEAN, INV, TF, ST, STR, TP, GP, TG, TG1, TGR,
    part, r1, r2, r3, r4, XA, XB, BTR, VACC, VP, r3v, r4v, PR, y1, y2, taps_ref, gain_ref, ss, rs, ls,
):
    sp = lax.axis_index("sp")
    tp = lax.axis_index("tp")
    z, x = sp // 4, sp % 4
    y, c = tp // 2, tp % 2

    def at_tp(t):
        return (sp, t)

    def at_y(yy):
        return (sp, (yy % 4) * 2 + c)

    def at_x(xx):
        return (z * 4 + xx % 4, tp)

    def at_z(zz):
        return ((zz % 4) * 4 + x, tp)

    partner = at_tp(y * 2 + (1 - c))

    scope = [None]

    def mark(name):
        if scope[0] is not None:
            scope[0].__exit__(None, None, None)
        scope[0] = jax.named_scope(name) if name else None
        if name:
            scope[0].__enter__()

    counter = [0]
    free = list(range(N_SENDS))
    sent = []

    def rcopy(src, dst, dev):
        i = counter[0]
        counter[0] += 1
        k = free.pop(0)
        cp = pltpu.make_async_remote_copy(
            src_ref=src, dst_ref=dst, send_sem=ss.at[k], recv_sem=rs.at[i],
            device_id=dev, device_id_type=MESH,
        )
        cp.start()
        sent.append((cp, k))
        return cp

    def drain(count):
        for cp, k in sent[:count]:
            cp.wait_send()
            free.append(k)
        del sent[:count]

    mark("entry")
    loads = []
    for i, (src, dst) in enumerate(
        ((x_hbm, X.at[tp]), (wv_hbm, WV), (wg_hbm, WG), (g_hbm, G.at[tp]), (wo_hbm, WO),
         (taps_hbm, taps_ref), (gain_hbm, gain_ref))
    ):
        cp = pltpu.make_async_copy(src, dst, ls.at[i])
        cp.start()
        loads.append(cp)

    barrier = pltpu.get_barrier_semaphore()
    peers = [at_tp((tp + d) % 8) for d in range(1, 8)]
    peers += [at_x(x + d) for d in range(1, 4)] + [at_z(z + d) for d in range(1, 4)]
    peers += [((sp + 1) % 16, tp), ((sp + 15) % 16, tp)]
    for dev in peers:
        pl.semaphore_signal(barrier, inc=1, device_id=dev, device_id_type=MESH)
    PV[...] = jnp.zeros((T, C), F32)
    PG[...] = jnp.zeros((T, C), F32)
    GA[...] = jnp.zeros((T, C), F32)
    pl.semaphore_wait(barrier, len(peers))

    jm = ((y + 3) % 4) * 2 + c
    jp = ((y + 1) % 4) * 2 + c
    jo = ((y + 2) % 4) * 2 + c
    LO, HIH = pl.ds(0, 256), pl.ds(256, 256)

    class Gather:
        def __init__(self, buf):
            self.b = buf

        def start(self):
            b = self.b
            self.h1p = rcopy(b.at[tp, LO], b.at[tp, LO], at_y(y + 1))
            self.h1m = rcopy(b.at[tp, HIH], b.at[tp, HIH], at_y(y + 3))
            self.d0 = rcopy(b.at[tp], b.at[tp], partner)
            self.h2p = rcopy(b.at[tp, HIH], b.at[tp, HIH], at_y(y + 1))
            self.h2m = rcopy(b.at[tp, LO], b.at[tp, LO], at_y(y + 3))

        def first(self):
            b = self.b
            self.h1p.wait_recv()
            self.fp = rcopy(b.at[jm, LO], b.at[jm, LO], at_y(y + 1))
            self.d1p = rcopy(b.at[jm, LO], b.at[jm, LO], partner)
            self.h1m.wait_recv()
            self.fm = rcopy(b.at[jp, HIH], b.at[jp, HIH], at_y(y + 3))
            self.d1m = rcopy(b.at[jp, HIH], b.at[jp, HIH], partner)

        def second(self):
            b = self.b
            self.h2p.wait_recv()
            self.d2p = rcopy(b.at[jm, HIH], b.at[jm, HIH], partner)
            self.h2m.wait_recv()
            self.d2m = rcopy(b.at[jp, LO], b.at[jp, LO], partner)

        def third(self):
            b = self.b
            self.fp.wait_recv()
            self.d3p = rcopy(b.at[jo, LO], b.at[jo, LO], partner)
            self.fm.wait_recv()
            self.d3m = rcopy(b.at[jo, HIH], b.at[jo, HIH], partner)

    def mm(buf, pairs, d_even, d_odd, row_even, row_odd, lo, hi):
        def body(i, _):
            e = i % 2
            par = i // 2
            cc = c + par - 2 * c * par
            j = ((y + d_even + e * (d_odd - d_even)) % 4) * 2 + cc
            row = pl.multiple_of(row_even + e * (row_odd - row_even), 256)
            rows = pl.ds(row, 256)
            a = buf[j, rows, :]
            for w, acc in pairs:
                for n in (0, 256):
                    acc[rows, n:n + 256] += dot_nn(a, w[j, :, n:n + 256])
            return 0

        lax.fori_loop(lo, hi, body, 0)

    toks = pl.ds(pl.multiple_of(c * 256, 256), 256)
    ex_a = []
    b0 = counter[0]
    counter[0] += 3
    bs = free[:3]
    del free[:3]
    bs0 = bs[0]

    def ex_b(d, yy):
        return pltpu.make_async_remote_copy(
            src_ref=X.at[pl.ds(2 * yy, 2), toks], dst_ref=XB.at[d - 1, :, toks],
            send_sem=ss.at[bs0 + d - 1], recv_sem=rs.at[b0 + d - 1],
            device_id=at_z(z + d), device_id_type=MESH,
        )

    def exchange(yy):
        yy = yy % 4
        for d in (1, 3, 2):
            t = (x + d) % 4
            cols = pl.ds(pl.multiple_of((t % 2) * 256, 256), 256)
            ex_a.append((d, rcopy(X.at[yy * 2 + t // 2, toks, cols], XA.at[d - 1, yy, toks], at_x(t))))

        @pl.when(yy != z)
        def _():
            ex_b((yy + 4 - z) % 4, yy).start()

    def exchange_relay():
        out = []
        for d in (1, 3, 2):
            for dd, cp in ex_a:
                if dd == d:
                    cp.wait_recv()
            out.append(rcopy(XA.at[d - 1, :, toks], XA.at[d - 1, :, toks], partner))
        for d in (1, 3, 2):
            ex_b(d, y).wait_recv()
            out.append(rcopy(XB.at[d - 1, :, toks], XB.at[d - 1, :, toks], partner))
        return out

    gx, gg_ = Gather(X), Gather(G)
    vg = ((WV, PV), (WG, PG))
    wo = ((WO, GA),)
    mark("xload")
    loads[0].wait()
    gx.start()
    mark("wload")
    loads[1].wait()
    loads[2].wait()
    mark("x0")
    mm(X, vg, 0, 0, 0, 256, 0, 2)
    gx.d0.wait_recv()
    exchange(y)
    mm(X, vg, 0, 0, 0, 256, 2, 4)
    mark("x1w")
    gx.first()
    loads[3].wait()
    gg_.start()
    mark("x1")
    mm(X, vg, 3, 1, 0, 256, 0, 2)
    gx.d1p.wait_recv()
    gx.d1m.wait_recv()
    exchange(y + 3 + 2 * c)
    mm(X, vg, 3, 1, 0, 256, 2, 4)
    mark("x2w")
    gx.second()
    mark("x2")
    mm(X, vg, 3, 1, 256, 0, 0, 2)
    gx.d2p.wait_recv()
    gx.d2m.wait_recv()
    mm(X, vg, 3, 1, 256, 0, 2, 4)
    mark("x3w")
    gx.third()
    mark("x3")
    mm(X, vg, 2, 2, 0, 256, 0, 2)
    gx.d3p.wait_recv()
    gx.d3m.wait_recv()
    mm(X, vg, 2, 2, 0, 256, 2, 4)

    mark("hidden")
    loads[5].wait()
    loads[6].wait()
    TF[...] = jnp.zeros((32, C), F32)
    TF[0:TAPS, :] = taps_ref[...].astype(F32)
    def hidden_body(i, _):
        rows = pl.ds(pl.multiple_of(i * 32, 32), 32)
        out_rows = pl.ds(pl.multiple_of(i * 32 + PAD, 16), 32)
        for n, cs in enumerate(COLS):
            col = slice(cs, cs + 128)
            s = sig(PG[rows, col])
            PG[rows, col] = s
            HID[n, out_rows, :] = (PV[rows, col] * s).astype(BF16).astype(F32)
        return 0

    lax.fori_loop(0, T // 32, hidden_body, 0)

    following, previous = ((sp + 1) % 16, tp), ((sp + 15) % 16, tp)

    def halo_start(buf):
        up = rcopy(buf.at[:, pl.ds(T, PAD)], buf.at[:, pl.ds(0, PAD)], following)
        down = rcopy(buf.at[:, pl.ds(PAD, PAD)], buf.at[:, pl.ds(T + PAD, PAD)], previous)
        return up, down

    def halo_finish(buf, pair):
        pair[0].wait_recv()
        pair[1].wait_recv()

        @pl.when(sp == 0)
        def _():
            buf[:, 0:PAD, :] = jnp.zeros((4, PAD, 128), F32)

        @pl.when(sp == 15)
        def _():
            buf[:, T + PAD:T + 2 * PAD, :] = jnp.zeros((4, PAD, 128), F32)

    mark("g0")
    halo = halo_start(HID)
    exchange(y + 1 + 2 * c)
    exchange(y + 2)
    loads[4].wait()
    mm(G, wo, 0, 0, 0, 256, 0, 2)
    gg_.d0.wait_recv()
    mm(G, wo, 0, 0, 0, 256, 2, 4)
    mark("halo1w")
    halo_finish(HID, halo)
    mark("g1w")
    gg_.first()

    mark("conv")
    R = 64

    def conv_tile(src, r0, cs, flip):
        acc = jnp.zeros((R, 128), F32)
        for o in range(1, TAPS + 1):
            k = TAPS - o if flip else o - 1
            acc = acc + TF[k:k + 1, cs:cs + 128] * src[cs // 128, pl.ds(r0 + o, R), :]
        return acc

    def conv_body(i, _):
        r0 = pl.multiple_of(i * R, R)
        rows = pl.ds(r0, R)
        s = jnp.zeros((R, 128), F32)
        q = jnp.zeros((R, 128), F32)
        for cs in COLS:
            v = conv_tile(HID, r0, cs, False)
            NRM[rows, cs:cs + 128] = v
            s = s + v
            q = q + v * v
        SA[rows, :] = s
        SQ[rows, :] = q
        return 0

    lax.fori_loop(0, T // R, conv_body, 0)

    def stats_start(e):
        row = lax.broadcasted_iota(jnp.int32, (8, 128), 0)
        dims = (((1,), (1,)), ((), ()))
        tile = lax.dot_general(
            jnp.where(row == 0, 1.0, 0.0).astype(F32), SA[...], dims, precision=HI, preferred_element_type=F32
        ) + lax.dot_general(
            jnp.where(row == 1, 1.0, 0.0).astype(F32), SQ[...], dims, precision=HI, preferred_element_type=F32
        )
        packed = jnp.zeros((8, 128), F32)
        for r in range(4):
            packed = jnp.where(row == r, tile[0:1, 128 * r:128 * r + 128], packed)
            packed = jnp.where(row == r + 4, tile[1:2, 128 * r:128 * r + 128], packed)
        tile = packed
        ST[e] = tile
        STR[e, tp] = tile
        return [rcopy(ST.at[e], STR.at[e, tp], at_tp((tp + d) % 8)) for d in range(1, 8)]

    def stats_finish(e, copies):
        for cp in copies:
            cp.wait_recv()
        row = lax.broadcasted_iota(jnp.int32, (64, 256), 0) & 7
        lane = lax.broadcasted_iota(jnp.int32, (64, 256), 1)
        want = jnp.where(lane < 128, 0, 4)
        block = STR[e].reshape(64, 128)
        for t in range(0, T, 128):
            pick = jnp.where(row == want + t // 128, 1.0, 0.0).astype(F32)
            both = lax.dot_general(
                block, pick, (((0,), (0,)), ((), ())), precision=HI, preferred_element_type=F32
            ) * (1.0 / (NB * C))
            if e == 0:
                mean = both[:, :128]
                MEAN[t:t + 128, :] = mean
                INV[t:t + 128, :] = lax.rsqrt(both[:, 128:] - mean * mean + 1e-06)
            else:
                SA[t:t + 128, :] = both[:, :128]
                SQ[t:t + 128, :] = both[:, 128:]

    mark("stats1")
    stats = stats_start(0)
    mark("g1")
    mm(G, wo, 3, 1, 0, 256, 0, 2)
    gg_.d1p.wait_recv()
    gg_.d1m.wait_recv()
    mm(G, wo, 3, 1, 0, 256, 2, 4)
    mark("g2w")
    gg_.second()
    mark("g2")
    mm(G, wo, 3, 1, 256, 0, 0, 2)
    gg_.d2p.wait_recv()
    gg_.d2m.wait_recv()
    mm(G, wo, 3, 1, 256, 0, 2, 4)
    mark("g3w")
    gg_.third()
    mark("g3")
    mm(G, wo, 2, 2, 0, 256, 0, 2)
    gg_.d3p.wait_recv()
    gg_.d3m.wait_recv()
    mm(G, wo, 2, 2, 0, 256, 2, 4)

    mark("stats1w")
    stats_finish(0, stats)
    mark("scaled")
    GP[...] = jnp.zeros((8, C), F32)

    def scaled_body(i, _):
        rows = pl.ds(pl.multiple_of(i * 32, 32), 32)
        m, iv = MEAN[rows, :], INV[rows, :]
        s1 = jnp.zeros((32, 128), F32)
        s2 = jnp.zeros((32, 128), F32)
        for cs in COLS:
            col = slice(cs, cs + 128)
            n = (NRM[rows, col] - m) * iv
            NRM[rows, col] = n
            gain = gain_ref[0:1, col]
            sc = n * gain
            s = sig(sc)
            ACT[rows, col] = (sc * s).astype(BF16)
            gs = GA[rows, col] * s * (1.0 + sc * (1.0 - s))
            GP[:, col] += (gs * n).reshape(4, 8, 128).sum(axis=0)
            gn = gs * gain
            GA[rows, col] = gn
            s1 = s1 + gn
            s2 = s2 + gn * n
        SA[rows, :] = s1
        SQ[rows, :] = s2
        return 0

    lax.fori_loop(0, T // 32, scaled_body, 0)
    early = len(sent)
    mark("stats2")
    stats = stats_start(1)

    at_p = (at_x, at_z)
    at_q = (at_z, at_x)
    me_p = (x, z)
    me_q = (z, x)

    def dw(lhs, units, left, pair, lo=0, hi=4):
        def body(k, _):
            zz = (z + 2 + k) % 4
            for e in (0, 1):
                r = dot_nn(left, lhs[zz * 2 + pair, :, e * 256:e * 256 + 256]).astype(BF16)
                for n, u in enumerate(units):
                    a = r[n * 512:n * 512 + 256]
                    b = r[n * 512 + 256:n * 512 + 512]
                    part[u, 0, 2 * pair + e, zz] = a
                    part[u, 1, zz, 2 * pair + e] = b
            return 0

        lax.fori_loop(lo, hi, body, 0)

    class Scatter:
        def __init__(self, u, h):
            self.u, self.h = u, h
            self.p, self.q = me_p[h], me_q[h]

        def blk(self, dp, q0, n=2):
            return part.at[self.u, self.h, (self.p + dp) % 4, pl.ds(q0, n)]

        def s1(self):
            u, h, p = self.u, self.h, self.p
            self.a = rcopy(self.blk(2, 0), r1.at[u, h, 0], at_p[h](p + 1))
            self.b = rcopy(self.blk(2, 2), r1.at[u, h, 1], at_p[h](p + 3))

        def s2i(self):
            u, h, p = self.u, self.h, self.p
            self.c = rcopy(self.blk(1, 2), r2.at[u, h, 0, pl.ds(2, 2)], at_p[h](p + 1))
            self.d = rcopy(self.blk(3, 0), r2.at[u, h, 1, pl.ds(0, 2)], at_p[h](p + 3))

        def add(self, dst_index, rows, sources):
            u, h = self.u, self.h

            def body(i, _):
                rr = pl.ds(pl.multiple_of(rows + i * 32, 32), 32)
                v = part[(u, h) + dst_index + (rr,)].astype(F32)
                for ref, index, off in sources:
                    v = v + ref[index + (pl.ds(pl.multiple_of(off + i * 32, 32), 32),)].astype(F32)
                part[(u, h) + dst_index + (rr,)] = v.astype(BF16)
                return 0

            return body

        def s2d(self):
            u, h, p = self.u, self.h, self.p
            self.a.wait_recv()
            for q in (0, 1):
                lax.fori_loop(0, 8, self.add(((p + 1) % 4, q), 0, [(r1, (u, h, 0, q), 0)]), 0)
            self.e = rcopy(self.blk(1, 0), r2.at[u, h, 0, pl.ds(0, 2)], at_p[h](p + 1))
            self.b.wait_recv()
            for q in (2, 3):
                lax.fori_loop(0, 8, self.add(((p + 3) % 4, q), 0, [(r1, (u, h, 1, q - 2), 0)]), 0)
            self.f = rcopy(self.blk(3, 2), r2.at[u, h, 1, pl.ds(2, 2)], at_p[h](p + 3))

        def p1(self):
            u, h, p, q = self.u, self.h, self.p, self.q
            for cp in (self.c, self.d, self.e, self.f):
                cp.wait_recv()
            for dq in (2, 1, 3, 0):
                qq = (q + dq) % 4
                lax.fori_loop(
                    0, 8, self.add((p, qq), 0, [(r2, (u, h, 0, qq), 0), (r2, (u, h, 1, qq), 0)]), 0
                )
                if dq == 2:
                    src = part.at[u, h, p, qq]
                    self.i = rcopy(src.at[pl.ds(0, 128)], r3.at[u, h, 0], at_q[h](q + 1))
                    self.j = rcopy(src.at[pl.ds(128, 128)], r3.at[u, h, 1], at_q[h](q + 3))

        def p2(self):
            u, h, p, q = self.u, self.h, self.p, self.q
            up, down = (q + 1) % 4, (q + 3) % 4
            self.i.wait_recv()
            lax.fori_loop(0, 4, self.add((p, up), 0, [(r3, (u, h, 0), 0)]), 0)
            self.k = rcopy(part.at[u, h, p, up], r4.at[u, h, 0], at_q[h](q + 1))
            self.j.wait_recv()
            lax.fori_loop(0, 4, self.add((p, down), 128, [(r3, (u, h, 1), 0)]), 0)
            self.l = rcopy(part.at[u, h, p, down], r4.at[u, h, 1], at_q[h](q + 3))

        def finish(self):
            u, h, p, q = self.u, self.h, self.p, self.q
            self.k.wait_recv()
            self.l.wait_recv()
            for i in (0, 128):
                rr = slice(i, i + 128)
                v = (
                    part[u, h, p, q, rr].astype(F32)
                    + r4[u, h, 0, rr].astype(F32)
                    + r4[u, h, 1, rr].astype(F32)
                )
                w_out[u, :, h * 256 + i:h * 256 + i + 128] = v.T.astype(BF16)

    sc = [[Scatter(0, h) for h in (0, 1)]]

    def flipped(src, n):
        eye = (
            lax.broadcasted_iota(jnp.int32, (256, 256), 0) == lax.broadcasted_iota(jnp.int32, (256, 256), 1)
        ).astype(F32).astype(BF16)
        return dot_nt(eye, src[:, n:n + 256]).astype(BF16)

    for n in (0, 256):
        AT[n:n + 256, :] = flipped(ACT, n)
    dw(G, [0], AT[...], 1 - x // 2)
    sc[0][0].s1()
    mark("ow_dw2")
    dw(G, [0], AT[...], x // 2, 0, 1)
    sc[0][1].s1()
    dw(G, [0], AT[...], x // 2, 1, 4)
    mark("stats2w")
    stats_finish(1, stats)

    mark("gc")
    def gc_body(i, _):
        rows = pl.ds(pl.multiple_of(i * 32, 32), 32)
        out_rows = pl.ds(pl.multiple_of(i * 32 + PAD, 16), 32)
        f, s, iv = SA[rows, :], SQ[rows, :], INV[rows, :]
        for cs in COLS:
            col = slice(cs, cs + 128)
            GC[cs // 128, out_rows, :] = iv * (GA[rows, col] - f - NRM[rows, col] * s)
        return 0

    lax.fori_loop(0, T // 32, gc_body, 0)
    halo = halo_start(GC)
    for h in (0, 1):
        sc[0][h].s2i()

    mark("taps")
    for cs in COLS:
        def tap_body(i, accs, cs=cs):
            r0 = pl.multiple_of(i * 32, 32)
            g = GC[cs // 128, pl.ds(r0 + PAD, 32), :]
            accs = list(accs)
            for o in range(1, TAPS + 1):
                prod = HID[cs // 128, pl.ds(r0 + o, 32), :] * g
                accs[o - 1] = accs[o - 1] + prod.reshape(4, 8, 128).sum(axis=0)
            return tuple(accs)

        accs = lax.fori_loop(
            0, T // 32, tap_body, tuple(jnp.zeros((8, 128), F32) for _ in range(TAPS))
        )
        for k, a in enumerate(accs):
            TP[k:k + 1, cs:cs + 128] = jnp.sum(a, axis=0, keepdims=True)
    TP[TAPS:TAPS + 1, :] = jnp.sum(GP[...], axis=0, keepdims=True)

    def small_send(e, src, me, at):
        TGR[e, me] = src(me)[...]
        return [rcopy(src((me + d) % 4), TGR.at[e, me], at(me + d)) for d in (1, 3, 2)]

    def small_sum(e, copies):
        for cp in copies:
            cp.wait_recv()
        v = TGR[e, 0].astype(F32)
        for i in range(1, 4):
            v = v + TGR[e, i].astype(F32)
        return v.astype(BF16)

    for t in range(4):
        TG[t] = TP[:, t * 128:t * 128 + 128].astype(BF16)
    small = small_send(0, lambda t: TG.at[t], x, at_x)
    mark("relay")
    relays = exchange_relay()
    drain(early)
    mark("halo2w")
    halo_finish(GC, halo)

    mark("back")
    def back_body(i, _):
        r0 = pl.multiple_of(i * R, R)
        rows = pl.ds(r0, R)
        for cs in COLS:
            col = slice(cs, cs + 128)
            gh = conv_tile(GC, r0, cs, True)
            s = PG[rows, col]
            gv = gh * s
            GV[rows, col] = gv.astype(BF16)
            GG[rows, col] = (gv * PV[rows, col] * (1.0 - s)).astype(BF16)
        return 0

    lax.fori_loop(0, T // R, back_body, 0)

    middle = len(sent)
    mark("vg_t")
    for n in (0, 256):
        BT[n // 256, 0:256, :] = flipped(GV, n)

    class Spread:
        def __init__(self, h, u):
            self.h, self.p = h, me_p[h]
            self.lo, self.hi = pl.ds(u * 256, 128), pl.ds(u * 256 + 128, 128)

        def start(self):
            h, p, lo, hi = self.h, self.p, self.lo, self.hi
            own, got = BT.at[h], BTR.at[h]
            nxt, prv = at_p[h](p + 1), at_p[h](p + 3)
            self.h1p = rcopy(own.at[lo], got.at[0, lo], nxt)
            self.h1m = rcopy(own.at[hi], got.at[2, hi], prv)
            self.h2p = rcopy(own.at[hi], got.at[0, hi], nxt)
            self.h2m = rcopy(own.at[lo], got.at[2, lo], prv)

        def first(self):
            h, p, lo, hi = self.h, self.p, self.lo, self.hi
            got = BTR.at[h]
            self.h1p.wait_recv()
            self.fp = rcopy(got.at[0, lo], got.at[1, lo], at_p[h](p + 1))
            self.h1m.wait_recv()
            self.fm = rcopy(got.at[2, hi], got.at[1, hi], at_p[h](p + 3))

        def second(self):
            self.h2p.wait_recv()
            self.h2m.wait_recv()

        def third(self):
            self.fp.wait_recv()
            self.fm.wait_recv()

    def own_in(h, q):
        zz, xx = (q, x) if h == 0 else (z, q)
        cols = pl.ds(pl.multiple_of((xx % 2) * 256, 256), 256)
        return X[zz * 2 + xx // 2, :, cols]

    def got_in(h, k, q):
        if h == 0:
            return XA[k, q]
        return XB[k, q // 2, :, pl.ds(pl.multiple_of((q % 2) * 256, 256), 256)]

    def vg_own(h):
        def body(q, _):
            VACC[h, q] = dot_nn(BT[h], own_in(h, q))
            return 0

        lax.fori_loop(0, 4, body, 0)

    def vg_near(h, u):
        rows = pl.ds(u * 256, 256)

        def body(q, _):
            VACC[h, q, rows] += dot_nn(BTR[h, 0, rows], got_in(h, 0, q)) + dot_nn(BTR[h, 2, rows], got_in(h, 2, q))
            return 0

        lax.fori_loop(0, 4, body, 0)

    class Last:
        def __init__(self, h, u):
            self.h, self.u, self.q = h, u, me_q[h]
            self.rows = pl.ds(u * 256, 256)

        def make(self, dq):
            h, rows = self.h, self.rows
            qq = (self.q + dq) % 4
            VP[h, qq, rows] = (VACC[h, qq, rows] + dot_nn(BTR[h, 1, rows], got_in(h, 1, qq))).astype(BF16)

        def s1(self):
            h, u, q = self.h, self.u, self.q
            src = VP.at[h, (q + 2) % 4]
            self.i = rcopy(src.at[pl.ds(u * 256, 128)], r3v.at[h, u, 0], at_q[h](q + 1))
            self.j = rcopy(src.at[pl.ds(u * 256 + 128, 128)], r3v.at[h, u, 1], at_q[h](q + 3))

        def s2(self):
            h, u, q, rows = self.h, self.u, self.q, self.rows

            def add(qq, row0, k):
                def body(i, _):
                    rr = pl.ds(pl.multiple_of(row0 + i * 64, 64), 64)
                    fr = pl.ds(pl.multiple_of(i * 64, 64), 64)
                    VP[h, qq, rr] = (VP[h, qq, rr].astype(F32) + r3v[h, u, k, fr].astype(F32)).astype(BF16)
                    return 0

                lax.fori_loop(0, 2, body, 0)

            up, down = (q + 1) % 4, (q + 3) % 4
            self.i.wait_recv()
            add(up, u * 256, 0)
            self.k = rcopy(VP.at[h, up, rows], r4v.at[h, 0, rows], at_q[h](q + 1))
            self.j.wait_recv()
            add(down, u * 256 + 128, 1)
            self.l = rcopy(VP.at[h, down, rows], r4v.at[h, 1, rows], at_q[h](q + 3))

        def finish(self):
            h, u, q = self.h, self.u, self.q
            self.k.wait_recv()
            self.l.wait_recv()
            for i in (0, 128):
                rr = slice(u * 256 + i, u * 256 + i + 128)
                v = VP[h, q, rr].astype(F32) + r4v[h, 0, rr].astype(F32) + r4v[h, 1, rr].astype(F32)
                w_out[u + 1, :, h * 256 + i:h * 256 + i + 128] = v.T.astype(BF16)

    spread = [[Spread(0, u), Spread(1, u)] for u in (0, 1)]
    last = [[Last(0, u), Last(1, u)] for u in (0, 1)]
    for h in (0, 1):
        spread[0][h].start()
    for n in (0, 256):
        BT[n // 256, 256:512, :] = flipped(GG, n)

    mark("partial1")
    def partial(parity):
        def body(i, _):
            yy = i // 2
            rows = pl.ds(pl.multiple_of((i % 2) * 256, 256), 256)
            j = yy * 2 + parity
            gv, gt = GV[rows, :], GG[rows, :]
            for n in (0, 256):
                G[parity * 4 + yy, rows, n:n + 256] = (
                    dot_nt(gv, WV[j, n:n + 256, :]) + dot_nt(gt, WG[j, n:n + 256, :])
                ).astype(BF16)
            return 0

        lax.fori_loop(0, 8, body, 0)

    partial(1 - c)
    swap = rcopy(G.at[pl.ds((1 - c) * 4, 4)], PR, partner)
    mark("v_first")
    for h in (0, 1):
        spread[0][h].first()
    for h in (0, 1):
        spread[1][h].start()
    mark("partial2")
    partial(c)
    mark("yadd")
    swap.wait_recv()

    def y_add(block, row0, n, sources):
        def body(i, _):
            rr = pl.ds(pl.multiple_of(row0 + i * 32, 32), 32)
            v = G[block, rr].astype(F32)
            for ref, index, off in sources:
                v = v + ref[index + (pl.ds(pl.multiple_of(off + i * 32, 32), 32),)].astype(F32)
            G[block, rr] = v.astype(BF16)
            return 0

        lax.fori_loop(0, n // 32, body, 0)

    base = c * 4
    y2_, yp_, ym_ = (y + 2) % 4, (y + 1) % 4, (y + 3) % 4
    y_add(base + y2_, 0, T, [(PR, (y2_,), 0)])
    ya = rcopy(G.at[base + y2_, LO], y1.at[0], at_y(y + 1))
    yb = rcopy(G.at[base + y2_, HIH], y1.at[1], at_y(y + 3))
    y_add(base + yp_, 0, T, [(PR, (yp_,), 0)])
    yc = rcopy(G.at[base + yp_, HIH], y2.at[0, HIH], at_y(y + 1))
    y_add(base + ym_, 0, T, [(PR, (ym_,), 0)])
    yd = rcopy(G.at[base + ym_, LO], y2.at[1, LO], at_y(y + 3))
    y_add(base + y, 0, T, [(PR, (y,), 0)])

    mark("vg_own")
    for h in (0, 1):
        vg_own(h)
    mark("g_first")
    for h in (0, 1):
        spread[1][h].first()
    mark("ow_s2d")
    for h in (0, 1):
        sc[0][h].s2d()
    for cp in relays:
        cp.wait_recv()
    drain(middle)
    mark("v_near")
    for h in (0, 1):
        spread[0][h].second()
    for h in (0, 1):
        vg_near(h, 0)
    mark("v_third")
    for h in (0, 1):
        spread[0][h].third()
    mark("v_far")
    for h in (0, 1):
        last[0][h].make(2)
        last[0][h].s1()
    for dq in (1, 3, 0):
        for h in (0, 1):
            last[0][h].make(dq)
    mark("y_s2")
    ya.wait_recv()
    y_add(base + yp_, 0, 256, [(y1, (0,), 0)])
    ye = rcopy(G.at[base + yp_, LO], y2.at[0, LO], at_y(y + 1))
    yb.wait_recv()
    y_add(base + ym_, 256, 256, [(y1, (1,), 0)])
    yf = rcopy(G.at[base + ym_, HIH], y2.at[1, HIH], at_y(y + 3))
    mark("small")
    TG1[0] = small_sum(0, small)
    small = small_send(1, lambda t: TG1.at[0], z, at_z)
    mark("g_second")
    for h in (0, 1):
        spread[1][h].second()
    mark("g_near")
    for h in (0, 1):
        vg_near(h, 1)
    mark("g_third")
    for h in (0, 1):
        spread[1][h].third()
    mark("g_far")
    for h in (0, 1):
        last[1][h].make(2)
        last[1][h].s1()
    for dq in (1, 3, 0):
        for h in (0, 1):
            last[1][h].make(dq)
    mark("ow_p1")
    for h in (0, 1):
        sc[0][h].p1()
    TG1[1] = small_sum(1, small)
    small = small_send(2, lambda t: TG1.at[1], x, at_x)
    mark("v_s2")
    for h in (0, 1):
        last[0][h].s2()
    mark("g_s2")
    for h in (0, 1):
        last[1][h].s2()
    mark("ow_p2")
    for h in (0, 1):
        sc[0][h].p2()
    for cp in small:
        cp.wait_recv()
    for t in range(4):
        small_out[:, t * 128:t * 128 + 128] = TGR[2, t].astype(F32)
    mark("y_fin")
    for cp in (yc, yd, ye, yf):
        cp.wait_recv()

    def gi_body(i, _):
        rr = pl.ds(pl.multiple_of(i * 32, 32), 32)
        gi_out[rr, :] = (
            G[base + y, rr].astype(F32) + y2[0, rr].astype(F32) + y2[1, rr].astype(F32)
        ).astype(BF16)
        return 0

    lax.fori_loop(0, T // 32, gi_body, 0)
    mark("fin")
    for h in (0, 1):
        last[0][h].finish()
    mark("g_fin")
    for h in (0, 1):
        last[1][h].finish()
    mark("ow_fin")
    for h in (0, 1):
        sc[0][h].finish()
    mark("sends")
    drain(len(sent))
    for d in (1, 2, 3):
        ex_b(d, (z + d) % 4).wait_send()
    mark(None)
    assert counter[0] == N_COPIES


def unpack(gi_in, w_in, small_in, gi, gvw, ggw, gow, gt, gg, b_out, so):
    writes = [pltpu.make_async_copy(gi_in, gi, so.at[3])]
    writes[0].start()
    for u, dst in enumerate((gow, gvw, ggw)):
        b_out[u] = w_in[u].astype(F32)
        writes.append(pltpu.make_async_copy(b_out.at[u], dst, so.at[u]))
        writes[-1].start()
    gt[...] = small_in[0:TAPS]
    gg[...] = small_in[TAPS:TAPS + 1]
    for cp in writes:
        cp.wait()


def local(inputs, w_value, w_gate, taps, ln_gain, w_out, grad_out):
    vm = pltpu.VMEM
    anyspace = pl.BlockSpec(memory_space=pl.ANY)
    in_vmem = pl.BlockSpec(memory_space=pltpu.VMEM)
    shape3 = (NB, C, C)
    gi, w3, small = pl.pallas_call(
        kernel,
        out_shape=(
            vm((T, C), BF16),
            vm((3, 256, C), BF16),
            vm((32, C), F32),
        ),
        in_specs=[anyspace] * 7,
        out_specs=(in_vmem,) * 3,
        scratch_shapes=[
            vm((NB, T, C), BF16), vm((NB, T, C), BF16),
            vm(shape3, BF16), vm(shape3, BF16), vm(shape3, BF16),
            vm((T, C), F32), vm((T, C), F32), vm((T, C), F32), vm((T, C), F32),
            vm((4, T + 2 * PAD, 128), F32), vm((4, T + 2 * PAD, 128), F32),
            vm((T, C), BF16), vm((T, C), BF16), vm((T, C), BF16),
            vm((512, T), BF16), vm((2, 512, T), BF16),
            vm((T, 128), F32), vm((T, 128), F32), vm((T, 128), F32), vm((T, 128), F32),
            vm((32, C), F32),
            vm((2, 8, 128), F32), vm((2, NB, 8, 128), F32),
            vm((32, C), F32), vm((8, C), F32),
            vm((4, 32, 128), BF16), vm((2, 32, 128), BF16), vm((3, 4, 32, 128), BF16),
            vm((1, 2, 4, 4, 256, 256), BF16),
            vm((1, 2, 2, 2, 256, 256), BF16),
            vm((1, 2, 2, 4, 256, 256), BF16),
            vm((1, 2, 2, 128, 256), BF16),
            vm((1, 2, 2, 256, 256), BF16),
            vm((3, 4, T, 256), BF16), vm((3, 2, T, C), BF16),
            vm((2, 3, 512, T), BF16),
            vm((2, 4, 512, 256), F32), vm((2, 4, 512, 256), BF16),
            vm((2, 2, 2, 128, 256), BF16), vm((2, 2, 512, 256), BF16),
            vm((4, T, C), BF16),
            vm((2, 256, C), BF16), vm((2, T, C), BF16),
            vm((TAPS, C), BF16), vm((1, C), F32),
            pltpu.SemaphoreType.DMA((N_SENDS,)),
            pltpu.SemaphoreType.DMA((N_COPIES,)),
            pltpu.SemaphoreType.DMA((7,)),
        ],
        compiler_params=pltpu.CompilerParams(
            collective_id=0, has_side_effects=True, vmem_limit_bytes=64 * 1024 * 1024 - 3 * 1024 * 1024
        ),
    )(
        inputs, grad_out, w_value.reshape(shape3), w_gate.reshape(shape3), w_out.reshape(shape3),
        taps, ln_gain.reshape(1, C),
    )
    gi, gvw, ggw, gow, gt, gg = pl.pallas_call(
        unpack,
        out_shape=(
            jax.ShapeDtypeStruct((T, C), BF16),
            jax.ShapeDtypeStruct((256, C), F32),
            jax.ShapeDtypeStruct((256, C), F32),
            jax.ShapeDtypeStruct((256, C), F32),
            jax.ShapeDtypeStruct((TAPS, C), F32),
            jax.ShapeDtypeStruct((1, C), F32),
        ),
        in_specs=[in_vmem] * 3,
        out_specs=(anyspace,) * 4 + (in_vmem,) * 2,
        scratch_shapes=[vm((3, 256, C), F32), pltpu.SemaphoreType.DMA((4,))],
        compiler_params=pltpu.CompilerParams(vmem_limit_bytes=8 * 1024 * 1024),
    )(gi, w3, small)
    return gi, gvw, ggw, gow, gt, gg.reshape(C)


def solution(mesh):
    in_specs = (
        P("sp", "tp"), P(None, "tp"), P(None, "tp"), P(None, "tp"), P("tp"), P(None, "tp"), P("sp", "tp"),
    )
    out_specs = (P("sp", "tp"), P("sp", "tp"), P("sp", "tp"), P("sp", "tp"), P(None, "tp"), P("tp"))
    return jax.shard_map(local, mesh=mesh, in_specs=in_specs, out_specs=out_specs, check_vma=False)
```

```python
import jax
import jax.numpy as jnp
from jax import lax
from jax.experimental import pallas as pl
from jax.experimental.pallas import tpu as pltpu
from jax.sharding import PartitionSpec as P

MESH = pl.DeviceIdType.MESH
F32 = jnp.float32
BF16 = jnp.bfloat16
HI = lax.Precision.HIGHEST
T = 512
C = 512
NB = 8
RAD = 15
TAPS = 31
PAD = 16
COLS = (0, 128, 256, 384)
N_COPIES = 141
N_SENDS = 76


def sig(v):
    return 1.0 / (1.0 + jnp.exp(-v))


def dot_nn(a, b):
    return lax.dot_general(a, b, (((1,), (0,)), ((), ())), preferred_element_type=F32)


def dot_nt(a, b):
    return lax.dot_general(a, b, (((1,), (1,)), ((), ())), preferred_element_type=F32)


def dot_tn(a, b):
    return lax.dot_general(a, b, (((0,), (0,)), ((), ())), preferred_element_type=F32)


def kernel(
    x_hbm, g_hbm, wv_hbm, wg_hbm, wo_hbm, taps_hbm, gain_hbm,
    gi_out, w_out, small_out,
    X, G, WV, WG, WO, PV, PG, GA, NRM, HID, GC, ACT, GV, GG, AT, BT,
    SA, SQ, MEAN, INV, TF, ST, STR, TP, GP, TG, TG1, TGR,
    part, r1, r2, r3, r4, XA, XB, BTR, VACC, VP, r3v, r4v, PR, y1, y2, taps_ref, gain_ref, ss, rs, ls,
):
    sp = lax.axis_index("sp")
    tp = lax.axis_index("tp")
    z, x = sp // 4, sp % 4
    y, c = tp // 2, tp % 2

    def at_tp(t):
        return (sp, t)

    def at_y(yy):
        return (sp, (yy % 4) * 2 + c)

    def at_x(xx):
        return (z * 4 + xx % 4, tp)

    def at_z(zz):
        return ((zz % 4) * 4 + x, tp)

    partner = at_tp(y * 2 + (1 - c))

    scope = [None]

    def mark(name):
        if scope[0] is not None:
            scope[0].__exit__(None, None, None)
        scope[0] = jax.named_scope(name) if name else None
        if name:
            scope[0].__enter__()

    counter = [0]
    free = list(range(N_SENDS))
    sent = []

    def rcopy(src, dst, dev):
        i = counter[0]
        counter[0] += 1
        k = free.pop(0)
        cp = pltpu.make_async_remote_copy(
            src_ref=src, dst_ref=dst, send_sem=ss.at[k], recv_sem=rs.at[i],
            device_id=dev, device_id_type=MESH,
        )
        cp.start()
        sent.append((cp, k))
        return cp

    def drain(count):
        for cp, k in sent[:count]:
            cp.wait_send()
            free.append(k)
        del sent[:count]

    mark("entry")
    loads = []
    for i, (src, dst) in enumerate(
        ((x_hbm, X.at[tp]), (wv_hbm, WV), (wg_hbm, WG), (g_hbm, G.at[tp]), (wo_hbm, WO),
         (taps_hbm, taps_ref), (gain_hbm, gain_ref))
    ):
        cp = pltpu.make_async_copy(src, dst, ls.at[i])
        cp.start()
        loads.append(cp)

    barrier = pltpu.get_barrier_semaphore()
    peers = [at_tp((tp + d) % 8) for d in range(1, 8)]
    peers += [at_x(x + d) for d in range(1, 4)] + [at_z(z + d) for d in range(1, 4)]
    peers += [((sp + 1) % 16, tp), ((sp + 15) % 16, tp)]
    for dev in peers:
        pl.semaphore_signal(barrier, inc=1, device_id=dev, device_id_type=MESH)
    PV[...] = jnp.zeros((T, C), F32)
    PG[...] = jnp.zeros((T, C), F32)
    GA[...] = jnp.zeros((T, C), F32)
    pl.semaphore_wait(barrier, len(peers))

    jm = ((y + 3) % 4) * 2 + c
    jp = ((y + 1) % 4) * 2 + c
    jo = ((y + 2) % 4) * 2 + c
    LO, HIH = pl.ds(0, 256), pl.ds(256, 256)

    class Gather:
        def __init__(self, buf):
            self.b = buf

        def start(self):
            b = self.b
            self.h1p = rcopy(b.at[tp, LO], b.at[tp, LO], at_y(y + 1))
            self.h1m = rcopy(b.at[tp, HIH], b.at[tp, HIH], at_y(y + 3))
            self.d0 = rcopy(b.at[tp], b.at[tp], partner)
            self.h2p = rcopy(b.at[tp, HIH], b.at[tp, HIH], at_y(y + 1))
            self.h2m = rcopy(b.at[tp, LO], b.at[tp, LO], at_y(y + 3))

        def first(self):
            b = self.b
            self.h1p.wait_recv()
            self.fp = rcopy(b.at[jm, LO], b.at[jm, LO], at_y(y + 1))
            self.d1p = rcopy(b.at[jm, LO], b.at[jm, LO], partner)
            self.h1m.wait_recv()
            self.fm = rcopy(b.at[jp, HIH], b.at[jp, HIH], at_y(y + 3))
            self.d1m = rcopy(b.at[jp, HIH], b.at[jp, HIH], partner)

        def second(self):
            b = self.b
            self.h2p.wait_recv()
            self.d2p = rcopy(b.at[jm, HIH], b.at[jm, HIH], partner)
            self.h2m.wait_recv()
            self.d2m = rcopy(b.at[jp, LO], b.at[jp, LO], partner)

        def third(self):
            b = self.b
            self.fp.wait_recv()
            self.d3p = rcopy(b.at[jo, LO], b.at[jo, LO], partner)
            self.fm.wait_recv()
            self.d3m = rcopy(b.at[jo, HIH], b.at[jo, HIH], partner)

    def mm(buf, pairs, d_even, d_odd, row_even, row_odd, lo, hi):
        def body(i, _):
            e = i % 2
            par = i // 2
            cc = c + par - 2 * c * par
            j = ((y + d_even + e * (d_odd - d_even)) % 4) * 2 + cc
            row = pl.multiple_of(row_even + e * (row_odd - row_even), 256)
            rows = pl.ds(row, 256)
            a = buf[j, rows, :]
            for w, acc in pairs:
                for n in (0, 256):
                    acc[rows, n:n + 256] += dot_nn(a, w[j, :, n:n + 256])
            return 0

        lax.fori_loop(lo, hi, body, 0)

    toks = pl.ds(pl.multiple_of(c * 256, 256), 256)
    ex_a = []
    b0 = counter[0]
    counter[0] += 3
    bs = free[:3]
    del free[:3]
    bs0 = bs[0]

    def ex_b(d, yy):
        return pltpu.make_async_remote_copy(
            src_ref=X.at[pl.ds(2 * yy, 2), toks], dst_ref=XB.at[d - 1, :, toks],
            send_sem=ss.at[bs0 + d - 1], recv_sem=rs.at[b0 + d - 1],
            device_id=at_z(z + d), device_id_type=MESH,
        )

    def exchange(yy):
        yy = yy % 4
        for d in (1, 3, 2):
            t = (x + d) % 4
            cols = pl.ds(pl.multiple_of((t % 2) * 256, 256), 256)
            ex_a.append((d, rcopy(X.at[yy * 2 + t // 2, toks, cols], XA.at[d - 1, yy, toks], at_x(t))))

        @pl.when(yy != z)
        def _():
            ex_b((yy + 4 - z) % 4, yy).start()

    def exchange_relay():
        out = []
        for d in (1, 3, 2):
            for dd, cp in ex_a:
                if dd == d:
                    cp.wait_recv()
            out.append(rcopy(XA.at[d - 1, :, toks], XA.at[d - 1, :, toks], partner))
        for d in (1, 3, 2):
            ex_b(d, y).wait_recv()
            out.append(rcopy(XB.at[d - 1, :, toks], XB.at[d - 1, :, toks], partner))
        return out

    gx, gg_ = Gather(X), Gather(G)
    vg = ((WV, PV), (WG, PG))
    wo = ((WO, GA),)
    mark("xload")
    loads[0].wait()
    gx.start()
    mark("wload")
    loads[1].wait()
    loads[2].wait()
    mark("x0")
    mm(X, vg, 0, 0, 0, 256, 0, 2)
    gx.d0.wait_recv()
    exchange(y)
    mm(X, vg, 0, 0, 0, 256, 2, 4)
    mark("x1w")
    gx.first()
    loads[3].wait()
    gg_.start()
    mark("x1")
    mm(X, vg, 3, 1, 0, 256, 0, 2)
    gx.d1p.wait_recv()
    gx.d1m.wait_recv()
    exchange(y + 3 + 2 * c)
    mm(X, vg, 3, 1, 0, 256, 2, 4)
    mark("x2w")
    gx.second()
    mark("x2")
    mm(X, vg, 3, 1, 256, 0, 0, 2)
    gx.d2p.wait_recv()
    gx.d2m.wait_recv()
    mm(X, vg, 3, 1, 256, 0, 2, 4)
    mark("x3w")
    gx.third()
    mark("x3")
    mm(X, vg, 2, 2, 0, 256, 0, 2)
    gx.d3p.wait_recv()
    gx.d3m.wait_recv()
    mm(X, vg, 2, 2, 0, 256, 2, 4)

    mark("hidden")
    loads[5].wait()
    loads[6].wait()
    TF[...] = jnp.zeros((32, C), F32)
    TF[0:TAPS, :] = taps_ref[...].astype(F32)
    def hidden_body(i, _):
        rows = pl.ds(pl.multiple_of(i * 32, 32), 32)
        out_rows = pl.ds(pl.multiple_of(i * 32 + PAD, 16), 32)
        for n, cs in enumerate(COLS):
            col = slice(cs, cs + 128)
            s = sig(PG[rows, col])
            PG[rows, col] = s
            HID[n, out_rows, :] = (PV[rows, col] * s).astype(BF16).astype(F32)
        return 0

    lax.fori_loop(0, T // 32, hidden_body, 0)

    following, previous = ((sp + 1) % 16, tp), ((sp + 15) % 16, tp)

    def halo_start(buf):
        up = rcopy(buf.at[:, pl.ds(T, PAD)], buf.at[:, pl.ds(0, PAD)], following)
        down = rcopy(buf.at[:, pl.ds(PAD, PAD)], buf.at[:, pl.ds(T + PAD, PAD)], previous)
        return up, down

    def halo_finish(buf, pair):
        pair[0].wait_recv()
        pair[1].wait_recv()

        @pl.when(sp == 0)
        def _():
            buf[:, 0:PAD, :] = jnp.zeros((4, PAD, 128), F32)

        @pl.when(sp == 15)
        def _():
            buf[:, T + PAD:T + 2 * PAD, :] = jnp.zeros((4, PAD, 128), F32)

    mark("g0")
    halo = halo_start(HID)
    exchange(y + 1 + 2 * c)
    exchange(y + 2)
    loads[4].wait()
    mm(G, wo, 0, 0, 0, 256, 0, 2)
    gg_.d0.wait_recv()
    mm(G, wo, 0, 0, 0, 256, 2, 4)
    mark("halo1w")
    halo_finish(HID, halo)
    mark("g1w")
    gg_.first()

    mark("conv")
    R = 64

    def conv_tile(src, r0, cs, flip):
        acc = jnp.zeros((R, 128), F32)
        for o in range(1, TAPS + 1):
            k = TAPS - o if flip else o - 1
            acc = acc + TF[k:k + 1, cs:cs + 128] * src[cs // 128, pl.ds(r0 + o, R), :]
        return acc

    def conv_body(i, _):
        r0 = pl.multiple_of(i * R, R)
        rows = pl.ds(r0, R)
        s = jnp.zeros((R, 128), F32)
        q = jnp.zeros((R, 128), F32)
        for cs in COLS:
            v = conv_tile(HID, r0, cs, False)
            NRM[rows, cs:cs + 128] = v
            s = s + v
            q = q + v * v
        SA[rows, :] = s
        SQ[rows, :] = q
        return 0

    lax.fori_loop(0, T // R, conv_body, 0)

    def stats_start(e):
        row = lax.broadcasted_iota(jnp.int32, (8, 128), 0)
        dims = (((1,), (1,)), ((), ()))
        tile = lax.dot_general(
            jnp.where(row == 0, 1.0, 0.0).astype(F32), SA[...], dims, precision=HI, preferred_element_type=F32
        ) + lax.dot_general(
            jnp.where(row == 1, 1.0, 0.0).astype(F32), SQ[...], dims, precision=HI, preferred_element_type=F32
        )
        packed = jnp.zeros((8, 128), F32)
        for r in range(4):
            packed = jnp.where(row == r, tile[0:1, 128 * r:128 * r + 128], packed)
            packed = jnp.where(row == r + 4, tile[1:2, 128 * r:128 * r + 128], packed)
        tile = packed
        ST[e] = tile
        STR[e, tp] = tile
        return [rcopy(ST.at[e], STR.at[e, tp], at_tp((tp + d) % 8)) for d in range(1, 8)]

    def stats_finish(e, copies):
        for cp in copies:
            cp.wait_recv()
        row = lax.broadcasted_iota(jnp.int32, (64, 256), 0) & 7
        lane = lax.broadcasted_iota(jnp.int32, (64, 256), 1)
        want = jnp.where(lane < 128, 0, 4)
        block = STR[e].reshape(64, 128)
        for t in range(0, T, 128):
            pick = jnp.where(row == want + t // 128, 1.0, 0.0).astype(F32)
            both = lax.dot_general(
                block, pick, (((0,), (0,)), ((), ())), precision=HI, preferred_element_type=F32
            ) * (1.0 / (NB * C))
            if e == 0:
                mean = both[:, :128]
                MEAN[t:t + 128, :] = mean
                INV[t:t + 128, :] = lax.rsqrt(both[:, 128:] - mean * mean + 1e-06)
            else:
                SA[t:t + 128, :] = both[:, :128]
                SQ[t:t + 128, :] = both[:, 128:]

    mark("stats1")
    stats = stats_start(0)
    mark("g1")
    mm(G, wo, 3, 1, 0, 256, 0, 2)
    gg_.d1p.wait_recv()
    gg_.d1m.wait_recv()
    mm(G, wo, 3, 1, 0, 256, 2, 4)
    mark("g2w")
    gg_.second()
    mark("g2")
    mm(G, wo, 3, 1, 256, 0, 0, 2)
    gg_.d2p.wait_recv()
    gg_.d2m.wait_recv()
    mm(G, wo, 3, 1, 256, 0, 2, 4)
    mark("g3w")
    gg_.third()
    mark("g3")
    mm(G, wo, 2, 2, 0, 256, 0, 2)
    gg_.d3p.wait_recv()
    gg_.d3m.wait_recv()
    mm(G, wo, 2, 2, 0, 256, 2, 4)

    mark("stats1w")
    stats_finish(0, stats)
    mark("scaled")
    GP[...] = jnp.zeros((8, C), F32)

    def scaled_body(i, _):
        rows = pl.ds(pl.multiple_of(i * 32, 32), 32)
        m, iv = MEAN[rows, :], INV[rows, :]
        s1 = jnp.zeros((32, 128), F32)
        s2 = jnp.zeros((32, 128), F32)
        for cs in COLS:
            col = slice(cs, cs + 128)
            n = (NRM[rows, col] - m) * iv
            NRM[rows, col] = n
            gain = gain_ref[0:1, col]
            sc = n * gain
            s = sig(sc)
            ACT[rows, col] = (sc * s).astype(BF16)
            gs = GA[rows, col] * s * (1.0 + sc * (1.0 - s))
            GP[:, col] += (gs * n).reshape(4, 8, 128).sum(axis=0)
            gn = gs * gain
            GA[rows, col] = gn
            s1 = s1 + gn
            s2 = s2 + gn * n
        SA[rows, :] = s1
        SQ[rows, :] = s2
        return 0

    lax.fori_loop(0, T // 32, scaled_body, 0)
    early = len(sent)
    mark("stats2")
    stats = stats_start(1)

    at_p = (at_x, at_z)
    at_q = (at_z, at_x)
    me_p = (x, z)
    me_q = (z, x)

    def dw(lhs, units, left, pair, lo=0, hi=4):
        def body(k, _):
            zz = (z + 2 + k) % 4
            for e in (0, 1):
                r = dot_nn(left, lhs[zz * 2 + pair, :, e * 256:e * 256 + 256]).astype(BF16)
                for n, u in enumerate(units):
                    a = r[n * 512:n * 512 + 256]
                    b = r[n * 512 + 256:n * 512 + 512]
                    part[u, 0, 2 * pair + e, zz] = a
                    part[u, 1, zz, 2 * pair + e] = b
            return 0

        lax.fori_loop(lo, hi, body, 0)

    class Scatter:
        def __init__(self, u, h):
            self.u, self.h = u, h
            self.p, self.q = me_p[h], me_q[h]

        def blk(self, dp, q0, n=2):
            return part.at[self.u, self.h, (self.p + dp) % 4, pl.ds(q0, n)]

        def s1(self):
            u, h, p = self.u, self.h, self.p
            self.a = rcopy(self.blk(2, 0), r1.at[u, h, 0], at_p[h](p + 1))
            self.b = rcopy(self.blk(2, 2), r1.at[u, h, 1], at_p[h](p + 3))

        def s2i(self):
            u, h, p = self.u, self.h, self.p
            self.c = rcopy(self.blk(1, 2), r2.at[u, h, 0, pl.ds(2, 2)], at_p[h](p + 1))
            self.d = rcopy(self.blk(3, 0), r2.at[u, h, 1, pl.ds(0, 2)], at_p[h](p + 3))

        def add(self, dst_index, rows, sources):
            u, h = self.u, self.h

            def body(i, _):
                rr = pl.ds(pl.multiple_of(rows + i * 32, 32), 32)
                v = part[(u, h) + dst_index + (rr,)].astype(F32)
                for ref, index, off in sources:
                    v = v + ref[index + (pl.ds(pl.multiple_of(off + i * 32, 32), 32),)].astype(F32)
                part[(u, h) + dst_index + (rr,)] = v.astype(BF16)
                return 0

            return body

        def s2d(self):
            u, h, p = self.u, self.h, self.p
            self.a.wait_recv()
            for q in (0, 1):
                lax.fori_loop(0, 8, self.add(((p + 1) % 4, q), 0, [(r1, (u, h, 0, q), 0)]), 0)
            self.e = rcopy(self.blk(1, 0), r2.at[u, h, 0, pl.ds(0, 2)], at_p[h](p + 1))
            self.b.wait_recv()
            for q in (2, 3):
                lax.fori_loop(0, 8, self.add(((p + 3) % 4, q), 0, [(r1, (u, h, 1, q - 2), 0)]), 0)
            self.f = rcopy(self.blk(3, 2), r2.at[u, h, 1, pl.ds(2, 2)], at_p[h](p + 3))

        def p1(self):
            u, h, p, q = self.u, self.h, self.p, self.q
            for cp in (self.c, self.d, self.e, self.f):
                cp.wait_recv()
            for dq in (2, 1, 3, 0):
                qq = (q + dq) % 4
                lax.fori_loop(
                    0, 8, self.add((p, qq), 0, [(r2, (u, h, 0, qq), 0), (r2, (u, h, 1, qq), 0)]), 0
                )
                if dq == 2:
                    src = part.at[u, h, p, qq]
                    self.i = rcopy(src.at[pl.ds(0, 128)], r3.at[u, h, 0], at_q[h](q + 1))
                    self.j = rcopy(src.at[pl.ds(128, 128)], r3.at[u, h, 1], at_q[h](q + 3))

        def p2(self):
            u, h, p, q = self.u, self.h, self.p, self.q
            up, down = (q + 1) % 4, (q + 3) % 4
            self.i.wait_recv()
            lax.fori_loop(0, 4, self.add((p, up), 0, [(r3, (u, h, 0), 0)]), 0)
            self.k = rcopy(part.at[u, h, p, up], r4.at[u, h, 0], at_q[h](q + 1))
            self.j.wait_recv()
            lax.fori_loop(0, 4, self.add((p, down), 128, [(r3, (u, h, 1), 0)]), 0)
            self.l = rcopy(part.at[u, h, p, down], r4.at[u, h, 1], at_q[h](q + 3))

        def finish(self):
            u, h, p, q = self.u, self.h, self.p, self.q
            self.k.wait_recv()
            self.l.wait_recv()
            for i in (0, 128):
                rr = slice(i, i + 128)
                v = (
                    part[u, h, p, q, rr].astype(F32)
                    + r4[u, h, 0, rr].astype(F32)
                    + r4[u, h, 1, rr].astype(F32)
                )
                w_out[u, :, h * 256 + i:h * 256 + i + 128] = v.T.astype(BF16)

    sc = [[Scatter(0, h) for h in (0, 1)]]

    def flipped(src, n):
        eye = (
            lax.broadcasted_iota(jnp.int32, (256, 256), 0) == lax.broadcasted_iota(jnp.int32, (256, 256), 1)
        ).astype(F32).astype(BF16)
        return dot_nt(eye, src[:, n:n + 256]).astype(BF16)

    for n in (0, 256):
        AT[n:n + 256, :] = flipped(ACT, n)
    dw(G, [0], AT[...], 1 - x // 2)
    sc[0][0].s1()
    mark("ow_dw2")
    dw(G, [0], AT[...], x // 2, 0, 1)
    sc[0][1].s1()
    dw(G, [0], AT[...], x // 2, 1, 4)
    mark("stats2w")
    stats_finish(1, stats)

    mark("gc")
    def gc_body(i, _):
        rows = pl.ds(pl.multiple_of(i * 32, 32), 32)
        out_rows = pl.ds(pl.multiple_of(i * 32 + PAD, 16), 32)
        f, s, iv = SA[rows, :], SQ[rows, :], INV[rows, :]
        for cs in COLS:
            col = slice(cs, cs + 128)
            GC[cs // 128, out_rows, :] = iv * (GA[rows, col] - f - NRM[rows, col] * s)
        return 0

    lax.fori_loop(0, T // 32, gc_body, 0)
    halo = halo_start(GC)
    for h in (0, 1):
        sc[0][h].s2i()

    mark("taps")
    for cs in COLS:
        def tap_body(i, accs, cs=cs):
            r0 = pl.multiple_of(i * 32, 32)
            g = GC[cs // 128, pl.ds(r0 + PAD, 32), :]
            accs = list(accs)
            for o in range(1, TAPS + 1):
                prod = HID[cs // 128, pl.ds(r0 + o, 32), :] * g
                accs[o - 1] = accs[o - 1] + prod.reshape(4, 8, 128).sum(axis=0)
            return tuple(accs)

        accs = lax.fori_loop(
            0, T // 32, tap_body, tuple(jnp.zeros((8, 128), F32) for _ in range(TAPS))
        )
        for k, a in enumerate(accs):
            TP[k:k + 1, cs:cs + 128] = jnp.sum(a, axis=0, keepdims=True)
    TP[TAPS:TAPS + 1, :] = jnp.sum(GP[...], axis=0, keepdims=True)

    def small_send(e, src, me, at):
        TGR[e, me] = src(me)[...]
        return [rcopy(src((me + d) % 4), TGR.at[e, me], at(me + d)) for d in (1, 3, 2)]

    def small_sum(e, copies):
        for cp in copies:
            cp.wait_recv()
        v = TGR[e, 0].astype(F32)
        for i in range(1, 4):
            v = v + TGR[e, i].astype(F32)
        return v.astype(BF16)

    for t in range(4):
        TG[t] = TP[:, t * 128:t * 128 + 128].astype(BF16)
    small = small_send(0, lambda t: TG.at[t], x, at_x)
    mark("relay")
    relays = exchange_relay()
    drain(early)
    mark("halo2w")
    halo_finish(GC, halo)

    mark("back")
    def back_body(i, _):
        r0 = pl.multiple_of(i * R, R)
        rows = pl.ds(r0, R)
        for cs in COLS:
            col = slice(cs, cs + 128)
            gh = conv_tile(GC, r0, cs, True)
            s = PG[rows, col]
            gv = gh * s
            GV[rows, col] = gv.astype(BF16)
            GG[rows, col] = (gv * PV[rows, col] * (1.0 - s)).astype(BF16)
        return 0

    lax.fori_loop(0, T // R, back_body, 0)

    middle = len(sent)
    mark("vg_t")
    for n in (0, 256):
        BT[n // 256, 0:256, :] = flipped(GV, n)

    class Spread:
        def __init__(self, h, u):
            self.h, self.p = h, me_p[h]
            self.lo, self.hi = pl.ds(u * 256, 128), pl.ds(u * 256 + 128, 128)

        def start(self):
            h, p, lo, hi = self.h, self.p, self.lo, self.hi
            own, got = BT.at[h], BTR.at[h]
            nxt, prv = at_p[h](p + 1), at_p[h](p + 3)
            self.h1p = rcopy(own.at[lo], got.at[0, lo], nxt)
            self.h1m = rcopy(own.at[hi], got.at[2, hi], prv)
            self.h2p = rcopy(own.at[hi], got.at[0, hi], nxt)
            self.h2m = rcopy(own.at[lo], got.at[2, lo], prv)

        def first(self):
            h, p, lo, hi = self.h, self.p, self.lo, self.hi
            got = BTR.at[h]
            self.h1p.wait_recv()
            self.fp = rcopy(got.at[0, lo], got.at[1, lo], at_p[h](p + 1))
            self.h1m.wait_recv()
            self.fm = rcopy(got.at[2, hi], got.at[1, hi], at_p[h](p + 3))

        def second(self):
            self.h2p.wait_recv()
            self.h2m.wait_recv()

        def third(self):
            self.fp.wait_recv()
            self.fm.wait_recv()

    def own_in(h, q):
        zz, xx = (q, x) if h == 0 else (z, q)
        cols = pl.ds(pl.multiple_of((xx % 2) * 256, 256), 256)
        return X[zz * 2 + xx // 2, :, cols]

    def got_in(h, k, q):
        if h == 0:
            return XA[k, q]
        return XB[k, q // 2, :, pl.ds(pl.multiple_of((q % 2) * 256, 256), 256)]

    def vg_own(h):
        def body(q, _):
            VACC[h, q] = dot_nn(BT[h], own_in(h, q))
            return 0

        lax.fori_loop(0, 4, body, 0)

    def vg_near(h, u):
        rows = pl.ds(u * 256, 256)

        def body(q, _):
            VACC[h, q, rows] += dot_nn(BTR[h, 0, rows], got_in(h, 0, q)) + dot_nn(BTR[h, 2, rows], got_in(h, 2, q))
            return 0

        lax.fori_loop(0, 4, body, 0)

    class Last:
        def __init__(self, h, u):
            self.h, self.u, self.q = h, u, me_q[h]
            self.rows = pl.ds(u * 256, 256)

        def make(self, dq):
            h, rows = self.h, self.rows
            qq = (self.q + dq) % 4
            VP[h, qq, rows] = (VACC[h, qq, rows] + dot_nn(BTR[h, 1, rows], got_in(h, 1, qq))).astype(BF16)

        def s1(self):
            h, u, q = self.h, self.u, self.q
            src = VP.at[h, (q + 2) % 4]
            self.i = rcopy(src.at[pl.ds(u * 256, 128)], r3v.at[h, u, 0], at_q[h](q + 1))
            self.j = rcopy(src.at[pl.ds(u * 256 + 128, 128)], r3v.at[h, u, 1], at_q[h](q + 3))

        def s2(self):
            h, u, q, rows = self.h, self.u, self.q, self.rows

            def add(qq, row0, k):
                def body(i, _):
                    rr = pl.ds(pl.multiple_of(row0 + i * 64, 64), 64)
                    fr = pl.ds(pl.multiple_of(i * 64, 64), 64)
                    VP[h, qq, rr] = (VP[h, qq, rr].astype(F32) + r3v[h, u, k, fr].astype(F32)).astype(BF16)
                    return 0

                lax.fori_loop(0, 2, body, 0)

            up, down = (q + 1) % 4, (q + 3) % 4
            self.i.wait_recv()
            add(up, u * 256, 0)
            self.k = rcopy(VP.at[h, up, rows], r4v.at[h, 0, rows], at_q[h](q + 1))
            self.j.wait_recv()
            add(down, u * 256 + 128, 1)
            self.l = rcopy(VP.at[h, down, rows], r4v.at[h, 1, rows], at_q[h](q + 3))

        def finish(self):
            h, u, q = self.h, self.u, self.q
            self.k.wait_recv()
            self.l.wait_recv()
            for i in (0, 128):
                rr = slice(u * 256 + i, u * 256 + i + 128)
                v = VP[h, q, rr].astype(F32) + r4v[h, 0, rr].astype(F32) + r4v[h, 1, rr].astype(F32)
                w_out[u + 1, :, h * 256 + i:h * 256 + i + 128] = v.T.astype(BF16)

    spread = [[Spread(0, u), Spread(1, u)] for u in (0, 1)]
    last = [[Last(0, u), Last(1, u)] for u in (0, 1)]
    for h in (0, 1):
        spread[0][h].start()
    for n in (0, 256):
        BT[n // 256, 256:512, :] = flipped(GG, n)

    mark("partial1")
    def partial(parity):
        def body(i, _):
            yy = i // 2
            rows = pl.ds(pl.multiple_of((i % 2) * 256, 256), 256)
            j = yy * 2 + parity
            gv, gt = GV[rows, :], GG[rows, :]
            for n in (0, 256):
                G[parity * 4 + yy, rows, n:n + 256] = (
                    dot_nt(gv, WV[j, n:n + 256, :]) + dot_nt(gt, WG[j, n:n + 256, :])
                ).astype(BF16)
            return 0

        lax.fori_loop(0, 8, body, 0)

    partial(1 - c)
    swap = rcopy(G.at[pl.ds((1 - c) * 4, 4)], PR, partner)
    mark("small")
    TG1[0] = small_sum(0, small)
    small = small_send(1, lambda t: TG1.at[0], z, at_z)
    mark("v_first")
    for h in (0, 1):
        spread[0][h].first()
    for h in (0, 1):
        spread[1][h].start()
    mark("ow_s2d")
    for h in (0, 1):
        sc[0][h].s2d()
    mark("partial2")
    partial(c)
    mark("yadd")
    swap.wait_recv()

    def y_add(block, row0, n, sources):
        def body(i, _):
            rr = pl.ds(pl.multiple_of(row0 + i * 32, 32), 32)
            v = G[block, rr].astype(F32)
            for ref, index, off in sources:
                v = v + ref[index + (pl.ds(pl.multiple_of(off + i * 32, 32), 32),)].astype(F32)
            G[block, rr] = v.astype(BF16)
            return 0

        lax.fori_loop(0, n // 32, body, 0)

    base = c * 4
    y2_, yp_, ym_ = (y + 2) % 4, (y + 1) % 4, (y + 3) % 4
    y_add(base + y2_, 0, T, [(PR, (y2_,), 0)])
    ya = rcopy(G.at[base + y2_, LO], y1.at[0], at_y(y + 1))
    yb = rcopy(G.at[base + y2_, HIH], y1.at[1], at_y(y + 3))
    y_add(base + yp_, 0, T, [(PR, (yp_,), 0)])
    yc = rcopy(G.at[base + yp_, HIH], y2.at[0, HIH], at_y(y + 1))
    y_add(base + ym_, 0, T, [(PR, (ym_,), 0)])
    yd = rcopy(G.at[base + ym_, LO], y2.at[1, LO], at_y(y + 3))
    y_add(base + y, 0, T, [(PR, (y,), 0)])

    mark("small2")
    TG1[1] = small_sum(1, small)
    small = small_send(2, lambda t: TG1.at[1], x, at_x)
    mark("vg_own")
    for h in (0, 1):
        vg_own(h)
    mark("v_near")
    for cp in relays:
        cp.wait_recv()
    drain(middle)
    for h in (0, 1):
        spread[0][h].second()
    for h in (0, 1):
        vg_near(h, 0)
    mark("v_third")
    for h in (0, 1):
        spread[0][h].third()
    mark("v_far")
    for h in (0, 1):
        last[0][h].make(2)
        last[0][h].s1()
    for dq in (1, 3, 0):
        for h in (0, 1):
            last[0][h].make(dq)
    mark("g_first")
    for h in (0, 1):
        spread[1][h].first()
    mark("y_s2")
    ya.wait_recv()
    y_add(base + yp_, 0, 256, [(y1, (0,), 0)])
    ye = rcopy(G.at[base + yp_, LO], y2.at[0, LO], at_y(y + 1))
    yb.wait_recv()
    y_add(base + ym_, 256, 256, [(y1, (1,), 0)])
    yf = rcopy(G.at[base + ym_, HIH], y2.at[1, HIH], at_y(y + 3))
    mark("g_second")
    for h in (0, 1):
        spread[1][h].second()
    mark("g_near")
    for h in (0, 1):
        vg_near(h, 1)
    mark("ow_p1")
    for h in (0, 1):
        sc[0][h].p1()
    mark("v_s2")
    for h in (0, 1):
        last[0][h].s2()
    mark("g_third")
    for h in (0, 1):
        spread[1][h].third()
    mark("g_far")
    for h in (0, 1):
        last[1][h].make(2)
        last[1][h].s1()
    mark("ow_p2")
    for h in (0, 1):
        sc[0][h].p2()
    mark("g_rest")
    for dq in (1, 3, 0):
        for h in (0, 1):
            last[1][h].make(dq)
    mark("g_s2")
    for h in (0, 1):
        last[1][h].s2()
    mark("small3")
    for cp in small:
        cp.wait_recv()
    for t in range(4):
        small_out[:, t * 128:t * 128 + 128] = TGR[2, t].astype(F32)
    mark("y_fin")
    for cp in (yc, yd, ye, yf):
        cp.wait_recv()

    def gi_body(i, _):
        rr = pl.ds(pl.multiple_of(i * 32, 32), 32)
        gi_out[rr, :] = (
            G[base + y, rr].astype(F32) + y2[0, rr].astype(F32) + y2[1, rr].astype(F32)
        ).astype(BF16)
        return 0

    lax.fori_loop(0, T // 32, gi_body, 0)
    mark("fin_v")
    for h in (0, 1):
        last[0][h].finish()
    mark("fin_o")
    for h in (0, 1):
        sc[0][h].finish()
    mark("fin_g")
    for h in (0, 1):
        last[1][h].finish()
    mark("sends")
    drain(len(sent))
    for d in (1, 2, 3):
        ex_b(d, (z + d) % 4).wait_send()
    mark(None)
    assert counter[0] == N_COPIES


def unpack(gi_in, w_in, small_in, gi, gvw, ggw, gow, gt, gg, b_out, so):
    writes = [pltpu.make_async_copy(gi_in, gi, so.at[3])]
    writes[0].start()
    for u, dst in enumerate((gow, gvw, ggw)):
        b_out[u] = w_in[u].astype(F32)
        writes.append(pltpu.make_async_copy(b_out.at[u], dst, so.at[u]))
        writes[-1].start()
    gt[...] = small_in[0:TAPS]
    gg[...] = small_in[TAPS:TAPS + 1]
    for cp in writes:
        cp.wait()


def local(inputs, w_value, w_gate, taps, ln_gain, w_out, grad_out):
    vm = pltpu.VMEM
    anyspace = pl.BlockSpec(memory_space=pl.ANY)
    in_vmem = pl.BlockSpec(memory_space=pltpu.VMEM)
    shape3 = (NB, C, C)
    gi, w3, small = pl.pallas_call(
        kernel,
        out_shape=(
            vm((T, C), BF16),
            vm((3, 256, C), BF16),
            vm((32, C), F32),
        ),
        in_specs=[anyspace] * 7,
        out_specs=(in_vmem,) * 3,
        scratch_shapes=[
            vm((NB, T, C), BF16), vm((NB, T, C), BF16),
            vm(shape3, BF16), vm(shape3, BF16), vm(shape3, BF16),
            vm((T, C), F32), vm((T, C), F32), vm((T, C), F32), vm((T, C), F32),
            vm((4, T + 2 * PAD, 128), F32), vm((4, T + 2 * PAD, 128), F32),
            vm((T, C), BF16), vm((T, C), BF16), vm((T, C), BF16),
            vm((512, T), BF16), vm((2, 512, T), BF16),
            vm((T, 128), F32), vm((T, 128), F32), vm((T, 128), F32), vm((T, 128), F32),
            vm((32, C), F32),
            vm((2, 8, 128), F32), vm((2, NB, 8, 128), F32),
            vm((32, C), F32), vm((8, C), F32),
            vm((4, 32, 128), BF16), vm((2, 32, 128), BF16), vm((3, 4, 32, 128), BF16),
            vm((1, 2, 4, 4, 256, 256), BF16),
            vm((1, 2, 2, 2, 256, 256), BF16),
            vm((1, 2, 2, 4, 256, 256), BF16),
            vm((1, 2, 2, 128, 256), BF16),
            vm((1, 2, 2, 256, 256), BF16),
            vm((3, 4, T, 256), BF16), vm((3, 2, T, C), BF16),
            vm((2, 3, 512, T), BF16),
            vm((2, 4, 512, 256), F32), vm((2, 4, 512, 256), BF16),
            vm((2, 2, 2, 128, 256), BF16), vm((2, 2, 512, 256), BF16),
            vm((4, T, C), BF16),
            vm((2, 256, C), BF16), vm((2, T, C), BF16),
            vm((TAPS, C), BF16), vm((1, C), F32),
            pltpu.SemaphoreType.DMA((N_SENDS,)),
            pltpu.SemaphoreType.DMA((N_COPIES,)),
            pltpu.SemaphoreType.DMA((7,)),
        ],
        compiler_params=pltpu.CompilerParams(
            collective_id=0, has_side_effects=True, vmem_limit_bytes=64 * 1024 * 1024 - 3 * 1024 * 1024
        ),
    )(
        inputs, grad_out, w_value.reshape(shape3), w_gate.reshape(shape3), w_out.reshape(shape3),
        taps, ln_gain.reshape(1, C),
    )
    gi, gvw, ggw, gow, gt, gg = pl.pallas_call(
        unpack,
        out_shape=(
            jax.ShapeDtypeStruct((T, C), BF16),
            jax.ShapeDtypeStruct((256, C), F32),
            jax.ShapeDtypeStruct((256, C), F32),
            jax.ShapeDtypeStruct((256, C), F32),
            jax.ShapeDtypeStruct((TAPS, C), F32),
            jax.ShapeDtypeStruct((1, C), F32),
        ),
        in_specs=[in_vmem] * 3,
        out_specs=(anyspace,) * 4 + (in_vmem,) * 2,
        scratch_shapes=[vm((3, 256, C), F32), pltpu.SemaphoreType.DMA((4,))],
        compiler_params=pltpu.CompilerParams(vmem_limit_bytes=8 * 1024 * 1024),
    )(gi, w3, small)
    return gi, gvw, ggw, gow, gt, gg.reshape(C)


def solution(mesh):
    in_specs = (
        P("sp", "tp"), P(None, "tp"), P(None, "tp"), P(None, "tp"), P("tp"), P(None, "tp"), P("sp", "tp"),
    )
    out_specs = (P("sp", "tp"), P("sp", "tp"), P("sp", "tp"), P("sp", "tp"), P(None, "tp"), P("tp"))
    return jax.shard_map(local, mesh=mesh, in_specs=in_specs, out_specs=out_specs, check_vma=False)
```

```python
import jax
import jax.numpy as jnp
from jax import lax
from jax.experimental import pallas as pl
from jax.experimental.pallas import tpu as pltpu
from jax.sharding import PartitionSpec as P

MESH = pl.DeviceIdType.MESH
F32 = jnp.float32
BF16 = jnp.bfloat16
HI = lax.Precision.HIGHEST
T = 512
C = 512
NB = 8
RAD = 15
TAPS = 31
PAD = 16
COLS = (0, 128, 256, 384)
N_COPIES = 108
N_SENDS = 64


def sig(v):
    return 1.0 / (1.0 + jnp.exp(-v))


def dot_nn(a, b):
    return lax.dot_general(a, b, (((1,), (0,)), ((), ())), preferred_element_type=F32)


def dot_nt(a, b):
    return lax.dot_general(a, b, (((1,), (1,)), ((), ())), preferred_element_type=F32)


def dot_tn(a, b):
    return lax.dot_general(a, b, (((0,), (0,)), ((), ())), preferred_element_type=F32)


def kernel(
    x_hbm, g_hbm, wv_hbm, wg_hbm, wo_hbm, taps_hbm, gain_hbm,
    gi_out, w_out, small_out,
    X, G, WV, WG, WO, PV, PG, GA, NRM, HID, GC, ACT, GV, GG, AT, BT,
    SA, SQ, MEAN, INV, TF, ST, STR, TP, GP, TG, TG1, TGR,
    part, r1, r2, r3, r4, XA, XB, BTR, VACC, VP, r3v, r4v, PR, y1, y2, taps_ref, gain_ref, ss, rs, ls,
):
    sp = lax.axis_index("sp")
    tp = lax.axis_index("tp")
    z, x = sp // 4, sp % 4
    y, c = tp // 2, tp % 2

    def at_tp(t):
        return (sp, t)

    def at_y(yy):
        return (sp, (yy % 4) * 2 + c)

    def at_x(xx):
        return (z * 4 + xx % 4, tp)

    def at_z(zz):
        return ((zz % 4) * 4 + x, tp)

    partner = at_tp(y * 2 + (1 - c))

    scope = [None]

    def mark(name):
        if scope[0] is not None:
            scope[0].__exit__(None, None, None)
        scope[0] = jax.named_scope(name) if name else None
        if name:
            scope[0].__enter__()

    counter = [0]
    free = list(range(N_SENDS))
    sent = []

    def new_recv():
        counter[0] += 1
        return counter[0] - 1

    def wait_all(ref, i):
        pltpu.make_async_remote_copy(
            src_ref=ref, dst_ref=ref, send_sem=ss.at[0], recv_sem=rs.at[i],
            device_id=partner, device_id_type=MESH,
        ).wait_recv()

    def rcopy(src, dst, dev, recv=None):
        i = new_recv() if recv is None else recv
        k = free.pop(0)
        cp = pltpu.make_async_remote_copy(
            src_ref=src, dst_ref=dst, send_sem=ss.at[k], recv_sem=rs.at[i],
            device_id=dev, device_id_type=MESH,
        )
        cp.start()
        sent.append((cp, k))
        return cp

    def drain(count):
        for cp, k in sent[:count]:
            cp.wait_send()
            free.append(k)
        free.sort()
        del sent[:count]

    mark("entry")
    loads = []
    for i, (src, dst) in enumerate(
        ((x_hbm, X.at[tp]), (wv_hbm, WV), (wg_hbm, WG), (g_hbm, G.at[tp]), (wo_hbm, WO),
         (taps_hbm, taps_ref), (gain_hbm, gain_ref))
    ):
        cp = pltpu.make_async_copy(src, dst, ls.at[i])
        cp.start()
        loads.append(cp)

    barrier = pltpu.get_barrier_semaphore()
    peers = [at_tp((tp + d) % 8) for d in range(1, 8)]
    peers += [at_x(x + d) for d in range(1, 4)] + [at_z(z + d) for d in range(1, 4)]
    peers += [((sp + 1) % 16, tp), ((sp + 15) % 16, tp)]
    for dev in peers:
        pl.semaphore_signal(barrier, inc=1, device_id=dev, device_id_type=MESH)
    PV[...] = jnp.zeros((T, C), F32)
    PG[...] = jnp.zeros((T, C), F32)
    GA[...] = jnp.zeros((T, C), F32)
    pl.semaphore_wait(barrier, len(peers))

    jm = ((y + 3) % 4) * 2 + c
    jp = ((y + 1) % 4) * 2 + c
    jo = ((y + 2) % 4) * 2 + c
    LO, HIH = pl.ds(0, 256), pl.ds(256, 256)

    class Gather:
        def __init__(self, buf):
            self.b = buf

        def start(self):
            b = self.b
            self.h1p = rcopy(b.at[tp, LO], b.at[tp, LO], at_y(y + 1))
            self.h1m = rcopy(b.at[tp, HIH], b.at[tp, HIH], at_y(y + 3))
            self.d0 = rcopy(b.at[tp], b.at[tp], partner)
            self.h2p = rcopy(b.at[tp, HIH], b.at[tp, HIH], at_y(y + 1))
            self.h2m = rcopy(b.at[tp, LO], b.at[tp, LO], at_y(y + 3))

        def first(self):
            b = self.b
            self.h1p.wait_recv()
            self.fp = rcopy(b.at[jm, LO], b.at[jm, LO], at_y(y + 1))
            self.d1p = rcopy(b.at[jm, LO], b.at[jm, LO], partner)
            self.h1m.wait_recv()
            self.fm = rcopy(b.at[jp, HIH], b.at[jp, HIH], at_y(y + 3))
            self.d1m = rcopy(b.at[jp, HIH], b.at[jp, HIH], partner)

        def second(self):
            b = self.b
            self.h2p.wait_recv()
            self.d2p = rcopy(b.at[jm, HIH], b.at[jm, HIH], partner)
            self.h2m.wait_recv()
            self.d2m = rcopy(b.at[jp, LO], b.at[jp, LO], partner)

        def third(self):
            b = self.b
            self.fp.wait_recv()
            self.d3p = rcopy(b.at[jo, LO], b.at[jo, LO], partner)
            self.fm.wait_recv()
            self.d3m = rcopy(b.at[jo, HIH], b.at[jo, HIH], partner)

    def mm(buf, pairs, d_even, d_odd, row_even, row_odd, lo, hi):
        def body(i, _):
            e = i % 2
            par = i // 2
            cc = c + par - 2 * c * par
            j = ((y + d_even + e * (d_odd - d_even)) % 4) * 2 + cc
            row = pl.multiple_of(row_even + e * (row_odd - row_even), 256)
            rows = pl.ds(row, 256)
            a = buf[j, rows, :]
            for w, acc in pairs:
                for n in (0, 256):
                    acc[rows, n:n + 256] += dot_nn(a, w[j, :, n:n + 256])
            return 0

        lax.fori_loop(lo, hi, body, 0)

    toks = pl.ds(pl.multiple_of(c * 256, 256), 256)
    ex_a = [None] + [new_recv() for _ in range(3)]
    b0 = counter[0]
    counter[0] += 3
    bs = free[:3]
    del free[:3]
    bs0 = bs[0]

    def ex_b(d, yy):
        return pltpu.make_async_remote_copy(
            src_ref=X.at[pl.ds(2 * yy, 2), toks], dst_ref=XB.at[d - 1, :, toks],
            send_sem=ss.at[bs0 + d - 1], recv_sem=rs.at[b0 + d - 1],
            device_id=at_z(z + d), device_id_type=MESH,
        )

    def exchange(yy):
        yy = yy % 4
        for d in (1, 3, 2):
            t = (x + d) % 4
            cols = pl.ds(pl.multiple_of((t % 2) * 256, 256), 256)
            rcopy(X.at[yy * 2 + t // 2, toks, cols], XA.at[d - 1, yy, toks], at_x(t), ex_a[d])

        @pl.when(yy != z)
        def _():
            ex_b((yy + 4 - z) % 4, yy).start()

    def exchange_relay():
        out = []
        for d in (1, 3, 2):
            wait_all(XA.at[d - 1, :, toks], ex_a[d])
            out.append(rcopy(XA.at[d - 1, :, toks], XA.at[d - 1, :, toks], partner))
        for d in (1, 3, 2):
            ex_b(d, y).wait_recv()
            out.append(rcopy(XB.at[d - 1, :, toks], XB.at[d - 1, :, toks], partner))
        return out

    gx, gg_ = Gather(X), Gather(G)
    vg = ((WV, PV), (WG, PG))
    wo = ((WO, GA),)
    mark("xload")
    loads[0].wait()
    gx.start()
    mark("wload")
    loads[1].wait()
    loads[2].wait()
    mark("x0")
    mm(X, vg, 0, 0, 0, 256, 0, 2)
    gx.d0.wait_recv()
    exchange(y)
    mm(X, vg, 0, 0, 0, 256, 2, 4)
    mark("x1w")
    gx.first()
    loads[3].wait()
    gg_.start()
    mark("x1")
    mm(X, vg, 3, 1, 0, 256, 0, 2)
    gx.d1p.wait_recv()
    gx.d1m.wait_recv()
    exchange(y + 3 + 2 * c)
    mm(X, vg, 3, 1, 0, 256, 2, 4)
    mark("x2w")
    gx.second()
    mark("x2")
    mm(X, vg, 3, 1, 256, 0, 0, 2)
    gx.d2p.wait_recv()
    gx.d2m.wait_recv()
    mm(X, vg, 3, 1, 256, 0, 2, 4)
    mark("x3w")
    gx.third()
    mark("x3")
    mm(X, vg, 2, 2, 0, 256, 0, 2)
    gx.d3p.wait_recv()
    gx.d3m.wait_recv()
    mm(X, vg, 2, 2, 0, 256, 2, 4)

    first_sends = len(sent)
    mark("hidden")
    loads[5].wait()
    loads[6].wait()
    TF[...] = jnp.zeros((32, C), F32)
    TF[0:TAPS, :] = taps_ref[...].astype(F32)
    def hidden_body(i, _):
        rows = pl.ds(pl.multiple_of(i * 32, 32), 32)
        out_rows = pl.ds(pl.multiple_of(i * 32 + PAD, 16), 32)
        for n, cs in enumerate(COLS):
            col = slice(cs, cs + 128)
            s = sig(PG[rows, col])
            PG[rows, col] = s
            HID[n, out_rows, :] = (PV[rows, col] * s).astype(BF16).astype(F32)
        return 0

    lax.fori_loop(0, T // 32, hidden_body, 0)

    following, previous = ((sp + 1) % 16, tp), ((sp + 15) % 16, tp)

    def halo_start(buf):
        up = rcopy(buf.at[:, pl.ds(T, PAD)], buf.at[:, pl.ds(0, PAD)], following)
        down = rcopy(buf.at[:, pl.ds(PAD, PAD)], buf.at[:, pl.ds(T + PAD, PAD)], previous)
        return up, down

    def halo_finish(buf, pair):
        pair[0].wait_recv()
        pair[1].wait_recv()

        @pl.when(sp == 0)
        def _():
            buf[:, 0:PAD, :] = jnp.zeros((4, PAD, 128), F32)

        @pl.when(sp == 15)
        def _():
            buf[:, T + PAD:T + 2 * PAD, :] = jnp.zeros((4, PAD, 128), F32)

    mark("g0")
    halo = halo_start(HID)
    exchange(y + 1 + 2 * c)
    exchange(y + 2)
    loads[4].wait()
    mm(G, wo, 0, 0, 0, 256, 0, 2)
    gg_.d0.wait_recv()
    mm(G, wo, 0, 0, 0, 256, 2, 4)
    mark("halo1w")
    halo_finish(HID, halo)
    mark("g1w")
    gg_.first()

    mark("conv")
    R = 64

    def conv_tile(src, r0, cs, flip):
        acc = jnp.zeros((R, 128), F32)
        for o in range(1, TAPS + 1):
            k = TAPS - o if flip else o - 1
            acc = acc + TF[k:k + 1, cs:cs + 128] * src[cs // 128, pl.ds(r0 + o, R), :]
        return acc

    def conv_body(i, _):
        r0 = pl.multiple_of(i * R, R)
        rows = pl.ds(r0, R)
        s = jnp.zeros((R, 128), F32)
        q = jnp.zeros((R, 128), F32)
        for cs in COLS:
            v = conv_tile(HID, r0, cs, False)
            NRM[rows, cs:cs + 128] = v
            s = s + v
            q = q + v * v
        SA[rows, :] = s
        SQ[rows, :] = q
        return 0

    lax.fori_loop(0, T // R, conv_body, 0)

    def stats_start(e):
        row = lax.broadcasted_iota(jnp.int32, (8, 128), 0)
        dims = (((1,), (1,)), ((), ()))
        tile = lax.dot_general(
            jnp.where(row == 0, 1.0, 0.0).astype(F32), SA[...], dims, precision=HI, preferred_element_type=F32
        ) + lax.dot_general(
            jnp.where(row == 1, 1.0, 0.0).astype(F32), SQ[...], dims, precision=HI, preferred_element_type=F32
        )
        packed = jnp.zeros((8, 128), F32)
        for r in range(4):
            packed = jnp.where(row == r, tile[0:1, 128 * r:128 * r + 128], packed)
            packed = jnp.where(row == r + 4, tile[1:2, 128 * r:128 * r + 128], packed)
        tile = packed
        ST[e] = tile
        STR[e, tp] = tile
        i = new_recv()
        for d in range(1, 8):
            rcopy(ST.at[e], STR.at[e, tp], at_tp((tp + d) % 8), i)
        return i

    def stats_finish(e, i):
        wait_all(STR.at[e, pl.ds(0, 7)], i)
        row = lax.broadcasted_iota(jnp.int32, (64, 256), 0) & 7
        lane = lax.broadcasted_iota(jnp.int32, (64, 256), 1)
        want = jnp.where(lane < 128, 0, 4)
        block = STR[e].reshape(64, 128)
        for t in range(0, T, 128):
            pick = jnp.where(row == want + t // 128, 1.0, 0.0).astype(F32)
            both = lax.dot_general(
                block, pick, (((0,), (0,)), ((), ())), precision=HI, preferred_element_type=F32
            ) * (1.0 / (NB * C))
            if e == 0:
                mean = both[:, :128]
                MEAN[t:t + 128, :] = mean
                INV[t:t + 128, :] = lax.rsqrt(both[:, 128:] - mean * mean + 1e-06)
            else:
                SA[t:t + 128, :] = both[:, :128]
                SQ[t:t + 128, :] = both[:, 128:]

    mark("stats1")
    stats = stats_start(0)
    mark("g1")
    mm(G, wo, 3, 1, 0, 256, 0, 2)
    gg_.d1p.wait_recv()
    gg_.d1m.wait_recv()
    mm(G, wo, 3, 1, 0, 256, 2, 4)
    mark("g2w")
    drain(first_sends)
    gg_.second()
    mark("g2")
    mm(G, wo, 3, 1, 256, 0, 0, 2)
    gg_.d2p.wait_recv()
    gg_.d2m.wait_recv()
    mm(G, wo, 3, 1, 256, 0, 2, 4)
    mark("g3w")
    gg_.third()
    mark("g3")
    mm(G, wo, 2, 2, 0, 256, 0, 2)
    gg_.d3p.wait_recv()
    gg_.d3m.wait_recv()
    mm(G, wo, 2, 2, 0, 256, 2, 4)

    mark("stats1w")
    stats_finish(0, stats)
    mark("scaled")
    GP[...] = jnp.zeros((8, C), F32)

    def scaled_body(i, _):
        rows = pl.ds(pl.multiple_of(i * 32, 32), 32)
        m, iv = MEAN[rows, :], INV[rows, :]
        s1 = jnp.zeros((32, 128), F32)
        s2 = jnp.zeros((32, 128), F32)
        for cs in COLS:
            col = slice(cs, cs + 128)
            n = (NRM[rows, col] - m) * iv
            NRM[rows, col] = n
            gain = gain_ref[0:1, col]
            sc = n * gain
            s = sig(sc)
            ACT[rows, col] = (sc * s).astype(BF16)
            gs = GA[rows, col] * s * (1.0 + sc * (1.0 - s))
            GP[:, col] += (gs * n).reshape(4, 8, 128).sum(axis=0)
            gn = gs * gain
            GA[rows, col] = gn
            s1 = s1 + gn
            s2 = s2 + gn * n
        SA[rows, :] = s1
        SQ[rows, :] = s2
        return 0

    lax.fori_loop(0, T // 32, scaled_body, 0)
    early = len(sent)
    mark("stats2")
    stats = stats_start(1)

    at_p = (at_x, at_z)
    at_q = (at_z, at_x)
    me_p = (x, z)
    me_q = (z, x)

    def dw(lhs, units, left, pair, lo=0, hi=4):
        def body(k, _):
            zz = (z + 2 + k) % 4
            for e in (0, 1):
                r = dot_nn(left, lhs[zz * 2 + pair, :, e * 256:e * 256 + 256]).astype(BF16)
                for n, u in enumerate(units):
                    a = r[n * 512:n * 512 + 256]
                    b = r[n * 512 + 256:n * 512 + 512]
                    part[u, 0, 2 * pair + e, zz] = a
                    part[u, 1, zz, 2 * pair + e] = b
            return 0

        lax.fori_loop(lo, hi, body, 0)

    class Scatter:
        def __init__(self, u, h):
            self.u, self.h = u, h
            self.p, self.q = me_p[h], me_q[h]

        def blk(self, dp, q0, n=2):
            return part.at[self.u, self.h, (self.p + dp) % 4, pl.ds(q0, n)]

        def s1(self):
            u, h, p = self.u, self.h, self.p
            self.a = rcopy(self.blk(2, 0), r1.at[u, h, 0], at_p[h](p + 1))
            self.b = rcopy(self.blk(2, 2), r1.at[u, h, 1], at_p[h](p + 3))

        def s2i(self):
            u, h, p = self.u, self.h, self.p
            self.c = rcopy(self.blk(1, 2), r2.at[u, h, 0, pl.ds(2, 2)], at_p[h](p + 1))
            self.d = rcopy(self.blk(3, 0), r2.at[u, h, 1, pl.ds(0, 2)], at_p[h](p + 3))

        def add(self, dst_index, rows, sources):
            u, h = self.u, self.h

            def body(i, _):
                rr = pl.ds(pl.multiple_of(rows + i * 32, 32), 32)
                v = part[(u, h) + dst_index + (rr,)].astype(F32)
                for ref, index, off in sources:
                    v = v + ref[index + (pl.ds(pl.multiple_of(off + i * 32, 32), 32),)].astype(F32)
                part[(u, h) + dst_index + (rr,)] = v.astype(BF16)
                return 0

            return body

        def s2d(self):
            u, h, p = self.u, self.h, self.p
            self.a.wait_recv()
            for q in (0, 1):
                lax.fori_loop(0, 8, self.add(((p + 1) % 4, q), 0, [(r1, (u, h, 0, q), 0)]), 0)
            self.e = rcopy(self.blk(1, 0), r2.at[u, h, 0, pl.ds(0, 2)], at_p[h](p + 1))
            self.b.wait_recv()
            for q in (2, 3):
                lax.fori_loop(0, 8, self.add(((p + 3) % 4, q), 0, [(r1, (u, h, 1, q - 2), 0)]), 0)
            self.f = rcopy(self.blk(3, 2), r2.at[u, h, 1, pl.ds(2, 2)], at_p[h](p + 3))

        def p1(self):
            u, h, p, q = self.u, self.h, self.p, self.q
            for cp in (self.c, self.d, self.e, self.f):
                cp.wait_recv()
            for dq in (2, 1, 3, 0):
                qq = (q + dq) % 4
                lax.fori_loop(
                    0, 8, self.add((p, qq), 0, [(r2, (u, h, 0, qq), 0), (r2, (u, h, 1, qq), 0)]), 0
                )
                if dq == 2:
                    src = part.at[u, h, p, qq]
                    self.i = rcopy(src.at[pl.ds(0, 128)], r3.at[u, h, 0], at_q[h](q + 1))
                    self.j = rcopy(src.at[pl.ds(128, 128)], r3.at[u, h, 1], at_q[h](q + 3))

        def p2(self):
            u, h, p, q = self.u, self.h, self.p, self.q
            up, down = (q + 1) % 4, (q + 3) % 4
            self.i.wait_recv()
            lax.fori_loop(0, 4, self.add((p, up), 0, [(r3, (u, h, 0), 0)]), 0)
            self.k = new_recv()
            rcopy(part.at[u, h, p, up], r4.at[u, h, 0], at_q[h](q + 1), self.k)
            self.j.wait_recv()
            lax.fori_loop(0, 4, self.add((p, down), 128, [(r3, (u, h, 1), 0)]), 0)
            rcopy(part.at[u, h, p, down], r4.at[u, h, 1], at_q[h](q + 3), self.k)

        def finish(self):
            u, h, p, q = self.u, self.h, self.p, self.q
            wait_all(r4.at[u, h], self.k)
            for i in (0, 128):
                rr = slice(i, i + 128)
                v = (
                    part[u, h, p, q, rr].astype(F32)
                    + r4[u, h, 0, rr].astype(F32)
                    + r4[u, h, 1, rr].astype(F32)
                )
                w_out[u, :, h * 256 + i:h * 256 + i + 128] = v.T.astype(BF16)

    sc = [[Scatter(0, h) for h in (0, 1)]]

    def flipped(src, n):
        eye = (
            lax.broadcasted_iota(jnp.int32, (256, 256), 0) == lax.broadcasted_iota(jnp.int32, (256, 256), 1)
        ).astype(F32).astype(BF16)
        return dot_nt(eye, src[:, n:n + 256]).astype(BF16)

    for n in (0, 256):
        AT[n:n + 256, :] = flipped(ACT, n)
    dw(G, [0], AT[...], 1 - x // 2)
    sc[0][0].s1()
    mark("ow_dw2")
    dw(G, [0], AT[...], x // 2, 0, 1)
    sc[0][1].s1()
    dw(G, [0], AT[...], x // 2, 1, 4)
    mark("stats2w")
    stats_finish(1, stats)

    mark("gc")
    def gc_body(i, _):
        rows = pl.ds(pl.multiple_of(i * 32, 32), 32)
        out_rows = pl.ds(pl.multiple_of(i * 32 + PAD, 16), 32)
        f, s, iv = SA[rows, :], SQ[rows, :], INV[rows, :]
        for cs in COLS:
            col = slice(cs, cs + 128)
            GC[cs // 128, out_rows, :] = iv * (GA[rows, col] - f - NRM[rows, col] * s)
        return 0

    lax.fori_loop(0, T // 32, gc_body, 0)
    halo = halo_start(GC)
    for h in (0, 1):
        sc[0][h].s2i()

    mark("taps")
    for cs in COLS:
        def tap_body(i, accs, cs=cs):
            r0 = pl.multiple_of(i * 32, 32)
            g = GC[cs // 128, pl.ds(r0 + PAD, 32), :]
            accs = list(accs)
            for o in range(1, TAPS + 1):
                prod = HID[cs // 128, pl.ds(r0 + o, 32), :] * g
                accs[o - 1] = accs[o - 1] + prod.reshape(4, 8, 128).sum(axis=0)
            return tuple(accs)

        accs = lax.fori_loop(
            0, T // 32, tap_body, tuple(jnp.zeros((8, 128), F32) for _ in range(TAPS))
        )
        for k, a in enumerate(accs):
            TP[k:k + 1, cs:cs + 128] = jnp.sum(a, axis=0, keepdims=True)
    TP[TAPS:TAPS + 1, :] = jnp.sum(GP[...], axis=0, keepdims=True)

    def small_send(e, src, me, at):
        TGR[e, me] = src(me)[...]
        i = new_recv()
        for d in (1, 3, 2):
            rcopy(src((me + d) % 4), TGR.at[e, me], at(me + d), i)
        return i

    def small_sum(e, i):
        wait_all(TGR.at[e, pl.ds(0, 3)], i)
        v = TGR[e, 0].astype(F32)
        for i in range(1, 4):
            v = v + TGR[e, i].astype(F32)
        return v.astype(BF16)

    for t in range(4):
        TG[t] = TP[:, t * 128:t * 128 + 128].astype(BF16)
    small = small_send(0, lambda t: TG.at[t], x, at_x)
    mark("relay")
    relays = exchange_relay()
    drain(early)
    mark("halo2w")
    halo_finish(GC, halo)

    mark("back")
    def back_body(i, _):
        r0 = pl.multiple_of(i * R, R)
        rows = pl.ds(r0, R)
        for cs in COLS:
            col = slice(cs, cs + 128)
            gh = conv_tile(GC, r0, cs, True)
            s = PG[rows, col]
            gv = gh * s
            GV[rows, col] = gv.astype(BF16)
            GG[rows, col] = (gv * PV[rows, col] * (1.0 - s)).astype(BF16)
        return 0

    lax.fori_loop(0, T // R, back_body, 0)

    middle = len(sent)
    mark("vg_t")
    for n in (0, 256):
        BT[n // 256, 0:256, :] = flipped(GV, n)

    class Spread:
        def __init__(self, h, u):
            self.h, self.p = h, me_p[h]
            self.lo, self.hi = pl.ds(u * 256, 128), pl.ds(u * 256 + 128, 128)

        def start(self):
            h, p, lo, hi = self.h, self.p, self.lo, self.hi
            own, got = BT.at[h], BTR.at[h]
            nxt, prv = at_p[h](p + 1), at_p[h](p + 3)
            self.h1p = rcopy(own.at[lo], got.at[0, lo], nxt)
            self.h1m = rcopy(own.at[hi], got.at[2, hi], prv)
            self.h2p = rcopy(own.at[hi], got.at[0, hi], nxt)
            self.h2m = rcopy(own.at[lo], got.at[2, lo], prv)

        def first(self):
            h, p, lo, hi = self.h, self.p, self.lo, self.hi
            got = BTR.at[h]
            self.h1p.wait_recv()
            self.fp = rcopy(got.at[0, lo], got.at[1, lo], at_p[h](p + 1))
            self.h1m.wait_recv()
            self.fm = rcopy(got.at[2, hi], got.at[1, hi], at_p[h](p + 3))

        def second(self):
            self.h2p.wait_recv()
            self.h2m.wait_recv()

        def third(self):
            self.fp.wait_recv()
            self.fm.wait_recv()

    def own_in(h, q):
        zz, xx = (q, x) if h == 0 else (z, q)
        cols = pl.ds(pl.multiple_of((xx % 2) * 256, 256), 256)
        return X[zz * 2 + xx // 2, :, cols]

    def got_in(h, k, q):
        if h == 0:
            return XA[k, q]
        return XB[k, q // 2, :, pl.ds(pl.multiple_of((q % 2) * 256, 256), 256)]

    def vg_own(h):
        def body(q, _):
            VACC[h, q] = dot_nn(BT[h], own_in(h, q))
            return 0

        lax.fori_loop(0, 4, body, 0)

    def vg_near(h, u):
        rows = pl.ds(u * 256, 256)

        def body(q, _):
            VACC[h, q, rows] += dot_nn(BTR[h, 0, rows], got_in(h, 0, q)) + dot_nn(BTR[h, 2, rows], got_in(h, 2, q))
            return 0

        lax.fori_loop(0, 4, body, 0)

    class Last:
        def __init__(self, h, u):
            self.h, self.u, self.q = h, u, me_q[h]
            self.rows = pl.ds(u * 256, 256)

        def make(self, dq):
            h, rows = self.h, self.rows
            qq = (self.q + dq) % 4
            VP[h, qq, rows] = (VACC[h, qq, rows] + dot_nn(BTR[h, 1, rows], got_in(h, 1, qq))).astype(BF16)

        def s1(self):
            h, u, q = self.h, self.u, self.q
            src = VP.at[h, (q + 2) % 4]
            self.i = rcopy(src.at[pl.ds(u * 256, 128)], r3v.at[h, u, 0], at_q[h](q + 1))
            self.j = rcopy(src.at[pl.ds(u * 256 + 128, 128)], r3v.at[h, u, 1], at_q[h](q + 3))

        def s2(self):
            h, u, q, rows = self.h, self.u, self.q, self.rows

            def add(qq, row0, k):
                def body(i, _):
                    rr = pl.ds(pl.multiple_of(row0 + i * 64, 64), 64)
                    fr = pl.ds(pl.multiple_of(i * 64, 64), 64)
                    VP[h, qq, rr] = (VP[h, qq, rr].astype(F32) + r3v[h, u, k, fr].astype(F32)).astype(BF16)
                    return 0

                lax.fori_loop(0, 2, body, 0)

            up, down = (q + 1) % 4, (q + 3) % 4
            self.i.wait_recv()
            add(up, u * 256, 0)
            self.k = new_recv()
            rcopy(VP.at[h, up, rows], r4v.at[h, 0, rows], at_q[h](q + 1), self.k)
            self.j.wait_recv()
            add(down, u * 256 + 128, 1)
            rcopy(VP.at[h, down, rows], r4v.at[h, 1, rows], at_q[h](q + 3), self.k)

        def finish(self):
            h, u, q = self.h, self.u, self.q
            wait_all(r4v.at[h, :, self.rows], self.k)
            for i in (0, 128):
                rr = slice(u * 256 + i, u * 256 + i + 128)
                v = VP[h, q, rr].astype(F32) + r4v[h, 0, rr].astype(F32) + r4v[h, 1, rr].astype(F32)
                w_out[u + 1, :, h * 256 + i:h * 256 + i + 128] = v.T.astype(BF16)

    spread = [[Spread(0, u), Spread(1, u)] for u in (0, 1)]
    last = [[Last(0, u), Last(1, u)] for u in (0, 1)]
    for h in (0, 1):
        spread[0][h].start()
    for n in (0, 256):
        BT[n // 256, 256:512, :] = flipped(GG, n)

    mark("partial1")
    def partial(parity):
        def body(i, _):
            yy = i // 2
            rows = pl.ds(pl.multiple_of((i % 2) * 256, 256), 256)
            j = yy * 2 + parity
            gv, gt = GV[rows, :], GG[rows, :]
            for n in (0, 256):
                G[parity * 4 + yy, rows, n:n + 256] = (
                    dot_nt(gv, WV[j, n:n + 256, :]) + dot_nt(gt, WG[j, n:n + 256, :])
                ).astype(BF16)
            return 0

        lax.fori_loop(0, 8, body, 0)

    partial(1 - c)
    swap = rcopy(G.at[pl.ds((1 - c) * 4, 4)], PR, partner)
    mark("small")
    TG1[0] = small_sum(0, small)
    small = small_send(1, lambda t: TG1.at[0], z, at_z)
    mark("v_first")
    for h in (0, 1):
        spread[0][h].first()
    for h in (0, 1):
        spread[1][h].start()
    mark("ow_s2d")
    for h in (0, 1):
        sc[0][h].s2d()
    mark("partial2")
    partial(c)
    mark("yadd")
    swap.wait_recv()

    def y_add(block, row0, n, sources):
        def body(i, _):
            rr = pl.ds(pl.multiple_of(row0 + i * 32, 32), 32)
            v = G[block, rr].astype(F32)
            for ref, index, off in sources:
                v = v + ref[index + (pl.ds(pl.multiple_of(off + i * 32, 32), 32),)].astype(F32)
            G[block, rr] = v.astype(BF16)
            return 0

        lax.fori_loop(0, n // 32, body, 0)

    base = c * 4
    y2_, yp_, ym_ = (y + 2) % 4, (y + 1) % 4, (y + 3) % 4
    y_add(base + y2_, 0, T, [(PR, (y2_,), 0)])
    ya = rcopy(G.at[base + y2_, LO], y1.at[0], at_y(y + 1))
    yb = rcopy(G.at[base + y2_, HIH], y1.at[1], at_y(y + 3))
    y_add(base + yp_, 0, T, [(PR, (yp_,), 0)])
    yc = rcopy(G.at[base + yp_, HIH], y2.at[0, HIH], at_y(y + 1))
    y_add(base + ym_, 0, T, [(PR, (ym_,), 0)])
    yd = rcopy(G.at[base + ym_, LO], y2.at[1, LO], at_y(y + 3))
    y_add(base + y, 0, T, [(PR, (y,), 0)])

    mark("small2")
    TG1[1] = small_sum(1, small)
    small = small_send(2, lambda t: TG1.at[1], x, at_x)
    mark("vg_own")
    for h in (0, 1):
        vg_own(h)
    third = len(sent) - middle
    mark("v_near")
    for cp in relays:
        cp.wait_recv()
    drain(middle)
    for h in (0, 1):
        spread[0][h].second()
    for h in (0, 1):
        vg_near(h, 0)
    mark("v_third")
    for h in (0, 1):
        spread[0][h].third()
    mark("v_far")
    for h in (0, 1):
        last[0][h].make(2)
        last[0][h].s1()
    for dq in (1, 3, 0):
        for h in (0, 1):
            last[0][h].make(dq)
    mark("g_first")
    for h in (0, 1):
        spread[1][h].first()
    mark("y_s2")
    ya.wait_recv()
    y_add(base + yp_, 0, 256, [(y1, (0,), 0)])
    ye = rcopy(G.at[base + yp_, LO], y2.at[0, LO], at_y(y + 1))
    yb.wait_recv()
    y_add(base + ym_, 256, 256, [(y1, (1,), 0)])
    yf = rcopy(G.at[base + ym_, HIH], y2.at[1, HIH], at_y(y + 3))
    mark("g_second")
    for h in (0, 1):
        spread[1][h].second()
    mark("g_near")
    for h in (0, 1):
        vg_near(h, 1)
    drain(third)
    mark("ow_p1")
    for h in (0, 1):
        sc[0][h].p1()
    mark("v_s2")
    for h in (0, 1):
        last[0][h].s2()
    mark("g_third")
    for h in (0, 1):
        spread[1][h].third()
    mark("g_far")
    for h in (0, 1):
        last[1][h].make(2)
        last[1][h].s1()
    mark("ow_p2")
    for h in (0, 1):
        sc[0][h].p2()
    mark("g_rest")
    for dq in (1, 3, 0):
        for h in (0, 1):
            last[1][h].make(dq)
    mark("g_s2")
    for h in (0, 1):
        last[1][h].s2()
    mark("small3")
    wait_all(TGR.at[2, pl.ds(0, 3)], small)
    for t in range(4):
        small_out[:, t * 128:t * 128 + 128] = TGR[2, t].astype(F32)
    mark("y_fin")
    for cp in (yc, yd, ye, yf):
        cp.wait_recv()

    def gi_body(i, _):
        rr = pl.ds(pl.multiple_of(i * 32, 32), 32)
        gi_out[rr, :] = (
            G[base + y, rr].astype(F32) + y2[0, rr].astype(F32) + y2[1, rr].astype(F32)
        ).astype(BF16)
        return 0

    lax.fori_loop(0, T // 32, gi_body, 0)
    mark("fin_v")
    for h in (0, 1):
        last[0][h].finish()
    mark("fin_o")
    for h in (0, 1):
        sc[0][h].finish()
    mark("fin_g")
    for h in (0, 1):
        last[1][h].finish()
    mark("sends")
    drain(len(sent))
    for d in (1, 2, 3):
        ex_b(d, (z + d) % 4).wait_send()
    mark(None)
    assert counter[0] == N_COPIES


def unpack(gi_in, w_in, small_in, gi, gvw, ggw, gow, gt, gg, b_out, so):
    writes = [pltpu.make_async_copy(gi_in, gi, so.at[3])]
    writes[0].start()
    for u, dst in enumerate((gow, gvw, ggw)):
        b_out[u] = w_in[u].astype(F32)
        writes.append(pltpu.make_async_copy(b_out.at[u], dst, so.at[u]))
        writes[-1].start()
    gt[...] = small_in[0:TAPS]
    gg[...] = small_in[TAPS:TAPS + 1]
    for cp in writes:
        cp.wait()


def local(inputs, w_value, w_gate, taps, ln_gain, w_out, grad_out):
    vm = pltpu.VMEM
    anyspace = pl.BlockSpec(memory_space=pl.ANY)
    in_vmem = pl.BlockSpec(memory_space=pltpu.VMEM)
    shape3 = (NB, C, C)
    gi, w3, small = pl.pallas_call(
        kernel,
        out_shape=(
            vm((T, C), BF16),
            vm((3, 256, C), BF16),
            vm((32, C), F32),
        ),
        in_specs=[anyspace] * 7,
        out_specs=(in_vmem,) * 3,
        scratch_shapes=[
            vm((NB, T, C), BF16), vm((NB, T, C), BF16),
            vm(shape3, BF16), vm(shape3, BF16), vm(shape3, BF16),
            vm((T, C), F32), vm((T, C), F32), vm((T, C), F32), vm((T, C), F32),
            vm((4, T + 2 * PAD, 128), F32), vm((4, T + 2 * PAD, 128), F32),
            vm((T, C), BF16), vm((T, C), BF16), vm((T, C), BF16),
            vm((512, T), BF16), vm((2, 512, T), BF16),
            vm((T, 128), F32), vm((T, 128), F32), vm((T, 128), F32), vm((T, 128), F32),
            vm((32, C), F32),
            vm((2, 8, 128), F32), vm((2, NB, 8, 128), F32),
            vm((32, C), F32), vm((8, C), F32),
            vm((4, 32, 128), BF16), vm((2, 32, 128), BF16), vm((3, 4, 32, 128), BF16),
            vm((1, 2, 4, 4, 256, 256), BF16),
            vm((1, 2, 2, 2, 256, 256), BF16),
            vm((1, 2, 2, 4, 256, 256), BF16),
            vm((1, 2, 2, 128, 256), BF16),
            vm((1, 2, 2, 256, 256), BF16),
            vm((3, 4, T, 256), BF16), vm((3, 2, T, C), BF16),
            vm((2, 3, 512, T), BF16),
            vm((2, 4, 512, 256), F32), vm((2, 4, 512, 256), BF16),
            vm((2, 2, 2, 128, 256), BF16), vm((2, 2, 512, 256), BF16),
            vm((4, T, C), BF16),
            vm((2, 256, C), BF16), vm((2, T, C), BF16),
            vm((TAPS, C), BF16), vm((1, C), F32),
            pltpu.SemaphoreType.DMA((N_SENDS,)),
            pltpu.SemaphoreType.DMA((N_COPIES,)),
            pltpu.SemaphoreType.DMA((7,)),
        ],
        compiler_params=pltpu.CompilerParams(
            collective_id=0, has_side_effects=True, vmem_limit_bytes=64 * 1024 * 1024 - 3 * 1024 * 1024
        ),
    )(
        inputs, grad_out, w_value.reshape(shape3), w_gate.reshape(shape3), w_out.reshape(shape3),
        taps, ln_gain.reshape(1, C),
    )
    gi, gvw, ggw, gow, gt, gg = pl.pallas_call(
        unpack,
        out_shape=(
            jax.ShapeDtypeStruct((T, C), BF16),
            jax.ShapeDtypeStruct((256, C), F32),
            jax.ShapeDtypeStruct((256, C), F32),
            jax.ShapeDtypeStruct((256, C), F32),
            jax.ShapeDtypeStruct((TAPS, C), F32),
            jax.ShapeDtypeStruct((1, C), F32),
        ),
        in_specs=[in_vmem] * 3,
        out_specs=(anyspace,) * 4 + (in_vmem,) * 2,
        scratch_shapes=[vm((3, 256, C), F32), pltpu.SemaphoreType.DMA((4,))],
        compiler_params=pltpu.CompilerParams(vmem_limit_bytes=8 * 1024 * 1024),
    )(gi, w3, small)
    return gi, gvw, ggw, gow, gt, gg.reshape(C)


def solution(mesh):
    in_specs = (
        P("sp", "tp"), P(None, "tp"), P(None, "tp"), P(None, "tp"), P("tp"), P(None, "tp"), P("sp", "tp"),
    )
    out_specs = (P("sp", "tp"), P("sp", "tp"), P("sp", "tp"), P("sp", "tp"), P(None, "tp"), P("tp"))
    return jax.shard_map(local, mesh=mesh, in_specs=in_specs, out_specs=out_specs, check_vma=False)
```

```python
import jax
import jax.numpy as jnp
from jax import lax
from jax.experimental import pallas as pl
from jax.experimental.pallas import tpu as pltpu
from jax.sharding import PartitionSpec as P

MESH = pl.DeviceIdType.MESH
F32 = jnp.float32
BF16 = jnp.bfloat16
HI = lax.Precision.HIGHEST
T = 512
C = 512
NB = 8
RAD = 15
TAPS = 31
PAD = 16
COLS = (0, 128, 256, 384)
N_COPIES = 108
N_SENDS = 64


def sig(v):
    return 1.0 / (1.0 + jnp.exp(-v))


def dot_nn(a, b):
    return lax.dot_general(a, b, (((1,), (0,)), ((), ())), preferred_element_type=F32)


def dot_nt(a, b):
    return lax.dot_general(a, b, (((1,), (1,)), ((), ())), preferred_element_type=F32)


def dot_tn(a, b):
    return lax.dot_general(a, b, (((0,), (0,)), ((), ())), preferred_element_type=F32)


def kernel(
    x_hbm, g_hbm, wv_hbm, wg_hbm, wo_hbm, taps_hbm, gain_hbm,
    gi_out, w_out, small_out,
    X, G, WV, WG, WO, PV, PG, GA, NRM, HID, GC, ACT, GV, GG, AT, BT,
    SA, SQ, MEAN, INV, TF, ST, STR, TP, GP, TG, TG1, TGR,
    part, r1, r2, r3, r4, XA, XB, BTR, VACC, VP, r3v, r4v, PR, y1, y2, taps_ref, gain_ref, ss, rs, ls,
):
    sp = lax.axis_index("sp")
    tp = lax.axis_index("tp")
    z, x = sp // 4, sp % 4
    y, c = tp // 2, tp % 2

    def at_tp(t):
        return (sp, t)

    def at_y(yy):
        return (sp, (yy % 4) * 2 + c)

    def at_x(xx):
        return (z * 4 + xx % 4, tp)

    def at_z(zz):
        return ((zz % 4) * 4 + x, tp)

    partner = at_tp(y * 2 + (1 - c))

    scope = [None]

    def mark(name):
        if scope[0] is not None:
            scope[0].__exit__(None, None, None)
        scope[0] = jax.named_scope(name) if name else None
        if name:
            scope[0].__enter__()

    counter = [0]
    free = list(range(N_SENDS))
    sent = []

    def new_recv():
        counter[0] += 1
        return counter[0] - 1

    def wait_all(ref, i):
        pltpu.make_async_remote_copy(
            src_ref=ref, dst_ref=ref, send_sem=ss.at[0], recv_sem=rs.at[i],
            device_id=partner, device_id_type=MESH,
        ).wait_recv()

    def rcopy(src, dst, dev, recv=None):
        i = new_recv() if recv is None else recv
        k = free.pop(0)
        cp = pltpu.make_async_remote_copy(
            src_ref=src, dst_ref=dst, send_sem=ss.at[k], recv_sem=rs.at[i],
            device_id=dev, device_id_type=MESH,
        )
        cp.start()
        sent.append((cp, k))
        return cp

    def drain(count):
        for cp, k in sent[:count]:
            cp.wait_send()
            free.append(k)
        free.sort()
        del sent[:count]

    mark("entry")
    loads = []
    for i, (src, dst) in enumerate(
        ((x_hbm, X.at[tp]), (wv_hbm, WV), (wg_hbm, WG), (g_hbm, G.at[tp]), (wo_hbm, WO),
         (taps_hbm, taps_ref), (gain_hbm, gain_ref))
    ):
        cp = pltpu.make_async_copy(src, dst, ls.at[i])
        cp.start()
        loads.append(cp)

    barrier = pltpu.get_barrier_semaphore()
    peers = [at_tp((tp + d) % 8) for d in range(1, 8)]
    peers += [at_x(x + d) for d in range(1, 4)] + [at_z(z + d) for d in range(1, 4)]
    peers += [((sp + 1) % 16, tp), ((sp + 15) % 16, tp)]
    for dev in peers:
        pl.semaphore_signal(barrier, inc=1, device_id=dev, device_id_type=MESH)
    PV[...] = jnp.zeros((T, C), F32)
    PG[...] = jnp.zeros((T, C), F32)
    GA[...] = jnp.zeros((T, C), F32)
    pl.semaphore_wait(barrier, len(peers))

    jm = ((y + 3) % 4) * 2 + c
    jp = ((y + 1) % 4) * 2 + c
    jo = ((y + 2) % 4) * 2 + c
    LO, HIH = pl.ds(0, 256), pl.ds(256, 256)

    class Gather:
        def __init__(self, buf):
            self.b = buf

        def start(self):
            b = self.b
            self.h1p = rcopy(b.at[tp, LO], b.at[tp, LO], at_y(y + 1))
            self.h1m = rcopy(b.at[tp, HIH], b.at[tp, HIH], at_y(y + 3))
            self.d0 = rcopy(b.at[tp], b.at[tp], partner)
            self.h2p = rcopy(b.at[tp, HIH], b.at[tp, HIH], at_y(y + 1))
            self.h2m = rcopy(b.at[tp, LO], b.at[tp, LO], at_y(y + 3))

        def first(self):
            b = self.b
            self.h1p.wait_recv()
            self.fp = rcopy(b.at[jm, LO], b.at[jm, LO], at_y(y + 1))
            self.d1p = rcopy(b.at[jm, LO], b.at[jm, LO], partner)
            self.h1m.wait_recv()
            self.fm = rcopy(b.at[jp, HIH], b.at[jp, HIH], at_y(y + 3))
            self.d1m = rcopy(b.at[jp, HIH], b.at[jp, HIH], partner)

        def second(self):
            b = self.b
            self.h2p.wait_recv()
            self.d2p = rcopy(b.at[jm, HIH], b.at[jm, HIH], partner)
            self.h2m.wait_recv()
            self.d2m = rcopy(b.at[jp, LO], b.at[jp, LO], partner)

        def third(self):
            b = self.b
            self.fp.wait_recv()
            self.d3p = rcopy(b.at[jo, LO], b.at[jo, LO], partner)
            self.fm.wait_recv()
            self.d3m = rcopy(b.at[jo, HIH], b.at[jo, HIH], partner)

    def mm(buf, pairs, d_even, d_odd, row_even, row_odd, lo, hi):
        def body(i, _):
            e = i % 2
            par = i // 2
            cc = c + par - 2 * c * par
            j = ((y + d_even + e * (d_odd - d_even)) % 4) * 2 + cc
            row = pl.multiple_of(row_even + e * (row_odd - row_even), 256)
            rows = pl.ds(row, 256)
            a = buf[j, rows, :]
            for w, acc in pairs:
                for n in (0, 256):
                    acc[rows, n:n + 256] += dot_nn(a, w[j, :, n:n + 256])
            return 0

        lax.fori_loop(lo, hi, body, 0)

    toks = pl.ds(pl.multiple_of(c * 256, 256), 256)
    ex_a = [None] + [new_recv() for _ in range(3)]
    b0 = counter[0]
    counter[0] += 3
    bs = free[:3]
    del free[:3]
    bs0 = bs[0]

    def ex_b(d, yy):
        return pltpu.make_async_remote_copy(
            src_ref=X.at[pl.ds(2 * yy, 2), toks], dst_ref=XB.at[d - 1, :, toks],
            send_sem=ss.at[bs0 + d - 1], recv_sem=rs.at[b0 + d - 1],
            device_id=at_z(z + d), device_id_type=MESH,
        )

    def exchange(yy):
        yy = yy % 4
        for d in (1, 3, 2):
            t = (x + d) % 4
            cols = pl.ds(pl.multiple_of((t % 2) * 256, 256), 256)
            rcopy(X.at[yy * 2 + t // 2, toks, cols], XA.at[d - 1, yy, toks], at_x(t), ex_a[d])

        @pl.when(yy != z)
        def _():
            ex_b((yy + 4 - z) % 4, yy).start()

    def exchange_relay():
        out = []
        for d in (1, 3, 2):
            wait_all(XA.at[d - 1, :, toks], ex_a[d])
            out.append(rcopy(XA.at[d - 1, :, toks], XA.at[d - 1, :, toks], partner))
        for d in (1, 3, 2):
            ex_b(d, y).wait_recv()
            out.append(rcopy(XB.at[d - 1, :, toks], XB.at[d - 1, :, toks], partner))
        return out

    gx, gg_ = Gather(X), Gather(G)
    vg = ((WV, PV), (WG, PG))
    wo = ((WO, GA),)
    mark("xload")
    loads[0].wait()
    gx.start()
    mark("wload")
    loads[1].wait()
    loads[2].wait()
    mark("x0")
    mm(X, vg, 0, 0, 0, 256, 0, 2)
    gx.d0.wait_recv()
    exchange(y)
    mm(X, vg, 0, 0, 0, 256, 2, 4)
    mark("x1w")
    gx.first()
    loads[3].wait()
    gg_.start()
    mark("x1")
    mm(X, vg, 3, 1, 0, 256, 0, 2)
    gx.d1p.wait_recv()
    gx.d1m.wait_recv()
    exchange(y + 3 + 2 * c)
    mm(X, vg, 3, 1, 0, 256, 2, 4)
    mark("x2w")
    gx.second()
    mark("x2")
    mm(X, vg, 3, 1, 256, 0, 0, 2)
    gx.d2p.wait_recv()
    gx.d2m.wait_recv()
    mm(X, vg, 3, 1, 256, 0, 2, 4)
    mark("x3w")
    gx.third()
    mark("x3")
    mm(X, vg, 2, 2, 0, 256, 0, 2)
    gx.d3p.wait_recv()
    gx.d3m.wait_recv()
    mm(X, vg, 2, 2, 0, 256, 2, 4)

    first_sends = len(sent)
    mark("hidden")
    loads[5].wait()
    loads[6].wait()
    TF[...] = jnp.zeros((32, C), F32)
    TF[0:TAPS, :] = taps_ref[...].astype(F32)
    def hidden_body(i, _):
        rows = pl.ds(pl.multiple_of(i * 32, 32), 32)
        out_rows = pl.ds(pl.multiple_of(i * 32 + PAD, 16), 32)
        for n, cs in enumerate(COLS):
            col = slice(cs, cs + 128)
            s = sig(PG[rows, col])
            PG[rows, col] = s
            HID[n, out_rows, :] = (PV[rows, col] * s).astype(BF16).astype(F32)
        return 0

    lax.fori_loop(0, T // 32, hidden_body, 0)

    following, previous = ((sp + 1) % 16, tp), ((sp + 15) % 16, tp)

    def halo_start(buf):
        up = rcopy(buf.at[:, pl.ds(T, PAD)], buf.at[:, pl.ds(0, PAD)], following)
        down = rcopy(buf.at[:, pl.ds(PAD, PAD)], buf.at[:, pl.ds(T + PAD, PAD)], previous)
        return up, down

    def halo_finish(buf, pair):
        pair[0].wait_recv()
        pair[1].wait_recv()

        @pl.when(sp == 0)
        def _():
            buf[:, 0:PAD, :] = jnp.zeros((4, PAD, 128), F32)

        @pl.when(sp == 15)
        def _():
            buf[:, T + PAD:T + 2 * PAD, :] = jnp.zeros((4, PAD, 128), F32)

    mark("g0")
    halo = halo_start(HID)
    exchange(y + 1 + 2 * c)
    exchange(y + 2)
    loads[4].wait()
    mm(G, wo, 0, 0, 0, 256, 0, 2)
    gg_.d0.wait_recv()
    mm(G, wo, 0, 0, 0, 256, 2, 4)
    mark("halo1w")
    halo_finish(HID, halo)
    mark("g1w")
    gg_.first()

    mark("conv")
    R = 64

    def conv_tile(src, r0, cs, flip):
        acc = jnp.zeros((R, 128), F32)
        for o in range(1, TAPS + 1):
            k = TAPS - o if flip else o - 1
            acc = acc + TF[k:k + 1, cs:cs + 128] * src[cs // 128, pl.ds(r0 + o, R), :]
        return acc

    def conv_body(i, _):
        r0 = pl.multiple_of(i * R, R)
        rows = pl.ds(r0, R)
        s = jnp.zeros((R, 128), F32)
        q = jnp.zeros((R, 128), F32)
        for cs in COLS:
            v = conv_tile(HID, r0, cs, False)
            NRM[rows, cs:cs + 128] = v
            s = s + v
            q = q + v * v
        SA[rows, :] = s
        SQ[rows, :] = q
        return 0

    lax.fori_loop(0, T // R, conv_body, 0)

    def stats_start(e):
        row = lax.broadcasted_iota(jnp.int32, (8, 128), 0)
        dims = (((1,), (1,)), ((), ()))
        tile = lax.dot_general(
            jnp.where(row == 0, 1.0, 0.0).astype(F32), SA[...], dims, precision=HI, preferred_element_type=F32
        ) + lax.dot_general(
            jnp.where(row == 1, 1.0, 0.0).astype(F32), SQ[...], dims, precision=HI, preferred_element_type=F32
        )
        packed = jnp.zeros((8, 128), F32)
        for r in range(4):
            packed = jnp.where(row == r, tile[0:1, 128 * r:128 * r + 128], packed)
            packed = jnp.where(row == r + 4, tile[1:2, 128 * r:128 * r + 128], packed)
        tile = packed
        ST[e] = tile
        STR[e, tp] = tile
        i = new_recv()
        for d in range(1, 8):
            rcopy(ST.at[e], STR.at[e, tp], at_tp((tp + d) % 8), i)
        return i

    def stats_finish(e, i):
        wait_all(STR.at[e, pl.ds(0, 7)], i)
        row = lax.broadcasted_iota(jnp.int32, (64, 256), 0) & 7
        lane = lax.broadcasted_iota(jnp.int32, (64, 256), 1)
        want = jnp.where(lane < 128, 0, 4)
        block = STR[e].reshape(64, 128)
        for t in range(0, T, 128):
            pick = jnp.where(row == want + t // 128, 1.0, 0.0).astype(F32)
            both = lax.dot_general(
                block, pick, (((0,), (0,)), ((), ())), precision=HI, preferred_element_type=F32
            ) * (1.0 / (NB * C))
            if e == 0:
                mean = both[:, :128]
                MEAN[t:t + 128, :] = mean
                INV[t:t + 128, :] = lax.rsqrt(both[:, 128:] - mean * mean + 1e-06)
            else:
                SA[t:t + 128, :] = both[:, :128]
                SQ[t:t + 128, :] = both[:, 128:]

    mark("stats1")
    stats = stats_start(0)
    mark("g1")
    mm(G, wo, 3, 1, 0, 256, 0, 2)
    gg_.d1p.wait_recv()
    gg_.d1m.wait_recv()
    mm(G, wo, 3, 1, 0, 256, 2, 4)
    mark("g2w")
    drain(first_sends)
    gg_.second()
    mark("g2")
    mm(G, wo, 3, 1, 256, 0, 0, 2)
    gg_.d2p.wait_recv()
    gg_.d2m.wait_recv()
    mm(G, wo, 3, 1, 256, 0, 2, 4)
    mark("g3w")
    gg_.third()
    mark("g3")
    mm(G, wo, 2, 2, 0, 256, 0, 2)
    gg_.d3p.wait_recv()
    gg_.d3m.wait_recv()
    mm(G, wo, 2, 2, 0, 256, 2, 4)

    mark("stats1w")
    stats_finish(0, stats)
    mark("scaled")
    GP[...] = jnp.zeros((8, C), F32)

    def scaled_body(i, _):
        rows = pl.ds(pl.multiple_of(i * 32, 32), 32)
        m, iv = MEAN[rows, :], INV[rows, :]
        s1 = jnp.zeros((32, 128), F32)
        s2 = jnp.zeros((32, 128), F32)
        for cs in COLS:
            col = slice(cs, cs + 128)
            n = (NRM[rows, col] - m) * iv
            NRM[rows, col] = n
            gain = gain_ref[0:1, col]
            sc = n * gain
            s = sig(sc)
            ACT[rows, col] = (sc * s).astype(BF16)
            gs = GA[rows, col] * s * (1.0 + sc * (1.0 - s))
            GP[:, col] += (gs * n).reshape(4, 8, 128).sum(axis=0)
            gn = gs * gain
            GA[rows, col] = gn
            s1 = s1 + gn
            s2 = s2 + gn * n
        SA[rows, :] = s1
        SQ[rows, :] = s2
        return 0

    lax.fori_loop(0, T // 32, scaled_body, 0)
    early = len(sent)
    mark("stats2")
    stats = stats_start(1)

    at_p = (at_x, at_z)
    at_q = (at_z, at_x)
    me_p = (x, z)
    me_q = (z, x)

    def dw(lhs, units, left, pair, lo=0, hi=4):
        def body(k, _):
            zz = (z + 2 + k) % 4
            for e in (0, 1):
                r = dot_nn(left, lhs[zz * 2 + pair, :, e * 256:e * 256 + 256]).astype(BF16)
                for n, u in enumerate(units):
                    a = r[n * 512:n * 512 + 256]
                    b = r[n * 512 + 256:n * 512 + 512]
                    part[u, 0, 2 * pair + e, zz] = a
                    part[u, 1, zz, 2 * pair + e] = b
            return 0

        lax.fori_loop(lo, hi, body, 0)

    class Scatter:
        def __init__(self, u, h):
            self.u, self.h = u, h
            self.p, self.q = me_p[h], me_q[h]

        def blk(self, dp, q0, n=2):
            return part.at[self.u, self.h, (self.p + dp) % 4, pl.ds(q0, n)]

        def s1(self):
            u, h, p = self.u, self.h, self.p
            self.a = rcopy(self.blk(2, 0), r1.at[u, h, 0], at_p[h](p + 1))
            self.b = rcopy(self.blk(2, 2), r1.at[u, h, 1], at_p[h](p + 3))

        def s2i(self):
            u, h, p = self.u, self.h, self.p
            self.c = rcopy(self.blk(1, 2), r2.at[u, h, 0, pl.ds(2, 2)], at_p[h](p + 1))
            self.d = rcopy(self.blk(3, 0), r2.at[u, h, 1, pl.ds(0, 2)], at_p[h](p + 3))

        def add(self, dst_index, rows, sources):
            u, h = self.u, self.h

            def body(i, _):
                rr = pl.ds(pl.multiple_of(rows + i * 32, 32), 32)
                v = part[(u, h) + dst_index + (rr,)].astype(F32)
                for ref, index, off in sources:
                    v = v + ref[index + (pl.ds(pl.multiple_of(off + i * 32, 32), 32),)].astype(F32)
                part[(u, h) + dst_index + (rr,)] = v.astype(BF16)
                return 0

            return body

        def s2d(self):
            u, h, p = self.u, self.h, self.p
            self.a.wait_recv()
            for q in (0, 1):
                lax.fori_loop(0, 8, self.add(((p + 1) % 4, q), 0, [(r1, (u, h, 0, q), 0)]), 0)
            self.e = rcopy(self.blk(1, 0), r2.at[u, h, 0, pl.ds(0, 2)], at_p[h](p + 1))
            self.b.wait_recv()
            for q in (2, 3):
                lax.fori_loop(0, 8, self.add(((p + 3) % 4, q), 0, [(r1, (u, h, 1, q - 2), 0)]), 0)
            self.f = rcopy(self.blk(3, 2), r2.at[u, h, 1, pl.ds(2, 2)], at_p[h](p + 3))

        def p1(self):
            u, h, p, q = self.u, self.h, self.p, self.q
            for cp in (self.c, self.d, self.e, self.f):
                cp.wait_recv()
            for dq in (2, 1, 3, 0):
                qq = (q + dq) % 4
                lax.fori_loop(
                    0, 8, self.add((p, qq), 0, [(r2, (u, h, 0, qq), 0), (r2, (u, h, 1, qq), 0)]), 0
                )
                if dq == 2:
                    src = part.at[u, h, p, qq]
                    self.i = rcopy(src.at[pl.ds(0, 128)], r3.at[u, h, 0], at_q[h](q + 1))
                    self.j = rcopy(src.at[pl.ds(128, 128)], r3.at[u, h, 1], at_q[h](q + 3))

        def p2(self):
            u, h, p, q = self.u, self.h, self.p, self.q
            up, down = (q + 1) % 4, (q + 3) % 4
            self.i.wait_recv()
            lax.fori_loop(0, 4, self.add((p, up), 0, [(r3, (u, h, 0), 0)]), 0)
            self.k = new_recv()
            rcopy(part.at[u, h, p, up], r4.at[u, h, 0], at_q[h](q + 1), self.k)
            self.j.wait_recv()
            lax.fori_loop(0, 4, self.add((p, down), 128, [(r3, (u, h, 1), 0)]), 0)
            rcopy(part.at[u, h, p, down], r4.at[u, h, 1], at_q[h](q + 3), self.k)

        def finish(self):
            u, h, p, q = self.u, self.h, self.p, self.q
            wait_all(r4.at[u, h], self.k)
            for i in (0, 128):
                rr = slice(i, i + 128)
                v = (
                    part[u, h, p, q, rr].astype(F32)
                    + r4[u, h, 0, rr].astype(F32)
                    + r4[u, h, 1, rr].astype(F32)
                )
                w_out[u, :, h * 256 + i:h * 256 + i + 128] = v.T.astype(BF16)

    sc = [[Scatter(0, h) for h in (0, 1)]]

    def flipped(src, n):
        eye = (
            lax.broadcasted_iota(jnp.int32, (256, 256), 0) == lax.broadcasted_iota(jnp.int32, (256, 256), 1)
        ).astype(F32).astype(BF16)
        return dot_nt(eye, src[:, n:n + 256]).astype(BF16)

    for n in (0, 256):
        AT[n:n + 256, :] = flipped(ACT, n)
    dw(G, [0], AT[...], 1 - x // 2)
    sc[0][0].s1()
    mark("ow_dw2")
    dw(G, [0], AT[...], x // 2, 0, 1)
    sc[0][1].s1()
    mark("stats2w")
    stats_finish(1, stats)

    mark("gc")
    def gc_body(i, _):
        rows = pl.ds(pl.multiple_of(i * 32, 32), 32)
        out_rows = pl.ds(pl.multiple_of(i * 32 + PAD, 16), 32)
        f, s, iv = SA[rows, :], SQ[rows, :], INV[rows, :]
        for cs in COLS:
            col = slice(cs, cs + 128)
            GC[cs // 128, out_rows, :] = iv * (GA[rows, col] - f - NRM[rows, col] * s)
        return 0

    lax.fori_loop(0, T // 32, gc_body, 0)
    halo = halo_start(GC)
    dw(G, [0], AT[...], x // 2, 1, 4)
    for h in (0, 1):
        sc[0][h].s2i()

    mark("taps")
    for cs in COLS:
        def tap_body(i, accs, cs=cs):
            r0 = pl.multiple_of(i * 32, 32)
            g = GC[cs // 128, pl.ds(r0 + PAD, 32), :]
            accs = list(accs)
            for o in range(1, TAPS + 1):
                prod = HID[cs // 128, pl.ds(r0 + o, 32), :] * g
                accs[o - 1] = accs[o - 1] + prod.reshape(4, 8, 128).sum(axis=0)
            return tuple(accs)

        accs = lax.fori_loop(
            0, T // 32, tap_body, tuple(jnp.zeros((8, 128), F32) for _ in range(TAPS))
        )
        for k, a in enumerate(accs):
            TP[k:k + 1, cs:cs + 128] = jnp.sum(a, axis=0, keepdims=True)
    TP[TAPS:TAPS + 1, :] = jnp.sum(GP[...], axis=0, keepdims=True)

    def small_send(e, src, me, at):
        TGR[e, me] = src(me)[...]
        i = new_recv()
        for d in (1, 3, 2):
            rcopy(src((me + d) % 4), TGR.at[e, me], at(me + d), i)
        return i

    def small_sum(e, i):
        wait_all(TGR.at[e, pl.ds(0, 3)], i)
        v = TGR[e, 0].astype(F32)
        for i in range(1, 4):
            v = v + TGR[e, i].astype(F32)
        return v.astype(BF16)

    for t in range(4):
        TG[t] = TP[:, t * 128:t * 128 + 128].astype(BF16)
    small = small_send(0, lambda t: TG.at[t], x, at_x)
    mark("relay")
    relays = exchange_relay()
    drain(early)
    mark("halo2w")
    halo_finish(GC, halo)

    mark("back")
    def back_body(i, _):
        r0 = pl.multiple_of(i * R, R)
        rows = pl.ds(r0, R)
        for cs in COLS:
            col = slice(cs, cs + 128)
            gh = conv_tile(GC, r0, cs, True)
            s = PG[rows, col]
            gv = gh * s
            GV[rows, col] = gv.astype(BF16)
            GG[rows, col] = (gv * PV[rows, col] * (1.0 - s)).astype(BF16)
        return 0

    lax.fori_loop(0, T // R, back_body, 0)

    middle = len(sent)
    mark("vg_t")
    for n in (0, 256):
        BT[n // 256, 0:256, :] = flipped(GV, n)

    class Spread:
        def __init__(self, h, u):
            self.h, self.p = h, me_p[h]
            self.lo, self.hi = pl.ds(u * 256, 128), pl.ds(u * 256 + 128, 128)

        def start(self):
            h, p, lo, hi = self.h, self.p, self.lo, self.hi
            own, got = BT.at[h], BTR.at[h]
            nxt, prv = at_p[h](p + 1), at_p[h](p + 3)
            self.h1p = rcopy(own.at[lo], got.at[0, lo], nxt)
            self.h1m = rcopy(own.at[hi], got.at[2, hi], prv)
            self.h2p = rcopy(own.at[hi], got.at[0, hi], nxt)
            self.h2m = rcopy(own.at[lo], got.at[2, lo], prv)

        def first(self):
            h, p, lo, hi = self.h, self.p, self.lo, self.hi
            got = BTR.at[h]
            self.h1p.wait_recv()
            self.fp = rcopy(got.at[0, lo], got.at[1, lo], at_p[h](p + 1))
            self.h1m.wait_recv()
            self.fm = rcopy(got.at[2, hi], got.at[1, hi], at_p[h](p + 3))

        def second(self):
            self.h2p.wait_recv()
            self.h2m.wait_recv()

        def third(self):
            self.fp.wait_recv()
            self.fm.wait_recv()

    def own_in(h, q):
        zz, xx = (q, x) if h == 0 else (z, q)
        cols = pl.ds(pl.multiple_of((xx % 2) * 256, 256), 256)
        return X[zz * 2 + xx // 2, :, cols]

    def got_in(h, k, q):
        if h == 0:
            return XA[k, q]
        return XB[k, q // 2, :, pl.ds(pl.multiple_of((q % 2) * 256, 256), 256)]

    def vg_own(h):
        def body(q, _):
            VACC[h, q] = dot_nn(BT[h], own_in(h, q))
            return 0

        lax.fori_loop(0, 4, body, 0)

    def vg_near(h, u):
        rows = pl.ds(u * 256, 256)

        def body(q, _):
            VACC[h, q, rows] += dot_nn(BTR[h, 0, rows], got_in(h, 0, q)) + dot_nn(BTR[h, 2, rows], got_in(h, 2, q))
            return 0

        lax.fori_loop(0, 4, body, 0)

    class Last:
        def __init__(self, h, u):
            self.h, self.u, self.q = h, u, me_q[h]
            self.rows = pl.ds(u * 256, 256)

        def make(self, dq):
            h, rows = self.h, self.rows
            qq = (self.q + dq) % 4
            VP[h, qq, rows] = (VACC[h, qq, rows] + dot_nn(BTR[h, 1, rows], got_in(h, 1, qq))).astype(BF16)

        def s1(self):
            h, u, q = self.h, self.u, self.q
            src = VP.at[h, (q + 2) % 4]
            self.i = rcopy(src.at[pl.ds(u * 256, 128)], r3v.at[h, u, 0], at_q[h](q + 1))
            self.j = rcopy(src.at[pl.ds(u * 256 + 128, 128)], r3v.at[h, u, 1], at_q[h](q + 3))

        def s2(self):
            h, u, q, rows = self.h, self.u, self.q, self.rows

            def add(qq, row0, k):
                def body(i, _):
                    rr = pl.ds(pl.multiple_of(row0 + i * 64, 64), 64)
                    fr = pl.ds(pl.multiple_of(i * 64, 64), 64)
                    VP[h, qq, rr] = (VP[h, qq, rr].astype(F32) + r3v[h, u, k, fr].astype(F32)).astype(BF16)
                    return 0

                lax.fori_loop(0, 2, body, 0)

            up, down = (q + 1) % 4, (q + 3) % 4
            self.i.wait_recv()
            add(up, u * 256, 0)
            self.k = new_recv()
            rcopy(VP.at[h, up, rows], r4v.at[h, 0, rows], at_q[h](q + 1), self.k)
            self.j.wait_recv()
            add(down, u * 256 + 128, 1)
            rcopy(VP.at[h, down, rows], r4v.at[h, 1, rows], at_q[h](q + 3), self.k)

        def finish(self):
            h, u, q = self.h, self.u, self.q
            wait_all(r4v.at[h, :, self.rows], self.k)
            for i in (0, 128):
                rr = slice(u * 256 + i, u * 256 + i + 128)
                v = VP[h, q, rr].astype(F32) + r4v[h, 0, rr].astype(F32) + r4v[h, 1, rr].astype(F32)
                w_out[u + 1, :, h * 256 + i:h * 256 + i + 128] = v.T.astype(BF16)

    spread = [[Spread(0, u), Spread(1, u)] for u in (0, 1)]
    last = [[Last(0, u), Last(1, u)] for u in (0, 1)]
    for h in (0, 1):
        spread[0][h].start()
    for n in (0, 256):
        BT[n // 256, 256:512, :] = flipped(GG, n)

    mark("partial1")
    def partial(parity):
        def body(i, _):
            yy = i // 2
            rows = pl.ds(pl.multiple_of((i % 2) * 256, 256), 256)
            j = yy * 2 + parity
            gv, gt = GV[rows, :], GG[rows, :]
            for n in (0, 256):
                G[parity * 4 + yy, rows, n:n + 256] = (
                    dot_nt(gv, WV[j, n:n + 256, :]) + dot_nt(gt, WG[j, n:n + 256, :])
                ).astype(BF16)
            return 0

        lax.fori_loop(0, 8, body, 0)

    partial(1 - c)
    swap = rcopy(G.at[pl.ds((1 - c) * 4, 4)], PR, partner)
    mark("small")
    TG1[0] = small_sum(0, small)
    small = small_send(1, lambda t: TG1.at[0], z, at_z)
    mark("v_first")
    for h in (0, 1):
        spread[0][h].first()
    for h in (0, 1):
        spread[1][h].start()
    mark("ow_s2d")
    for h in (0, 1):
        sc[0][h].s2d()
    mark("partial2")
    partial(c)
    mark("yadd")
    swap.wait_recv()

    def y_add(block, row0, n, sources):
        def body(i, _):
            rr = pl.ds(pl.multiple_of(row0 + i * 32, 32), 32)
            v = G[block, rr].astype(F32)
            for ref, index, off in sources:
                v = v + ref[index + (pl.ds(pl.multiple_of(off + i * 32, 32), 32),)].astype(F32)
            G[block, rr] = v.astype(BF16)
            return 0

        lax.fori_loop(0, n // 32, body, 0)

    base = c * 4
    y2_, yp_, ym_ = (y + 2) % 4, (y + 1) % 4, (y + 3) % 4
    y_add(base + y2_, 0, T, [(PR, (y2_,), 0)])
    ya = rcopy(G.at[base + y2_, LO], y1.at[0], at_y(y + 1))
    yb = rcopy(G.at[base + y2_, HIH], y1.at[1], at_y(y + 3))
    y_add(base + yp_, 0, T, [(PR, (yp_,), 0)])
    yc = rcopy(G.at[base + yp_, HIH], y2.at[0, HIH], at_y(y + 1))
    y_add(base + ym_, 0, T, [(PR, (ym_,), 0)])
    yd = rcopy(G.at[base + ym_, LO], y2.at[1, LO], at_y(y + 3))
    y_add(base + y, 0, T, [(PR, (y,), 0)])

    mark("small2")
    TG1[1] = small_sum(1, small)
    small = small_send(2, lambda t: TG1.at[1], x, at_x)
    mark("vg_own")
    for h in (0, 1):
        vg_own(h)
    third = len(sent) - middle
    mark("v_near")
    for cp in relays:
        cp.wait_recv()
    drain(middle)
    for h in (0, 1):
        spread[0][h].second()
    for h in (0, 1):
        vg_near(h, 0)
    mark("v_third")
    for h in (0, 1):
        spread[0][h].third()
    mark("v_far")
    for h in (0, 1):
        last[0][h].make(2)
        last[0][h].s1()
    for dq in (1, 3, 0):
        for h in (0, 1):
            last[0][h].make(dq)
    mark("g_first")
    for h in (0, 1):
        spread[1][h].first()
    mark("y_s2")
    ya.wait_recv()
    y_add(base + yp_, 0, 256, [(y1, (0,), 0)])
    ye = rcopy(G.at[base + yp_, LO], y2.at[0, LO], at_y(y + 1))
    yb.wait_recv()
    y_add(base + ym_, 256, 256, [(y1, (1,), 0)])
    yf = rcopy(G.at[base + ym_, HIH], y2.at[1, HIH], at_y(y + 3))
    mark("g_second")
    for h in (0, 1):
        spread[1][h].second()
    mark("g_near")
    for h in (0, 1):
        vg_near(h, 1)
    drain(third)
    mark("ow_p1")
    for h in (0, 1):
        sc[0][h].p1()
    mark("v_s2")
    for h in (0, 1):
        last[0][h].s2()
    mark("g_third")
    for h in (0, 1):
        spread[1][h].third()
    mark("g_far")
    for h in (0, 1):
        last[1][h].make(2)
        last[1][h].s1()
    mark("ow_p2")
    for h in (0, 1):
        sc[0][h].p2()
    mark("g_rest")
    for dq in (1, 3, 0):
        for h in (0, 1):
            last[1][h].make(dq)
    mark("g_s2")
    for h in (0, 1):
        last[1][h].s2()
    mark("small3")
    wait_all(TGR.at[2, pl.ds(0, 3)], small)
    for t in range(4):
        small_out[:, t * 128:t * 128 + 128] = TGR[2, t].astype(F32)
    mark("y_fin")
    for cp in (yc, yd, ye, yf):
        cp.wait_recv()

    def gi_body(i, _):
        rr = pl.ds(pl.multiple_of(i * 32, 32), 32)
        gi_out[rr, :] = (
            G[base + y, rr].astype(F32) + y2[0, rr].astype(F32) + y2[1, rr].astype(F32)
        ).astype(BF16)
        return 0

    lax.fori_loop(0, T // 32, gi_body, 0)
    mark("fin_v")
    for h in (0, 1):
        last[0][h].finish()
    mark("fin_o")
    for h in (0, 1):
        sc[0][h].finish()
    mark("fin_g")
    for h in (0, 1):
        last[1][h].finish()
    mark("sends")
    drain(len(sent))
    for d in (1, 2, 3):
        ex_b(d, (z + d) % 4).wait_send()
    mark(None)
    assert counter[0] == N_COPIES


def unpack(gi_in, w_in, small_in, gi, gvw, ggw, gow, gt, gg, b_out, so):
    writes = [pltpu.make_async_copy(gi_in, gi, so.at[3])]
    writes[0].start()
    for u, dst in enumerate((gow, gvw, ggw)):
        b_out[u] = w_in[u].astype(F32)
        writes.append(pltpu.make_async_copy(b_out.at[u], dst, so.at[u]))
        writes[-1].start()
    gt[...] = small_in[0:TAPS]
    gg[...] = small_in[TAPS:TAPS + 1]
    for cp in writes:
        cp.wait()


def local(inputs, w_value, w_gate, taps, ln_gain, w_out, grad_out):
    vm = pltpu.VMEM
    anyspace = pl.BlockSpec(memory_space=pl.ANY)
    in_vmem = pl.BlockSpec(memory_space=pltpu.VMEM)
    shape3 = (NB, C, C)
    gi, w3, small = pl.pallas_call(
        kernel,
        out_shape=(
            vm((T, C), BF16),
            vm((3, 256, C), BF16),
            vm((32, C), F32),
        ),
        in_specs=[anyspace] * 7,
        out_specs=(in_vmem,) * 3,
        scratch_shapes=[
            vm((NB, T, C), BF16), vm((NB, T, C), BF16),
            vm(shape3, BF16), vm(shape3, BF16), vm(shape3, BF16),
            vm((T, C), F32), vm((T, C), F32), vm((T, C), F32), vm((T, C), F32),
            vm((4, T + 2 * PAD, 128), F32), vm((4, T + 2 * PAD, 128), F32),
            vm((T, C), BF16), vm((T, C), BF16), vm((T, C), BF16),
            vm((512, T), BF16), vm((2, 512, T), BF16),
            vm((T, 128), F32), vm((T, 128), F32), vm((T, 128), F32), vm((T, 128), F32),
            vm((32, C), F32),
            vm((2, 8, 128), F32), vm((2, NB, 8, 128), F32),
            vm((32, C), F32), vm((8, C), F32),
            vm((4, 32, 128), BF16), vm((2, 32, 128), BF16), vm((3, 4, 32, 128), BF16),
            vm((1, 2, 4, 4, 256, 256), BF16),
            vm((1, 2, 2, 2, 256, 256), BF16),
            vm((1, 2, 2, 4, 256, 256), BF16),
            vm((1, 2, 2, 128, 256), BF16),
            vm((1, 2, 2, 256, 256), BF16),
            vm((3, 4, T, 256), BF16), vm((3, 2, T, C), BF16),
            vm((2, 3, 512, T), BF16),
            vm((2, 4, 512, 256), F32), vm((2, 4, 512, 256), BF16),
            vm((2, 2, 2, 128, 256), BF16), vm((2, 2, 512, 256), BF16),
            vm((4, T, C), BF16),
            vm((2, 256, C), BF16), vm((2, T, C), BF16),
            vm((TAPS, C), BF16), vm((1, C), F32),
            pltpu.SemaphoreType.DMA((N_SENDS,)),
            pltpu.SemaphoreType.DMA((N_COPIES,)),
            pltpu.SemaphoreType.DMA((7,)),
        ],
        compiler_params=pltpu.CompilerParams(
            collective_id=0, has_side_effects=True, vmem_limit_bytes=64 * 1024 * 1024 - 3 * 1024 * 1024
        ),
    )(
        inputs, grad_out, w_value.reshape(shape3), w_gate.reshape(shape3), w_out.reshape(shape3),
        taps, ln_gain.reshape(1, C),
    )
    gi, gvw, ggw, gow, gt, gg = pl.pallas_call(
        unpack,
        out_shape=(
            jax.ShapeDtypeStruct((T, C), BF16),
            jax.ShapeDtypeStruct((256, C), F32),
            jax.ShapeDtypeStruct((256, C), F32),
            jax.ShapeDtypeStruct((256, C), F32),
            jax.ShapeDtypeStruct((TAPS, C), F32),
            jax.ShapeDtypeStruct((1, C), F32),
        ),
        in_specs=[in_vmem] * 3,
        out_specs=(anyspace,) * 4 + (in_vmem,) * 2,
        scratch_shapes=[vm((3, 256, C), F32), pltpu.SemaphoreType.DMA((4,))],
        compiler_params=pltpu.CompilerParams(vmem_limit_bytes=8 * 1024 * 1024),
    )(gi, w3, small)
    return gi, gvw, ggw, gow, gt, gg.reshape(C)


def solution(mesh):
    in_specs = (
        P("sp", "tp"), P(None, "tp"), P(None, "tp"), P(None, "tp"), P("tp"), P(None, "tp"), P("sp", "tp"),
    )
    out_specs = (P("sp", "tp"), P("sp", "tp"), P("sp", "tp"), P("sp", "tp"), P(None, "tp"), P("tp"))
    return jax.shard_map(local, mesh=mesh, in_specs=in_specs, out_specs=out_specs, check_vma=False)
```
